128 devices in a mesh: rep: 2 (over z_hi), fs: 32 (over z_lo, y, x), tp: 2 (over core).
Axes of the slice: x: 4, y: 4, z: 4 (z_hi: 2, z_lo: 2; z = z_hi * 2 + z_lo), core: 2. Of those that a mesh axis runs over, the one named last changes fastest.
Arguments:
- inputs: bfloat16 [32768, 1024], P(('rep', 'fs', 'tp')), may hold values from -6 to 6
- up_proj: bfloat16 [1024, 4096], P('fs', 'tp'), may hold values from -0.1875 to 0.1875
- down_proj: bfloat16 [4096, 1024], P('tp', 'fs'), may hold values from -0.09375 to 0.09375
- out_cotangent: bfloat16 [32768, 1024], P(('rep', 'fs', 'tp')), may hold values from -24 to 24
Outputs:
- grad_inputs: bfloat16 [32768, 1024], P(('rep', 'fs', 'tp'))
- grad_up: float32 [1024, 4096], P('fs', 'tp')
- grad_down: float32 [4096, 1024], P('tp', 'fs')
- energy_up: float32 [1024], P('fs')
- energy_down: float32 [4096], P('tp')
The draws below stay inside these ranges and needn't reach their ends.
All inputs are finite; a program needn't handle non-finite values.
Results may differ from the reference program's by a relative error of at most 0.001.
Values may be sent and summed in bfloat16 or wider, within the bound.
A program may use at most 128 MiB of HBM per device.

```python
import jax
import jax.numpy as jnp
from jax import lax

D = 1024
FF = 4096
TOKENS = 32768


def raised(entries, key, source, target, parts, factor):
    owner, partner = [(jnp.arange(entries.shape[position]) // (entries.shape[position] // parts)).reshape([-1 if axis == position else 1 for axis in range(entries.ndim)]) for position in (source, target)]
    chosen = jax.random.permutation(key, parts)[partner]
    strong = (owner == chosen) | (owner == (partner + parts // 2) % parts)
    return jnp.where(strong, factor * entries, entries)


def level_of(rng, extent, shards, smallest, top_value):
    factor_of = 1.0
    for dim, blocks in shards:
        heights = jax.random.uniform(jax.random.fold_in(jax.random.fold_in(rng, 6), dim), (blocks,), jnp.float32, smallest / len(shards), top_value / len(shards))
        factor_of = factor_of * jnp.repeat(jnp.exp(heights), extent[dim] // blocks).reshape((-1,) + (1,) * (len(extent) - 1 - dim))
    return factor_of


def gaussian(rng, dims, width, bound, cuts=(), dtype=jnp.bfloat16):
    array = width * jax.random.normal(rng, dims, jnp.float32)
    if cuts:
        array = array * level_of(rng, dims, cuts, -0.22, 0.18)
    return jnp.clip(array, -bound, bound).astype(dtype)


def heavy_noise(key, shape, deviation, reach, split, heavy, held_as=jnp.bfloat16):
    entries = deviation * jax.random.normal(key, shape, jnp.float32)
    if split:
        entries = entries * level_of(key, shape, split, -0.22, 0.18)
    return jnp.clip(raised(entries, jax.random.fold_in(key, 3), *heavy), -reach, reach).astype(held_as)


def setup_inputs(seed: int = 0) -> dict:
    streams_of = jax.random.split(jax.random.key(seed), 5)
    return {
        "inputs": gaussian(streams_of[0], (TOKENS, D), 1.0, 6.0, ((0, 128),)),
        "up_proj": gaussian(streams_of[1], (D, FF), D ** -0.5, 0.1875, ((0, 32), (1, 2))),
        "down_proj": gaussian(streams_of[2], (FF, D), FF ** -0.5, 0.09375, ((0, 2), (1, 32))),
        "out_cotangent": heavy_noise(streams_of[3], (TOKENS, D), 1.0, 24.0, ((0, 128),), (0, 1, 128, 5.5)),
    }


def contract(left, right, left_dim, right_dim):
    return lax.dot_general(left, right, (((left_dim,), (right_dim,)), ((), ())), preferred_element_type=jnp.float32)


def reference(inputs, up_proj, down_proj, out_cotangent):
    factor = float(TOKENS) ** -0.5
    pre = jnp.dot(inputs, up_proj, preferred_element_type=jnp.float32)
    active = jnp.square(jax.nn.relu(pre)).astype(jnp.bfloat16)
    back = contract(out_cotangent, down_proj, 1, 1)
    grad_pre = (2.0 * jax.nn.relu(pre) * back).astype(jnp.bfloat16)
    grad_inputs = contract(grad_pre, up_proj, 1, 1).astype(jnp.bfloat16)
    grad_up = contract(inputs, grad_pre, 0, 0) * factor
    grad_down = contract(active, out_cotangent, 0, 0) * factor
    energy_up = jnp.sum(grad_up * grad_up, axis=1) / FF
    energy_down = jnp.sum(grad_down * grad_down, axis=1) / D
    return grad_inputs, grad_up, grad_down, energy_up, energy_down
```

```python
import jax
import jax.numpy as jnp
from jax import lax
from jax.experimental import pallas as pl
from jax.experimental.pallas import tpu as pltpu
from jax.sharding import Mesh
from jax.sharding import PartitionSpec as P

FS = ("fs_0", "fs_1", "fs_2")
REP_FS_TP = ("rep", "fs_0", "fs_1", "fs_2", "tp")
MESH = pl.DeviceIdType.MESH
BF = jnp.bfloat16
F32 = jnp.float32
RIGHT, LEFT = 0, 1
UP, DN = 0, 1
COPIES = 240


def make_kernel(tokens, width, cols, ff, factor):
    lanes = [pl.ds(c * 128, 128) for c in range(cols // 128)]

    def kernel(
        x_ref, up_ref, dn_ref, cot_ref,
        gin_ref, gup_ref, gdn_ref, eup_ref, edn_ref,
        X, C, XT, CT, W, RP, ACT, GP, G,
        s1s, s1r, c1s, c1r, R1, s2s, s2r, c2s, c2r, R2, s3s, s3r, c3s, c3r,
        PART, DR, ZR, EX, EY, EZ, EU,
        ssem, rsem, lsem,
    ):
        r = lax.axis_index("rep")
        j = lax.axis_index("fs_0")
        y = lax.axis_index("fs_1")
        x = lax.axis_index("fs_2")
        t = lax.axis_index("tp")

        def at(pos, d):
            return lax.rem(pos + d, 4)

        def xdev(d):
            return {"fs_2": at(x, d)}

        def ydev(d):
            return {"fs_1": at(y, d)}

        zpeer = {"fs_0": 1 - j}
        rpeer = {"rep": 1 - r}
        rzpeer = {"rep": 1 - r, "fs_0": 1 - j}
        tpeer = {"tp": 1 - t}

        barrier = pltpu.get_barrier_semaphore()
        peers = [xdev(1), xdev(2), xdev(3), ydev(1), ydev(2), ydev(3), zpeer, rpeer, rzpeer, tpeer]
        for dev in peers:
            pl.semaphore_signal(barrier, inc=1, device_id=dev, device_id_type=MESH)
        pl.semaphore_wait(barrier, len(peers))

        copies = {}

        def send(key, src, dst, dev):
            n = len(copies)
            c = pltpu.make_async_remote_copy(
                src_ref=src, dst_ref=dst, send_sem=ssem.at[n], recv_sem=rsem.at[n],
                device_id=dev, device_id_type=MESH,
            )
            c.start()
            copies[key] = c

        def recv(key):
            copies[key].wait_recv()

        half = tokens // 2
        own = pl.ds(pl.multiple_of(j * cols, cols), cols)
        other = pl.ds(pl.multiple_of((1 - j) * cols, cols), cols)
        w_refs = (up_ref, dn_ref)

        for w in (UP, DN):
            send(("a2a", w), w_refs[w].at[:, :, other], W.at[w, j, y, x], zpeer)
        locals_ = [
            pltpu.make_async_copy(up_ref.at[:, :, own], W.at[UP, j, y, x], lsem.at[0]),
            pltpu.make_async_copy(dn_ref.at[:, :, own], W.at[DN, j, y, x], lsem.at[1]),
            pltpu.make_async_copy(x_ref, X.at[0], lsem.at[2]),
            pltpu.make_async_copy(cot_ref, C.at[0], lsem.at[3]),
        ]
        for c in locals_:
            c.start()

        def blk(ref, w, h, a, b):
            z = j if h == 0 else 1 - j
            return ref.at[w, z, b, a] if h == 0 else ref.at[w, z, a, b]

        def axes(h):
            return (x, y, xdev, ydev) if h == 0 else (y, x, ydev, xdev)

        def init(w, h):
            a, b, adev, bdev = axes(h)
            src = w_refs[w].at[:, :, own] if h == 0 else blk(W, w, h, a, b)
            dst = blk(W, w, h, a, b)
            send((1, w, h, 0), src, dst, adev(1))
            send((1, w, h, 1), src, dst, adev(3))
            send((2, w, h, 0, 0), src, dst, bdev(1))
            send((2, w, h, 0, 1), src, dst, bdev(3))

        def spread(w, h, s, a2):
            _, b, _, bdev = axes(h)
            ref = blk(W, w, h, a2, b)
            send((2, w, h, s, 0), ref, ref, bdev(1))
            send((2, w, h, s, 1), ref, ref, bdev(3))

        def step1(w, h):
            a, b, adev, _ = axes(h)
            recv((1, w, h, 0))
            ref = blk(W, w, h, at(a, 3), b).at[0]
            send((1, w, h, 2), ref, ref, adev(1))
            spread(w, h, 1, at(a, 3))
            recv((1, w, h, 1))
            ref = blk(W, w, h, at(a, 1), b).at[1]
            send((1, w, h, 3), ref, ref, adev(3))
            spread(w, h, 2, at(a, 1))

        def step2(w, h):
            a = axes(h)[0]
            recv((1, w, h, 2))
            recv((1, w, h, 3))
            spread(w, h, 3, at(a, 2))

        def fwd(w, h, s):
            a, b, _, bdev = axes(h)
            a2 = at(a, (0, 3, 1, 2)[s])
            recv((2, w, h, s, 0))
            ref = blk(W, w, h, a2, at(b, 3)).at[0]
            send((2, w, h, s, 2), ref, ref, bdev(1))
            recv((2, w, h, s, 1))
            ref = blk(W, w, h, a2, at(b, 1)).at[1]
            send((2, w, h, s, 3), ref, ref, bdev(3))

        def fin(w):
            for h in (0, 1):
                for s in range(4):
                    recv((2, w, h, s, 2))
                    recv((2, w, h, s, 3))

        def pass_on(name, buf, i):
            recv((name, "z", i))
            part = buf.at[2, pl.ds(i * half, half)]
            send((name, "zt", i), part, buf.at[3, pl.ds(i * half, half)], tpeer)

        def arrived(name, slot):
            if slot == 1:
                recv((name, "t"))
            if slot == 3:
                recv((name, "zt", 0))
                recv((name, "zt", 1))

        def turn(src, dst, slot):
            v = src[slot].T
            dst[:, :, :, :, slot * tokens:(slot + 1) * tokens] = v.reshape(2, 4, 4, width // 32, tokens)

        tile = min(512, cols)

        def weight(w, n):
            return W[w, :, :, :, :, :, pl.ds(pl.multiple_of(n * tile, tile), tile)].reshape(width, tile)

        def project(slot):
            def body(n, _):
                col = pl.ds(pl.multiple_of(n * tile, tile), tile)
                pre = jnp.maximum(jnp.dot(X[slot], weight(UP, n), preferred_element_type=F32), 0.0)
                RP[slot, :, col] = pre
                ACT[slot, :, col] = (pre * pre).astype(BF)
                return 0
            lax.fori_loop(0, cols // tile, body, 0)

        def pull_back(slot):
            def body(n, _):
                col = pl.ds(pl.multiple_of(n * tile, tile), tile)
                back = jnp.dot(C[slot], weight(DN, n), preferred_element_type=F32)
                GP[slot, :, col] = (2.0 * RP[slot, :, col] * back).astype(BF)
                return 0
            lax.fori_loop(0, cols // tile, body, 0)

        init(UP, 0)
        init(DN, 0)
        for name, src, dst in (("x", x_ref, X), ("c", cot_ref, C)):
            for i in (0, 1):
                rows = pl.ds(i * half, half)
                send((name, "z", i), src.at[rows], dst.at[2, rows], zpeer)
            send((name, "t"), src, dst.at[1], tpeer)
        recv(("a2a", UP))
        init(UP, 1)
        step1(UP, 0)
        fwd(UP, 0, 0)
        recv(("a2a", DN))
        init(DN, 1)
        step1(UP, 1)
        fwd(UP, 1, 0)
        step2(UP, 0)
        fwd(UP, 0, 1)
        fwd(UP, 0, 2)
        step1(DN, 0)
        fwd(DN, 0, 0)
        step2(UP, 1)
        fwd(UP, 1, 1)
        fwd(UP, 1, 2)
        step1(DN, 1)
        fwd(DN, 1, 0)
        for c in locals_:
            c.wait()
        turn(X, XT, 0)
        fwd(UP, 0, 3)
        fwd(UP, 1, 3)
        arrived("x", 1)
        turn(X, XT, 1)
        step2(DN, 0)
        fwd(DN, 0, 1)
        fwd(DN, 0, 2)
        pass_on("x", X, 0)
        turn(C, CT, 0)
        step2(DN, 1)
        fwd(DN, 1, 1)
        fwd(DN, 1, 2)
        arrived("c", 1)
        turn(C, CT, 1)
        pass_on("x", X, 1)
        fin(UP)
        project(0)
        project(1)
        turn(X, XT, 2)
        project(2)
        fwd(DN, 0, 3)
        fwd(DN, 1, 3)
        arrived("x", 3)
        turn(X, XT, 3)
        project(3)
        pass_on("c", C, 0)
        fin(DN)
        pull_back(0)
        pull_back(1)
        pass_on("c", C, 1)
        turn(C, CT, 2)
        arrived("c", 3)
        turn(C, CT, 3)

        lhs_of = (XT, CT)
        rhs_of = (GP, ACT)

        def gblk(w, h, a, b):
            z = j if h == 0 else 1 - j
            return G.at[w, z, a, b] if h == 0 else G.at[w, z, b, a]

        def raxes(h):
            return (y, x, ydev, xdev) if h == 0 else (x, y, xdev, ydev)

        def multiply(w, h, a1, a2):
            z = j if h == 0 else 1 - j
            lhs = lhs_of[w]
            if h == 0:
                l1, l2 = lhs[z, a1], lhs[z, a2]
            else:
                l1, l2 = lhs[z, :, a1], lhs[z, :, a2]
            rows = 4 * (width // 32)
            left = jnp.concatenate([l1.reshape(rows, -1), l2.reshape(rows, -1)], axis=0)

            def body(n, _):
                col = pl.ds(pl.multiple_of(n * tile, tile), tile)
                right = rhs_of[w][:, :, col].reshape(4 * tokens, tile)
                out = jnp.dot(left, right, preferred_element_type=F32)
                for k, a in enumerate((a1, a2)):
                    part = out[k * rows:(k + 1) * rows].reshape(4, width // 32, tile)
                    if h == 0:
                        G[w, z, a, :, :, col] = part
                    else:
                        G[w, z, :, a, :, col] = part
                return 0
            lax.fori_loop(0, cols // tile, body, 0)

        def encode(srcs, dst, scale):
            top = None
            for src in srcs:
                for c in lanes:
                    m = jnp.max(jnp.abs(src[:, c]).reshape(-1, 8, 128), axis=0)
                    top = m if top is None else jnp.maximum(top, m)
            top = jnp.maximum(top, 2e-34)
            scale[...] = top
            inv = 32768.0 / top
            for i, src in enumerate(srcs):
                for c in lanes:
                    v = src[:, c]
                    v3 = v.reshape(-1, 8, 128) * inv
                    for _ in range(3):
                        v3 = v3 * jnp.abs(v3)
                    dst[i, :, c] = v3.reshape(v.shape).astype(BF)

        def decode(buf, scale, i, c):
            v = buf[i, :, c].astype(F32)
            m = jnp.exp2(jnp.log2(jnp.abs(v)) * 0.125)
            m = jnp.where(v < 0, -m, m).reshape(-1, 8, 128) * (scale[...] * (1.0 / 32768.0))
            return m.reshape(v.shape)

        class Ring:
            def __init__(self, stage, w, h, pos, dev, parts, bufs):
                self.k = (stage, w, h)
                self.pos, self.dev, self.parts = pos, dev, parts
                self.sb, self.rb, self.sc, self.rc = (b.at[2 * w + h] for b in bufs)

            def post(self, i, srcs, d):
                encode(srcs, self.sb.at[i], self.sc.at[i])
                send(self.k + (i, "s"), self.sc.at[i], self.rc.at[i], self.dev(d))
                send(self.k + (i, "v"), self.sb.at[i], self.rb.at[i], self.dev(d))

            def take(self, i, refs):
                recv(self.k + (i, "s"))
                recv(self.k + (i, "v"))
                for n, ref in enumerate(refs):
                    for c in lanes:
                        ref[:, c] = ref[:, c] + decode(self.rb.at[i], self.rc.at[i], n, c)

            def far(self):
                self.post(0, self.parts(at(self.pos, 2), 0), 1)
                self.post(1, self.parts(at(self.pos, 2), 1), 3)

            def near_right(self):
                self.post(2, self.parts(at(self.pos, 1), 1), 1)

            def near_left(self):
                self.post(3, self.parts(at(self.pos, 3), 0), 3)

            def relay(self):
                p = self.parts(at(self.pos, 1), 0)
                self.take(0, p)
                self.post(4, p, 1)
                p = self.parts(at(self.pos, 3), 1)
                self.take(1, p)
                self.post(5, p, 3)

            def near_in(self):
                self.take(3, self.parts(self.pos, 0))
                self.take(2, self.parts(self.pos, 1))

            def last_in(self):
                self.take(4, self.parts(self.pos, 0))
                self.take(5, self.parts(self.pos, 1))

        def ring1(w, h):
            a, b, adev, bdev = raxes(h)
            return Ring(1, w, h, a, adev,
                        lambda place, side: [gblk(w, h, place, 2 * side + i) for i in (0, 1)],
                        (s1s, s1r, c1s, c1r))

        hr = width // 64

        def ring2(w, h):
            a, b, adev, bdev = raxes(h)
            return Ring(2, w, h, b, bdev,
                        lambda place, side: [gblk(w, h, a, place).at[pl.ds(side * hr, hr)]],
                        (s2s, s2r, c2s, c2r))

        first = {(w, h): ring1(w, h) for w in (UP, DN) for h in (0, 1)}
        second = {(w, h): ring2(w, h) for w in (UP, DN) for h in (0, 1)}

        def launch(w):
            for h in (0, 1):
                a = raxes(h)[0]
                multiply(w, h, at(a, 2), at(a, 1))
                first[w, h].far()
                first[w, h].near_right()
            for h in (0, 1):
                a = raxes(h)[0]
                multiply(w, h, at(a, 3), a)
                first[w, h].near_left()

        def launch2(w):
            for h in (0, 1):
                first[w, h].near_in()
            for h in (0, 1):
                first[w, h].last_in()
                second[w, h].far()
                second[w, h].near_right()
                second[w, h].near_left()

        def relay2(w):
            for h in (0, 1):
                second[w, h].relay()

        def launch3(w):
            for h in (0, 1):
                second[w, h].near_in()
                second[w, h].last_in()
                a, b, _, _ = raxes(h)
                encode([gblk(w, h, a, b)], s3s.at[w, h], c3s.at[w, h])
                peers_ = [(0, rpeer)] if h == 0 else [(1, zpeer), (2, rzpeer)]
                for i, dev in peers_:
                    send((3, w, i, "s"), c3s.at[w, h], c3r.at[w, i], dev)
                    send((3, w, i, "v"), s3s.at[w, h], s3r.at[w, i], dev)

        def finish(w, out):
            for i in range(3):
                recv((3, w, i, "s"))
                recv((3, w, i, "v"))
            for c in range(len(lanes)):
                lane = lanes[c]
                mine = decode(s3s.at[w, 0], c3s.at[w, 0], 0, lane)
                mine = mine + decode(s3r.at[w, 0], c3r.at[w, 0], 0, lane)
                out[:, pl.ds(pl.multiple_of(j * cols + c * 128, 128), 128)] = mine * factor
                theirs = decode(s3r.at[w, 1], c3r.at[w, 1], 0, lane)
                theirs = theirs + decode(s3r.at[w, 2], c3r.at[w, 2], 0, lane)
                out[:, pl.ds(pl.multiple_of((1 - j) * cols + c * 128, 128), 128)] = theirs * factor

        def input_part(slot, out):
            def body(n, _):
                w = W[UP, n // 2, pl.ds(2 * lax.rem(n, 2), 2)].reshape(width // 4, cols)
                v = lax.dot_general(GP[slot], w, (((1,), (1,)), ((), ())), preferred_element_type=F32)
                out[:, pl.ds(pl.multiple_of(n * (width // 4), width // 4), width // 4)] = v
                return 0
            lax.fori_loop(0, 4, body, 0)

        launch(DN)
        pull_back(2)
        pull_back(3)
        input_part(3, PART.at[0])
        send(("g", "t", 0), PART.at[0], DR.at[0], tpeer)
        input_part(2, PART.at[1])
        recv(("g", "t", 0))
        PART[1] = PART[1] + DR[0]
        send(("g", "z"), PART.at[1], ZR, zpeer)
        for h in (0, 1):
            first[DN, h].relay()
        launch(UP)
        input_part(1, PART.at[2])
        send(("g", "t", 1), PART.at[2], DR.at[1], tpeer)
        launch2(DN)
        for h in (0, 1):
            first[UP, h].relay()
        input_part(0, PART.at[3])
        recv(("g", "t", 1))
        relay2(DN)
        launch2(UP)
        launch3(DN)
        relay2(UP)
        finish(DN, gdn_ref)

        EX[x] = jnp.sum(gdn_ref[...] * gdn_ref[...], axis=0, keepdims=True)
        for d in (1, 2, 3):
            send(("e", "x", d), EX.at[x], EX.at[x], xdev(d))
        launch3(UP)
        for d in (1, 2, 3):
            recv(("e", "x", d))
        EY[y] = EX[0] + EX[1] + EX[2] + EX[3]
        for d in (1, 2, 3):
            send(("e", "y", d), EY.at[y], EY.at[y], ydev(d))
        recv(("g", "z"))
        gin_ref[...] = (PART[3] + DR[1] + ZR[...]).astype(BF)
        for d in (1, 2, 3):
            recv(("e", "y", d))
        EZ[0] = EY[0] + EY[1] + EY[2] + EY[3]
        send(("e", "z"), EZ.at[0], EZ.at[1], zpeer)
        finish(UP, gup_ref)
        total = None
        for c in range(2 * len(lanes)):
            v = gup_ref[:, c * 128:(c + 1) * 128]
            total = v * v if total is None else total + v * v
        EU[0] = total
        send(("e", "t"), EU.at[0], EU.at[1], tpeer)
        recv(("e", "z"))
        edn_ref[...] = (EZ[0] + EZ[1]) * (1.0 / width)
        recv(("e", "t"))
        both = jnp.sum(EU[0] + EU[1], axis=1, keepdims=True) * (1.0 / ff)
        eup_ref[...] = jnp.broadcast_to(both, eup_ref.shape)
        for c in copies.values():
            c.wait_send()

    return kernel


def per_device(inputs, up_proj, down_proj, out_cotangent):
    tokens, width = inputs.shape
    rows, hidden = up_proj.shape
    cols = hidden // 2
    ff = hidden * lax.axis_size("tp")
    all_tokens = tokens * lax.axis_size("rep") * lax.axis_size(FS) * lax.axis_size("tp")
    factor = float(all_tokens) ** (-0.5)
    up3 = up_proj.reshape(2, rows // 2, hidden)
    dn3 = down_proj.T.reshape(2, rows // 2, hidden)
    vm = pl.BlockSpec(memory_space=pltpu.VMEM)
    full = (2, 4, 4, rows)
    gin, gup, gdn, eup, edn = pl.pallas_call(
        make_kernel(tokens, width, cols, ff, factor),
        out_shape=(
            jax.ShapeDtypeStruct((tokens, width), BF),
            jax.ShapeDtypeStruct((rows, hidden), F32),
            jax.ShapeDtypeStruct((rows, hidden), F32),
            jax.ShapeDtypeStruct((rows, 128), F32),
            jax.ShapeDtypeStruct((1, hidden), F32),
        ),
        in_specs=[vm] * 4,
        out_specs=(vm,) * 5,
        scratch_shapes=[
            pltpu.VMEM((4, tokens, width), BF),
            pltpu.VMEM((4, tokens, width), BF),
            pltpu.VMEM(full + (4 * tokens,), BF),
            pltpu.VMEM(full + (4 * tokens,), BF),
            pltpu.VMEM((2, 2, 4, 4, 2, rows // 2, cols), BF),
            pltpu.VMEM((4, tokens, cols), F32),
            pltpu.VMEM((4, tokens, cols), BF),
            pltpu.VMEM((4, tokens, cols), BF),
            pltpu.VMEM((2,) + full + (cols,), F32),
            pltpu.VMEM((4, 6, 2, rows, cols), BF),
            pltpu.VMEM((4, 6, 2, rows, cols), BF),
            pltpu.VMEM((4, 6, 8, 128), F32),
            pltpu.VMEM((4, 6, 8, 128), F32),
            pltpu.VMEM((8, 128), F32),
            pltpu.VMEM((4, 6, 1, rows // 2, cols), BF),
            pltpu.VMEM((4, 6, 1, rows // 2, cols), BF),
            pltpu.VMEM((4, 6, 8, 128), F32),
            pltpu.VMEM((4, 6, 8, 128), F32),
            pltpu.VMEM((8, 128), F32),
            pltpu.VMEM((2, 2, 1, rows, cols), BF),
            pltpu.VMEM((2, 3, 1, rows, cols), BF),
            pltpu.VMEM((2, 2, 8, 128), F32),
            pltpu.VMEM((2, 3, 8, 128), F32),
            pltpu.VMEM((4, tokens, width), F32),
            pltpu.VMEM((2, tokens, width), F32),
            pltpu.VMEM((tokens, width), F32),
            pltpu.VMEM((4, 1, hidden), F32),
            pltpu.VMEM((4, 1, hidden), F32),
            pltpu.VMEM((2, 1, hidden), F32),
            pltpu.VMEM((2, rows, 128), F32),
            pltpu.SemaphoreType.DMA((COPIES,)),
            pltpu.SemaphoreType.DMA((COPIES,)),
            pltpu.SemaphoreType.DMA((4,)),
        ],
        compiler_params=pltpu.CompilerParams(
            collective_id=0, has_side_effects=True, vmem_limit_bytes=63 * 1024 * 1024
        ),
    )(inputs, up3, dn3, out_cotangent)
    return gin, gup, gdn.T, eup[:, 0], edn.reshape(hidden)


def solution(mesh):
    torus = Mesh(
        mesh.devices.reshape(mesh.shape["rep"], 2, 4, 4, mesh.shape["tp"]),
        ("rep", "fs_0", "fs_1", "fs_2", "tp"),
    )
    placed = (P(REP_FS_TP, None), P(FS, "tp"), P("tp", FS), P(REP_FS_TP, None))
    return jax.shard_map(
        per_device,
        mesh=torus,
        in_specs=placed,
        out_specs=(P(REP_FS_TP, None), P(FS, "tp"), P("tp", FS), P(FS), P("tp")),
        check_vma=False,
    )
```

```python
import jax
import jax.numpy as jnp
from jax import lax
from jax.experimental import pallas as pl
from jax.experimental.pallas import tpu as pltpu
from jax.sharding import Mesh
from jax.sharding import PartitionSpec as P

FS = ("fs_0", "fs_1", "fs_2")
REP_FS_TP = ("rep", "fs_0", "fs_1", "fs_2", "tp")
MESH = pl.DeviceIdType.MESH
BF = jnp.bfloat16
F32 = jnp.float32
RIGHT, LEFT = 0, 1
UP, DN = 0, 1
COPIES = 240


def make_kernel(tokens, width, cols, ff, factor):
    lanes = [pl.ds(c * 128, 128) for c in range(cols // 128)]

    def kernel(
        x_ref, up_ref, dn_ref, cot_ref,
        gin_ref, gup_ref, gdn_ref, eup_ref, edn_ref,
        X, C, XT, CT, W, RP, ACT, GP, G,
        s1s, s1r, c1s, c1r, s2s, s2r, c2s, c2r, s3s, s3r, c3s, c3r,
        PART, DR, ZS, ZR, zsc, EX, EY, EZ, EU,
        ssem, rsem, lsem,
    ):
        r = lax.axis_index("rep")
        j = lax.axis_index("fs_0")
        y = lax.axis_index("fs_1")
        x = lax.axis_index("fs_2")
        t = lax.axis_index("tp")

        def at(pos, d):
            return lax.rem(pos + d, 4)

        def xdev(d):
            return {"fs_2": at(x, d)}

        def ydev(d):
            return {"fs_1": at(y, d)}

        zpeer = {"fs_0": 1 - j}
        rpeer = {"rep": 1 - r}
        rzpeer = {"rep": 1 - r, "fs_0": 1 - j}
        tpeer = {"tp": 1 - t}

        barrier = pltpu.get_barrier_semaphore()
        peers = [xdev(1), xdev(2), xdev(3), ydev(1), ydev(2), ydev(3), zpeer, rpeer, rzpeer, tpeer]
        for dev in peers:
            pl.semaphore_signal(barrier, inc=1, device_id=dev, device_id_type=MESH)
        pl.semaphore_wait(barrier, len(peers))

        copies = {}

        def send(key, src, dst, dev):
            n = len(copies)
            c = pltpu.make_async_remote_copy(
                src_ref=src, dst_ref=dst, send_sem=ssem.at[n], recv_sem=rsem.at[n],
                device_id=dev, device_id_type=MESH,
            )
            c.start()
            copies[key] = c

        def recv(key):
            copies[key].wait_recv()

        half = tokens // 2
        own = pl.ds(pl.multiple_of(j * cols, cols), cols)
        other = pl.ds(pl.multiple_of((1 - j) * cols, cols), cols)
        w_refs = (up_ref, dn_ref)

        for w in (UP, DN):
            send(("a2a", w), w_refs[w].at[:, :, other], W.at[w, j, y, x], zpeer)
        locals_ = [
            pltpu.make_async_copy(up_ref.at[:, :, own], W.at[UP, j, y, x], lsem.at[0]),
            pltpu.make_async_copy(dn_ref.at[:, :, own], W.at[DN, j, y, x], lsem.at[1]),
            pltpu.make_async_copy(x_ref, X.at[0], lsem.at[2]),
            pltpu.make_async_copy(cot_ref, C.at[0], lsem.at[3]),
        ]
        for c in locals_:
            c.start()

        def blk(ref, w, h, a, b):
            z = j if h == 0 else 1 - j
            return ref.at[w, z, b, a] if h == 0 else ref.at[w, z, a, b]

        def axes(h):
            return (x, y, xdev, ydev) if h == 0 else (y, x, ydev, xdev)

        def init(w, h):
            a, b, adev, bdev = axes(h)
            src = w_refs[w].at[:, :, own] if h == 0 else blk(W, w, h, a, b)
            dst = blk(W, w, h, a, b)
            send((1, w, h, 0), src, dst, adev(1))
            send((1, w, h, 1), src, dst, adev(3))
            send((2, w, h, 0, 0), src, dst, bdev(1))
            send((2, w, h, 0, 1), src, dst, bdev(3))

        def spread(w, h, s, a2):
            _, b, _, bdev = axes(h)
            ref = blk(W, w, h, a2, b)
            send((2, w, h, s, 0), ref, ref, bdev(1))
            send((2, w, h, s, 1), ref, ref, bdev(3))

        def near(w, h, side):
            a, b, adev, _ = axes(h)
            recv((1, w, h, side))
            place, away = ((at(a, 3), 1), (at(a, 1), 3))[side]
            ref = blk(W, w, h, place, b).at[side]
            send((1, w, h, 2 + side), ref, ref, adev(away))
            spread(w, h, 1 + side, place)

        def step2(w, h):
            a = axes(h)[0]
            recv((1, w, h, 2))
            recv((1, w, h, 3))
            spread(w, h, 3, at(a, 2))

        def fwd(w, h, s):
            a, b, _, bdev = axes(h)
            a2 = at(a, (0, 3, 1, 2)[s])
            recv((2, w, h, s, 0))
            ref = blk(W, w, h, a2, at(b, 3)).at[0]
            send((2, w, h, s, 2), ref, ref, bdev(1))
            recv((2, w, h, s, 1))
            ref = blk(W, w, h, a2, at(b, 1)).at[1]
            send((2, w, h, s, 3), ref, ref, bdev(3))

        def fin(w):
            for h in (0, 1):
                for s in range(4):
                    recv((2, w, h, s, 2))
                    recv((2, w, h, s, 3))

        def pass_on(name, buf, i):
            recv((name, "z", i))
            part = buf.at[2, pl.ds(i * half, half)]
            send((name, "zt", i), part, buf.at[3, pl.ds(i * half, half)], tpeer)

        def arrived(name, slot):
            if slot == 1:
                recv((name, "t"))
            if slot == 3:
                recv((name, "zt", 0))
                recv((name, "zt", 1))

        def turn(src, dst, slot):
            v = src[slot].T
            dst[:, :, :, :, slot * tokens:(slot + 1) * tokens] = v.reshape(2, 4, 4, width // 32, tokens)

        def weight(w):
            return W[w].reshape(width, cols)

        def both(ref, s1, s2):
            return jnp.concatenate([ref[s1], ref[s2]], axis=0)

        def project(s1, s2):
            pre = jnp.maximum(jnp.dot(both(X, s1, s2), weight(UP), preferred_element_type=F32), 0.0)
            for n, slot in enumerate((s1, s2)):
                v = pre[n * tokens:(n + 1) * tokens]
                RP[slot] = v
                ACT[slot] = (v * v).astype(BF)

        def pull_back(s1, s2):
            back = jnp.dot(both(C, s1, s2), weight(DN), preferred_element_type=F32)
            for n, slot in enumerate((s1, s2)):
                GP[slot] = (2.0 * RP[slot] * back[n * tokens:(n + 1) * tokens]).astype(BF)

        init(UP, 0)
        init(DN, 0)
        for name, src, dst in (("x", x_ref, X), ("c", cot_ref, C)):
            for i in (0, 1):
                rows = pl.ds(i * half, half)
                send((name, "z", i), src.at[rows], dst.at[2, rows], zpeer)
            send((name, "t"), src, dst.at[1], tpeer)
        for c in locals_:
            c.wait()
        turn(X, XT, 0)
        turn(C, CT, 0)
        recv(("a2a", UP))
        init(UP, 1)
        recv(("a2a", DN))
        init(DN, 1)
        near(UP, 0, 0)
        near(UP, 0, 1)
        near(UP, 1, 0)
        near(UP, 1, 1)
        near(DN, 0, 0)
        step2(UP, 0)
        near(DN, 0, 1)
        fwd(UP, 0, 0)
        near(DN, 1, 0)
        step2(UP, 1)
        fwd(UP, 1, 2)
        fwd(UP, 1, 0)
        near(DN, 1, 1)
        fwd(UP, 0, 1)
        pass_on("x", X, 0)
        arrived("x", 1)
        turn(X, XT, 1)
        fwd(UP, 0, 3)
        fwd(UP, 1, 1)
        fwd(UP, 1, 3)
        fwd(UP, 0, 2)
        step2(DN, 0)
        fwd(DN, 0, 0)
        fwd(DN, 0, 2)
        step2(DN, 1)
        pass_on("x", X, 1)
        arrived("c", 1)
        turn(C, CT, 1)
        fwd(DN, 1, 1)
        fwd(DN, 0, 1)
        turn(X, XT, 2)
        arrived("x", 3)
        turn(X, XT, 3)
        fin(UP)
        project(0, 1)
        fwd(DN, 1, 2)
        fwd(DN, 1, 0)
        project(2, 3)
        fwd(DN, 0, 3)
        fwd(DN, 1, 3)
        pass_on("c", C, 0)
        fin(DN)
        pull_back(0, 1)
        pass_on("c", C, 1)
        turn(C, CT, 2)
        arrived("c", 3)
        turn(C, CT, 3)

        lhs_of = (XT, CT)
        rhs_of = (GP, ACT)

        def gblk(w, h, a, b):
            z = j if h == 0 else 1 - j
            return G.at[w, z, a, b] if h == 0 else G.at[w, z, b, a]

        def raxes(h):
            return (y, x, ydev, xdev) if h == 0 else (x, y, xdev, ydev)

        def multiply(w, h):
            z = j if h == 0 else 1 - j
            rows = 4 * (width // 32)
            left = lhs_of[w][z].reshape(4 * rows, 4 * tokens)
            out = jnp.dot(left, rhs_of[w][...].reshape(4 * tokens, cols), preferred_element_type=F32)
            G[w, z] = out.reshape(4, 4, width // 32, cols)

        def encode(srcs, dst, scale, steps=3):
            top = None
            for src in srcs:
                for c in lanes:
                    m = jnp.max(jnp.abs(src[:, c]).reshape(-1, 8, 128), axis=0)
                    top = m if top is None else jnp.maximum(top, m)
            top = jnp.maximum(top, 2e-34)
            scale[...] = top
            inv = 2.0 ** (120 >> steps) / top
            for i, src in enumerate(srcs):
                for c in lanes:
                    v = src[:, c]
                    v3 = v.reshape(-1, 8, 128) * inv
                    for _ in range(steps):
                        v3 = v3 * jnp.abs(v3)
                    dst[i, :, c] = v3.reshape(v.shape).astype(BF)

        def decode(buf, scale, i, c, steps=3):
            v = buf[i, :, c].astype(F32)
            m = jnp.exp2(jnp.log2(jnp.abs(v)) * 0.5 ** steps)
            m = jnp.where(v < 0, -m, m).reshape(-1, 8, 128) * (scale[...] * 0.5 ** (120 >> steps))
            return m.reshape(v.shape)

        class Ring:
            def __init__(self, stage, w, h, pos, dev, parts, bufs):
                self.k = (stage, w, h)
                self.pos, self.dev, self.parts = pos, dev, parts
                self.sb, self.rb, self.sc, self.rc = (b.at[2 * w + h] for b in bufs)

            def post(self, i, srcs, d):
                encode(srcs, self.sb.at[i], self.sc.at[i])
                send(self.k + (i, "s"), self.sc.at[i], self.rc.at[i], self.dev(d))
                send(self.k + (i, "v"), self.sb.at[i], self.rb.at[i], self.dev(d))

            def take(self, i, refs):
                recv(self.k + (i, "s"))
                recv(self.k + (i, "v"))
                for n, ref in enumerate(refs):
                    for c in lanes:
                        ref[:, c] = ref[:, c] + decode(self.rb.at[i], self.rc.at[i], n, c)

            def far(self):
                self.post(0, self.parts(at(self.pos, 2), 0), 1)
                self.post(1, self.parts(at(self.pos, 2), 1), 3)

            def near_right(self):
                self.post(2, self.parts(at(self.pos, 1), 1), 1)

            def near_left(self):
                self.post(3, self.parts(at(self.pos, 3), 0), 3)

            def relay(self):
                p = self.parts(at(self.pos, 1), 0)
                self.take(0, p)
                self.post(4, p, 1)
                p = self.parts(at(self.pos, 3), 1)
                self.take(1, p)
                self.post(5, p, 3)

            def near_in(self):
                self.take(3, self.parts(self.pos, 0))
                self.take(2, self.parts(self.pos, 1))

            def last_in(self):
                self.take(4, self.parts(self.pos, 0))
                self.take(5, self.parts(self.pos, 1))

        def ring1(w, h):
            a, b, adev, bdev = raxes(h)
            return Ring(1, w, h, a, adev,
                        lambda place, side: [gblk(w, h, place, 2 * side + i) for i in (0, 1)],
                        (s1s, s1r, c1s, c1r))

        hr = width // 64

        def ring2(w, h):
            a, b, adev, bdev = raxes(h)
            return Ring(2, w, h, b, bdev,
                        lambda place, side: [gblk(w, h, a, place).at[pl.ds(side * hr, hr)]],
                        (s2s, s2r, c2s, c2r))

        first = {(w, h): ring1(w, h) for w in (UP, DN) for h in (0, 1)}
        second = {(w, h): ring2(w, h) for w in (UP, DN) for h in (0, 1)}

        def launch(w, h):
            multiply(w, h)
            first[w, h].far()
            first[w, h].near_right()
            first[w, h].near_left()

        def launch2(w):
            for h in (0, 1):
                first[w, h].near_in()
            for h in (0, 1):
                first[w, h].last_in()
                second[w, h].far()
                second[w, h].near_right()
                second[w, h].near_left()

        def relay2(w):
            for h in (0, 1):
                second[w, h].relay()

        def launch3(w):
            for h in (0, 1):
                second[w, h].near_in()
                second[w, h].last_in()
                a, b, _, _ = raxes(h)
                encode([gblk(w, h, a, b)], s3s.at[w, h], c3s.at[w, h])
                peers_ = [(0, rpeer)] if h == 0 else [(1, zpeer), (2, rzpeer)]
                for i, dev in peers_:
                    send((3, w, i, "s"), c3s.at[w, h], c3r.at[w, i], dev)
                    send((3, w, i, "v"), s3s.at[w, h], s3r.at[w, i], dev)

        def finish(w, out):
            for i in range(3):
                recv((3, w, i, "s"))
                recv((3, w, i, "v"))
            for c in range(len(lanes)):
                lane = lanes[c]
                mine = decode(s3s.at[w, 0], c3s.at[w, 0], 0, lane)
                mine = mine + decode(s3r.at[w, 0], c3r.at[w, 0], 0, lane)
                out[:, pl.ds(pl.multiple_of(j * cols + c * 128, 128), 128)] = mine * factor
                theirs = decode(s3r.at[w, 1], c3r.at[w, 1], 0, lane)
                theirs = theirs + decode(s3r.at[w, 2], c3r.at[w, 2], 0, lane)
                out[:, pl.ds(pl.multiple_of((1 - j) * cols + c * 128, 128), 128)] = theirs * factor

        def input_part(s1, s2):
            w = W[UP].reshape(width, cols)
            v = lax.dot_general(both(GP, s1, s2), w, (((1,), (1,)), ((), ())), preferred_element_type=F32)
            PART[s1] = v[:tokens]
            PART[s2] = v[tokens:]

        launch(DN, 0)
        launch(DN, 1)
        pull_back(2, 3)
        launch(UP, 0)
        for h in (0, 1):
            first[DN, h].relay()
        launch(UP, 1)
        input_part(3, 1)
        for n, slot in enumerate((3, 1)):
            send(("g", "t", n), PART.at[slot], DR.at[n], tpeer)
        input_part(2, 0)
        launch2(DN)
        recv(("g", "t", 0))
        PART[2] = PART[2] + DR[0]
        encode([PART.at[2]], ZS, zsc.at[0], 4)
        send(("g", "zs"), zsc.at[0], zsc.at[1], zpeer)
        send(("g", "z"), ZS, ZR, zpeer)
        for h in (0, 1):
            first[UP, h].relay()
        relay2(DN)
        launch2(UP)
        launch3(DN)
        relay2(UP)
        finish(DN, gdn_ref)

        EX[x] = jnp.sum(gdn_ref[...] * gdn_ref[...], axis=0, keepdims=True)
        for d in (1, 2, 3):
            send(("e", "x", d), EX.at[x], EX.at[x], xdev(d))
        launch3(UP)
        for d in (1, 2, 3):
            recv(("e", "x", d))
        EY[y] = EX[0] + EX[1] + EX[2] + EX[3]
        for d in (1, 2, 3):
            send(("e", "y", d), EY.at[y], EY.at[y], ydev(d))
        recv(("g", "t", 1))
        recv(("g", "zs"))
        recv(("g", "z"))
        for c in lanes:
            far = decode(ZR, zsc.at[1], 0, c, 4)
            gin_ref[:, c] = (PART[0, :, c] + DR[1, :, c] + far).astype(BF)
        for d in (1, 2, 3):
            recv(("e", "y", d))
        EZ[0] = EY[0] + EY[1] + EY[2] + EY[3]
        send(("e", "z"), EZ.at[0], EZ.at[1], zpeer)
        finish(UP, gup_ref)
        total = None
        for c in range(2 * len(lanes)):
            v = gup_ref[:, c * 128:(c + 1) * 128]
            total = v * v if total is None else total + v * v
        EU[0] = total
        send(("e", "t"), EU.at[0], EU.at[1], tpeer)
        recv(("e", "z"))
        edn_ref[...] = (EZ[0] + EZ[1]) * (1.0 / width)
        recv(("e", "t"))
        eup_ref[...] = jnp.sum((EU[0] + EU[1]).T, axis=0, keepdims=True) * (1.0 / ff)
        for c in copies.values():
            c.wait_send()

    return kernel


def hand_over(results):
    vm = pl.BlockSpec(memory_space=pltpu.VMEM)
    shapes = [jax.ShapeDtypeStruct(v.shape, v.dtype) for v in results]
    shapes[4] = jax.ShapeDtypeStruct(results[4].shape[1:], F32)

    def kernel(*refs):
        for src, dst in zip(refs[:4], refs[5:9]):
            dst[...] = src[...]
        refs[9][...] = refs[4][0]

    return pl.pallas_call(kernel, out_shape=tuple(shapes), in_specs=[vm] * 5, out_specs=(vm,) * 5)(*results)


def per_device(inputs, up_proj, down_proj, out_cotangent):
    tokens, width = inputs.shape
    rows, hidden = up_proj.shape
    cols = hidden // 2
    ff = hidden * lax.axis_size("tp")
    all_tokens = tokens * lax.axis_size("rep") * lax.axis_size(FS) * lax.axis_size("tp")
    factor = float(all_tokens) ** (-0.5)
    up3 = up_proj.reshape(2, rows // 2, hidden)
    dn3 = down_proj.T.reshape(2, rows // 2, hidden)
    vm = pl.BlockSpec(memory_space=pltpu.VMEM)
    full = (2, 4, 4, rows)
    results = pl.pallas_call(
        make_kernel(tokens, width, cols, ff, factor),
        out_shape=(
            jax.ShapeDtypeStruct((tokens, width), BF),
            jax.ShapeDtypeStruct((rows, hidden), F32),
            jax.ShapeDtypeStruct((rows, hidden), F32),
            jax.ShapeDtypeStruct((1, rows), F32),
            jax.ShapeDtypeStruct((1, hidden), F32),
        ),
        in_specs=[vm] * 4,
        out_specs=(vm,) * 5,
        scratch_shapes=[
            pltpu.VMEM((4, tokens, width), BF),
            pltpu.VMEM((4, tokens, width), BF),
            pltpu.VMEM(full + (4 * tokens,), BF),
            pltpu.VMEM(full + (4 * tokens,), BF),
            pltpu.VMEM((2, 2, 4, 4, 2, rows // 2, cols), BF),
            pltpu.VMEM((4, tokens, cols), F32),
            pltpu.VMEM((4, tokens, cols), BF),
            pltpu.VMEM((4, tokens, cols), BF),
            pltpu.VMEM((2,) + full + (cols,), F32),
            pltpu.VMEM((4, 6, 2, rows, cols), BF),
            pltpu.VMEM((4, 6, 2, rows, cols), BF),
            pltpu.VMEM((4, 6, 8, 128), F32),
            pltpu.VMEM((4, 6, 8, 128), F32),
            pltpu.VMEM((4, 6, 1, rows // 2, cols), BF),
            pltpu.VMEM((4, 6, 1, rows // 2, cols), BF),
            pltpu.VMEM((4, 6, 8, 128), F32),
            pltpu.VMEM((4, 6, 8, 128), F32),
            pltpu.VMEM((2, 2, 1, rows, cols), BF),
            pltpu.VMEM((2, 3, 1, rows, cols), BF),
            pltpu.VMEM((2, 2, 8, 128), F32),
            pltpu.VMEM((2, 3, 8, 128), F32),
            pltpu.VMEM((4, tokens, width), F32),
            pltpu.VMEM((2, tokens, width), F32),
            pltpu.VMEM((1, tokens, width), BF),
            pltpu.VMEM((1, tokens, width), BF),
            pltpu.VMEM((2, 8, 128), F32),
            pltpu.VMEM((4, 1, hidden), F32),
            pltpu.VMEM((4, 1, hidden), F32),
            pltpu.VMEM((2, 1, hidden), F32),
            pltpu.VMEM((2, rows, 128), F32),
            pltpu.SemaphoreType.DMA((COPIES,)),
            pltpu.SemaphoreType.DMA((COPIES,)),
            pltpu.SemaphoreType.DMA((4,)),
        ],
        compiler_params=pltpu.CompilerParams(
            collective_id=0, has_side_effects=True, vmem_limit_bytes=63 * 1024 * 1024
        ),
    )(inputs, up3, dn3, out_cotangent)
    gin, gup, gdn, eup, edn = hand_over(results)
    return gin, gup, gdn.T, eup.reshape(rows), edn


def solution(mesh):
    torus = Mesh(
        mesh.devices.reshape(mesh.shape["rep"], 2, 4, 4, mesh.shape["tp"]),
        ("rep", "fs_0", "fs_1", "fs_2", "tp"),
    )
    placed = (P(REP_FS_TP, None), P(FS, "tp"), P("tp", FS), P(REP_FS_TP, None))
    return jax.shard_map(
        per_device,
        mesh=torus,
        in_specs=placed,
        out_specs=(P(REP_FS_TP, None), P(FS, "tp"), P("tp", FS), P(FS), P("tp")),
        check_vma=False,
    )
```

```python
import jax
import jax.numpy as jnp
from jax import lax
from jax.experimental import pallas as pl
from jax.experimental.pallas import tpu as pltpu
from jax.sharding import Mesh
from jax.sharding import PartitionSpec as P

FS = ("fs_0", "fs_1", "fs_2")
REP_FS_TP = ("rep", "fs_0", "fs_1", "fs_2", "tp")
MESH = pl.DeviceIdType.MESH
BF = jnp.bfloat16
F32 = jnp.float32
RIGHT, LEFT = 0, 1
UP, DN = 0, 1
COPIES = 240


ORDER = [
    ("init", 1, 0), ("init", 0, 0), ("init", 0, 1), ("near", 1, 0, 0), ("init", 1, 1), ("near", 0, 0, 1),
    ("near", 0, 0, 0), ("near", 0, 1, 0), ("near", 0, 1, 1), ("fwd", 0, 0, 0, 1), ("near", 1, 1, 1),
    ("step2", 0, 0), ("near", 1, 1, 0), ("fwd", 0, 0, 0, 0), ("pass", "x", 1), ("near", 1, 0, 1),
    ("fwd", 0, 0, 1, 0), ("fwd", 0, 1, 1, 0), ("fwd", 0, 1, 2, 1), ("fwd", 0, 0, 1, 1), ("fwd", 0, 1, 0, 1),
    ("turn", "x", 0), ("step2", 0, 1), ("fwd", 0, 0, 2, 0), ("fwd", 0, 0, 2, 1), ("fwd", 1, 1, 2, 0),
    ("fwd", 0, 1, 0, 0), ("fwd", 0, 1, 2, 0), ("turn", "c", 1), ("fwd", 1, 1, 1, 1), ("fwd", 0, 1, 1, 1),
    ("fwd", 1, 0, 1, 0), ("pass", "x", 0), ("fwd", 0, 1, 3, 0), ("step2", 1, 1), ("fwd", 0, 0, 3, 1),
    ("turn", "x", 2), ("fwd", 1, 1, 1, 0), ("step2", 1, 0), ("fwd", 1, 0, 2, 1), ("fwd", 0, 0, 3, 0),
    ("fwd", 1, 1, 0, 0), ("fwd", 0, 1, 3, 1), ("turn", "x", 1), ("fwd", 1, 0, 3, 0), ("fwd", 1, 0, 2, 0),
    ("fwd", 1, 0, 3, 1), ("fwd", 1, 1, 3, 0), ("pass", "c", 0), ("fwd", 1, 1, 2, 1), ("proj", 0),
    ("fwd", 1, 0, 1, 1), ("fwd", 1, 1, 3, 1), ("pass", "c", 1), ("turn", "c", 2), ("turn", "x", 3), ("proj", 1),
    ("fwd", 1, 0, 0, 1), ("turn", "c", 0), ("fwd", 1, 1, 0, 1), ("fwd", 1, 0, 0, 0), ("turn", "c", 3),
    ("mult", 1, 1), ("mult", 1, 0), ("far", 1, 0), ("far", 1, 1), ("nr", 1, 0), ("nr", 1, 1), ("nl", 1, 1),
    ("pull", 1), ("pull", 0), ("nl", 1, 0), ("ip", 0), ("mult", 0, 1), ("far", 0, 1), ("rl", 1, 0, 0),
    ("rl", 1, 0, 1), ("rl", 1, 1, 1), ("ip", 1), ("rl", 1, 1, 0), ("mult", 0, 0), ("far", 0, 0), ("ni", 1, 0),
    ("gz",), ("st2", 1, 0), ("nl", 0, 1), ("nl", 0, 0), ("nr", 0, 0), ("rl", 0, 1, 0), ("ni", 1, 1),
    ("st2", 1, 1), ("rl2", 1, 0, 1), ("rl", 0, 0, 1), ("rl2", 1, 0, 0), ("rl", 0, 0, 0), ("ni", 0, 0),
    ("rl", 0, 1, 1), ("st3", 1, 0), ("nr", 0, 1), ("rl2", 1, 1, 0), ("rl2", 1, 1, 1), ("st2", 0, 0),
    ("st3", 1, 1), ("gin",), ("ni", 0, 1), ("st2", 0, 1), ("rl2", 0, 0, 1), ("rl2", 0, 0, 0), ("fin", 1), ("ex",),
    ("rl2", 0, 1, 0), ("rl2", 0, 1, 1), ("st3", 0, 0), ("ey",), ("st3", 0, 1), ("ez",), ("fin", 0), ("eu",),
    ("eup",), ("edn",),
]


def make_kernel(tokens, width, cols, ff, factor):
    lanes = [pl.ds(c * 128, 128) for c in range(cols // 128)]

    def kernel(
        x_ref, up_ref, dn_ref, cot_ref,
        gin_ref, gup_ref, gdn_ref, eup_ref, edn_ref,
        X, C, XT, CT, W, RP, ACT, GP, G,
        s1s, s1r, c1s, c1r, s2s, s2r, c2s, c2r, s3s, s3r, c3s, c3r,
        PART, DR, ZS, ZR, zsc, EX, EY, EZ, EU,
        OTH, ssem, rsem, lsem,
    ):
        r = lax.axis_index("rep")
        j = lax.axis_index("fs_0")
        y = lax.axis_index("fs_1")
        x = lax.axis_index("fs_2")
        t = lax.axis_index("tp")

        def at(pos, d):
            return lax.rem(pos + d, 4)

        def xdev(d):
            return {"fs_2": at(x, d)}

        def ydev(d):
            return {"fs_1": at(y, d)}

        zpeer = {"fs_0": 1 - j}
        rpeer = {"rep": 1 - r}
        rzpeer = {"rep": 1 - r, "fs_0": 1 - j}
        tpeer = {"tp": 1 - t}

        own = pl.ds(pl.multiple_of(j * cols, cols), cols)
        other = pl.ds(pl.multiple_of((1 - j) * cols, cols), cols)
        loads = [
            pltpu.make_async_copy(up_ref.at[:, :, other], OTH.at[UP], lsem.at[0]),
            pltpu.make_async_copy(dn_ref.at[:, :, other], OTH.at[DN], lsem.at[1]),
            pltpu.make_async_copy(up_ref.at[:, :, own], W.at[UP, j, y, x], lsem.at[2]),
            pltpu.make_async_copy(dn_ref.at[:, :, own], W.at[DN, j, y, x], lsem.at[3]),
            pltpu.make_async_copy(x_ref, X.at[0], lsem.at[4]),
            pltpu.make_async_copy(cot_ref, C.at[0], lsem.at[5]),
        ]
        for c in loads:
            c.start()

        barrier = pltpu.get_barrier_semaphore()
        peers = [xdev(1), xdev(2), xdev(3), ydev(1), ydev(2), ydev(3), zpeer, rpeer, rzpeer, tpeer]
        for dev in peers:
            pl.semaphore_signal(barrier, inc=1, device_id=dev, device_id_type=MESH)
        pl.semaphore_wait(barrier, len(peers))

        copies = {}

        def send(key, src, dst, dev):
            n = len(copies)
            c = pltpu.make_async_remote_copy(
                src_ref=src, dst_ref=dst, send_sem=ssem.at[n], recv_sem=rsem.at[n],
                device_id=dev, device_id_type=MESH,
            )
            c.start()
            copies[key] = c

        def recv(key):
            copies[key].wait_recv()

        half = tokens // 2

        def blk(ref, w, h, a, b):
            z = j if h == 0 else 1 - j
            return ref.at[w, z, b, a] if h == 0 else ref.at[w, z, a, b]

        def axes(h):
            return (x, y, xdev, ydev) if h == 0 else (y, x, ydev, xdev)

        def init(w, h):
            a, b, adev, bdev = axes(h)
            if h == 1:
                recv(("a2a", w))
            src = dst = blk(W, w, h, a, b)
            send((1, w, h, 0), src, dst, adev(1))
            send((1, w, h, 1), src, dst, adev(3))
            send((2, w, h, 0, 0), src, dst, bdev(1))
            send((2, w, h, 0, 1), src, dst, bdev(3))

        def spread(w, h, s, a2):
            _, b, _, bdev = axes(h)
            ref = blk(W, w, h, a2, b)
            send((2, w, h, s, 0), ref, ref, bdev(1))
            send((2, w, h, s, 1), ref, ref, bdev(3))

        def near(w, h, side):
            a, b, adev, _ = axes(h)
            recv((1, w, h, side))
            place, away = ((at(a, 3), 1), (at(a, 1), 3))[side]
            ref = blk(W, w, h, place, b).at[side]
            send((1, w, h, 2 + side), ref, ref, adev(away))
            spread(w, h, 1 + side, place)

        def step2(w, h):
            a = axes(h)[0]
            recv((1, w, h, 2))
            recv((1, w, h, 3))
            spread(w, h, 3, at(a, 2))

        def fwd(w, h, s, side):
            a, b, _, bdev = axes(h)
            a2 = at(a, (0, 3, 1, 2)[s])
            recv((2, w, h, s, side))
            place, away = ((at(b, 3), 1), (at(b, 1), 3))[side]
            ref = blk(W, w, h, a2, place).at[side]
            send((2, w, h, s, 2 + side), ref, ref, bdev(away))

        whole = set()

        def fin(w):
            if w in whole:
                return
            whole.add(w)
            for h in (0, 1):
                for s in range(4):
                    recv((2, w, h, s, 2))
                    recv((2, w, h, s, 3))

        stock = {"x": (X, XT), "c": (C, CT)}

        def pass_on(name, i):
            recv((name, "z", i))
            rows = pl.ds(i * half, half)
            buf = stock[name][0]
            send((name, "zt", i), buf.at[2, rows], buf.at[3, rows], tpeer)

        def turn(name, slot):
            if slot == 1:
                recv((name, "t"))
            if slot == 3:
                recv((name, "zt", 0))
                recv((name, "zt", 1))
            src, dst = stock[name]
            v = src[slot].T
            dst[:, :, :, :, slot * tokens:(slot + 1) * tokens] = v.reshape(2, 4, 4, width // 32, tokens)

        def weight(w):
            return W[w].reshape(width, cols)

        def both(ref, s1, s2):
            return jnp.concatenate([ref[s1], ref[s2]], axis=0)

        def project(n):
            s1, s2 = 2 * n, 2 * n + 1
            fin(UP)
            pre = jnp.maximum(jnp.dot(both(X, s1, s2), weight(UP), preferred_element_type=F32), 0.0)
            for n, slot in enumerate((s1, s2)):
                v = pre[n * tokens:(n + 1) * tokens]
                RP[slot] = v
                ACT[slot] = (v * v).astype(BF)

        def pull_back(n):
            s1, s2 = 2 * n, 2 * n + 1
            fin(DN)
            back = jnp.dot(both(C, s1, s2), weight(DN), preferred_element_type=F32)
            for n, slot in enumerate((s1, s2)):
                GP[slot] = (2.0 * RP[slot] * back[n * tokens:(n + 1) * tokens]).astype(BF)

        lhs_of = (XT, CT)
        rhs_of = (GP, ACT)

        def gblk(w, h, a, b):
            z = j if h == 0 else 1 - j
            return G.at[w, z, a, b] if h == 0 else G.at[w, z, b, a]

        def raxes(h):
            return (y, x, ydev, xdev) if h == 0 else (x, y, xdev, ydev)

        def multiply(w, h):
            z = j if h == 0 else 1 - j
            rows = 4 * (width // 32)
            left = lhs_of[w][z].reshape(4 * rows, 4 * tokens)
            out = jnp.dot(left, rhs_of[w][...].reshape(4 * tokens, cols), preferred_element_type=F32)
            G[w, z] = out.reshape(4, 4, width // 32, cols)

        def encode(srcs, dst, scale, steps=3):
            top = None
            for src in srcs:
                for c in lanes:
                    m = jnp.max(jnp.abs(src[:, c]).reshape(-1, 8, 128), axis=0)
                    top = m if top is None else jnp.maximum(top, m)
            top = jnp.maximum(top, 2e-34)
            scale[...] = top
            inv = 2.0 ** (120 >> steps) / top
            for i, src in enumerate(srcs):
                for c in lanes:
                    v = src[:, c]
                    v3 = v.reshape(-1, 8, 128) * inv
                    for _ in range(steps):
                        v3 = v3 * jnp.abs(v3)
                    dst[i, :, c] = v3.reshape(v.shape).astype(BF)

        def decode(buf, scale, i, c, steps=3):
            v = buf[i, :, c].astype(F32)
            m = jnp.exp2(jnp.log2(jnp.abs(v)) * 0.5 ** steps)
            m = jnp.where(v < 0, -m, m).reshape(-1, 8, 128) * (scale[...] * 0.5 ** (120 >> steps))
            return m.reshape(v.shape)

        class Ring:
            def __init__(self, stage, w, h, pos, dev, parts, bufs):
                self.k = (stage, w, h)
                self.pos, self.dev, self.parts = pos, dev, parts
                self.sb, self.rb, self.sc, self.rc = (b.at[2 * w + h] for b in bufs)

            def post(self, i, srcs, d):
                encode(srcs, self.sb.at[i], self.sc.at[i])
                send(self.k + (i, "s"), self.sc.at[i], self.rc.at[i], self.dev(d))
                send(self.k + (i, "v"), self.sb.at[i], self.rb.at[i], self.dev(d))

            def take(self, i, refs):
                recv(self.k + (i, "s"))
                recv(self.k + (i, "v"))
                for n, ref in enumerate(refs):
                    for c in lanes:
                        ref[:, c] = ref[:, c] + decode(self.rb.at[i], self.rc.at[i], n, c)

            def far(self):
                self.post(0, self.parts(at(self.pos, 2), 0), 1)
                self.post(1, self.parts(at(self.pos, 2), 1), 3)

            def near_right(self):
                self.post(2, self.parts(at(self.pos, 1), 1), 1)

            def near_left(self):
                self.post(3, self.parts(at(self.pos, 3), 0), 3)

            def relay(self, side):
                p = self.parts(at(self.pos, (1, 3)[side]), side)
                self.take(side, p)
                self.post(4 + side, p, (1, 3)[side])

            def near_in(self):
                self.take(3, self.parts(self.pos, 0))
                self.take(2, self.parts(self.pos, 1))

            def last_in(self):
                self.take(4, self.parts(self.pos, 0))
                self.take(5, self.parts(self.pos, 1))

        def ring1(w, h):
            a, b, adev, bdev = raxes(h)
            return Ring(1, w, h, a, adev,
                        lambda place, side: [gblk(w, h, place, 2 * side + i) for i in (0, 1)],
                        (s1s, s1r, c1s, c1r))

        hr = width // 64

        def ring2(w, h):
            a, b, adev, bdev = raxes(h)
            return Ring(2, w, h, b, bdev,
                        lambda place, side: [gblk(w, h, a, place).at[pl.ds(side * hr, hr)]],
                        (s2s, s2r, c2s, c2r))

        first = {(w, h): ring1(w, h) for w in (UP, DN) for h in (0, 1)}
        second = {(w, h): ring2(w, h) for w in (UP, DN) for h in (0, 1)}

        def second_start(w, h):
            first[w, h].last_in()
            second[w, h].far()
            second[w, h].near_right()
            second[w, h].near_left()

        def third_start(w, h):
            second[w, h].near_in()
            second[w, h].last_in()
            a, b, _, _ = raxes(h)
            encode([gblk(w, h, a, b)], s3s.at[w, h], c3s.at[w, h])
            peers_ = [(0, rpeer)] if h == 0 else [(1, zpeer), (2, rzpeer)]
            for i, dev in peers_:
                send((3, w, i, "s"), c3s.at[w, h], c3r.at[w, i], dev)
                send((3, w, i, "v"), s3s.at[w, h], s3r.at[w, i], dev)

        def finish(w):
            out = (gup_ref, gdn_ref)[w]
            for i in range(3):
                recv((3, w, i, "s"))
                recv((3, w, i, "v"))
            for c in range(len(lanes)):
                lane = lanes[c]
                mine = decode(s3s.at[w, 0], c3s.at[w, 0], 0, lane)
                mine = mine + decode(s3r.at[w, 0], c3r.at[w, 0], 0, lane)
                out[:, pl.ds(pl.multiple_of(j * cols + c * 128, 128), 128)] = mine * factor
                theirs = decode(s3r.at[w, 1], c3r.at[w, 1], 0, lane)
                theirs = theirs + decode(s3r.at[w, 2], c3r.at[w, 2], 0, lane)
                out[:, pl.ds(pl.multiple_of((1 - j) * cols + c * 128, 128), 128)] = theirs * factor

        def input_part(n):
            s1, s2 = ((3, 1), (2, 0))[n]
            w = W[UP].reshape(width, cols)
            v = lax.dot_general(both(GP, s1, s2), w, (((1,), (1,)), ((), ())), preferred_element_type=F32)
            PART[s1] = v[:tokens]
            PART[s2] = v[tokens:]
            if n == 0:
                for i, slot in enumerate((3, 1)):
                    send(("g", "t", i), PART.at[slot], DR.at[i], tpeer)

        def input_send():
            recv(("g", "t", 0))
            PART[2] = PART[2] + DR[0]
            encode([PART.at[2]], ZS, zsc.at[0], 4)
            send(("g", "zs"), zsc.at[0], zsc.at[1], zpeer)
            send(("g", "z"), ZS, ZR, zpeer)

        def input_sum():
            recv(("g", "t", 1))
            recv(("g", "zs"))
            recv(("g", "z"))
            for c in lanes:
                far = decode(ZR, zsc.at[1], 0, c, 4)
                gin_ref[:, c] = (PART[0, :, c] + DR[1, :, c] + far).astype(BF)

        def energy_x():
            EX[x] = jnp.sum(gdn_ref[...] * gdn_ref[...], axis=0, keepdims=True)
            for d in (1, 2, 3):
                send(("e", "x", d), EX.at[x], EX.at[x], xdev(d))

        def energy_y():
            for d in (1, 2, 3):
                recv(("e", "x", d))
            EY[y] = EX[0] + EX[1] + EX[2] + EX[3]
            for d in (1, 2, 3):
                send(("e", "y", d), EY.at[y], EY.at[y], ydev(d))

        def energy_z():
            for d in (1, 2, 3):
                recv(("e", "y", d))
            EZ[0] = EY[0] + EY[1] + EY[2] + EY[3]
            send(("e", "z"), EZ.at[0], EZ.at[1], zpeer)

        def energy_down():
            recv(("e", "z"))
            edn_ref[...] = (EZ[0] + EZ[1]) * (1.0 / width)

        def energy_pair():
            total = None
            for c in range(2 * len(lanes)):
                v = gup_ref[:, c * 128:(c + 1) * 128]
                total = v * v if total is None else total + v * v
            EU[0] = total
            send(("e", "t"), EU.at[0], EU.at[1], tpeer)

        def energy_up():
            recv(("e", "t"))
            eup_ref[...] = jnp.sum((EU[0] + EU[1]).T, axis=0, keepdims=True) * (1.0 / ff)

        loads[0].wait()
        send(("a2a", UP), OTH.at[UP], W.at[UP, j, y, x], rzpeer)
        loads[1].wait()
        send(("a2a", DN), OTH.at[DN], W.at[DN, j, y, x], rzpeer)
        for c in loads[2:]:
            c.wait()
        for name in ("x", "c"):
            buf = stock[name][0]
            for i in (0, 1):
                rows = pl.ds(i * half, half)
                send((name, "z", i), buf.at[0, rows], buf.at[2, rows], zpeer)
            send((name, "t"), buf.at[0], buf.at[1], tpeer)
        todo = {
            "init": init, "near": near, "step2": step2, "fwd": fwd, "pass": pass_on, "turn": turn,
            "proj": project, "pull": pull_back, "mult": multiply,
            "far": lambda w, h: first[w, h].far(),
            "nr": lambda w, h: first[w, h].near_right(),
            "nl": lambda w, h: first[w, h].near_left(),
            "rl": lambda w, h, side: first[w, h].relay(side),
            "ni": lambda w, h: first[w, h].near_in(),
            "st2": second_start,
            "rl2": lambda w, h, side: second[w, h].relay(side),
            "st3": third_start, "fin": finish, "ip": input_part, "gz": input_send, "gin": input_sum,
            "ex": energy_x, "ey": energy_y, "ez": energy_z, "edn": energy_down,
            "eu": energy_pair, "eup": energy_up,
        }
        for name, *where in ORDER:
            todo[name](*where)
        for c in copies.values():
            c.wait_send()

    return kernel


def hand_over(results):
    vm = pl.BlockSpec(memory_space=pltpu.VMEM)
    shapes = [jax.ShapeDtypeStruct(v.shape, v.dtype) for v in results]
    shapes[4] = jax.ShapeDtypeStruct(results[4].shape[1:], F32)

    def kernel(*refs):
        for src, dst in zip(refs[:4], refs[5:9]):
            dst[...] = src[...]
        refs[9][...] = refs[4][0]

    return pl.pallas_call(kernel, out_shape=tuple(shapes), in_specs=[vm] * 5, out_specs=(vm,) * 5)(*results)


def per_device(inputs, up_proj, down_proj, out_cotangent):
    tokens, width = inputs.shape
    rows, hidden = up_proj.shape
    cols = hidden // 2
    ff = hidden * lax.axis_size("tp")
    all_tokens = tokens * lax.axis_size("rep") * lax.axis_size(FS) * lax.axis_size("tp")
    factor = float(all_tokens) ** (-0.5)
    up3 = up_proj.reshape(2, rows // 2, hidden)
    dn3 = down_proj.T.reshape(2, rows // 2, hidden)
    vm = pl.BlockSpec(memory_space=pltpu.VMEM)
    full = (2, 4, 4, rows)
    results = pl.pallas_call(
        make_kernel(tokens, width, cols, ff, factor),
        out_shape=(
            jax.ShapeDtypeStruct((tokens, width), BF),
            jax.ShapeDtypeStruct((rows, hidden), F32),
            jax.ShapeDtypeStruct((rows, hidden), F32),
            jax.ShapeDtypeStruct((1, rows), F32),
            jax.ShapeDtypeStruct((1, hidden), F32),
        ),
        in_specs=[pl.BlockSpec(memory_space=pl.ANY)] * 4,
        out_specs=(vm,) * 5,
        scratch_shapes=[
            pltpu.VMEM((4, tokens, width), BF),
            pltpu.VMEM((4, tokens, width), BF),
            pltpu.VMEM(full + (4 * tokens,), BF),
            pltpu.VMEM(full + (4 * tokens,), BF),
            pltpu.VMEM((2, 2, 4, 4, 2, rows // 2, cols), BF),
            pltpu.VMEM((4, tokens, cols), F32),
            pltpu.VMEM((4, tokens, cols), BF),
            pltpu.VMEM((4, tokens, cols), BF),
            pltpu.VMEM((2,) + full + (cols,), F32),
            pltpu.VMEM((4, 6, 2, rows, cols), BF),
            pltpu.VMEM((4, 6, 2, rows, cols), BF),
            pltpu.VMEM((4, 6, 8, 128), F32),
            pltpu.VMEM((4, 6, 8, 128), F32),
            pltpu.VMEM((4, 6, 1, rows // 2, cols), BF),
            pltpu.VMEM((4, 6, 1, rows // 2, cols), BF),
            pltpu.VMEM((4, 6, 8, 128), F32),
            pltpu.VMEM((4, 6, 8, 128), F32),
            pltpu.VMEM((2, 2, 1, rows, cols), BF),
            pltpu.VMEM((2, 3, 1, rows, cols), BF),
            pltpu.VMEM((2, 2, 8, 128), F32),
            pltpu.VMEM((2, 3, 8, 128), F32),
            pltpu.VMEM((4, tokens, width), F32),
            pltpu.VMEM((2, tokens, width), F32),
            pltpu.VMEM((1, tokens, width), BF),
            pltpu.VMEM((1, tokens, width), BF),
            pltpu.VMEM((2, 8, 128), F32),
            pltpu.VMEM((4, 1, hidden), F32),
            pltpu.VMEM((4, 1, hidden), F32),
            pltpu.VMEM((2, 1, hidden), F32),
            pltpu.VMEM((2, rows, 128), F32),
            pltpu.VMEM((2, 2, rows // 2, cols), BF),
            pltpu.SemaphoreType.DMA((COPIES,)),
            pltpu.SemaphoreType.DMA((COPIES,)),
            pltpu.SemaphoreType.DMA((6,)),
        ],
        compiler_params=pltpu.CompilerParams(
            collective_id=0, has_side_effects=True, vmem_limit_bytes=63 * 1024 * 1024
        ),
    )(inputs, up3, dn3, out_cotangent)
    gin, gup, gdn, eup, edn = hand_over(results)
    return gin, gup, gdn.T, eup.reshape(rows), edn


def solution(mesh):
    torus = Mesh(
        mesh.devices.reshape(mesh.shape["rep"], 2, 4, 4, mesh.shape["tp"]),
        ("rep", "fs_0", "fs_1", "fs_2", "tp"),
    )
    placed = (P(REP_FS_TP, None), P(FS, "tp"), P("tp", FS), P(REP_FS_TP, None))
    return jax.shard_map(
        per_device,
        mesh=torus,
        in_specs=placed,
        out_specs=(P(REP_FS_TP, None), P(FS, "tp"), P("tp", FS), P(FS), P("tp")),
        check_vma=False,
    )
```

```python
import jax
import jax.numpy as jnp
from jax import lax
from jax.experimental import pallas as pl
from jax.experimental.pallas import tpu as pltpu
from jax.sharding import Mesh
from jax.sharding import PartitionSpec as P

FS = ("fs_0", "fs_1", "fs_2")
REP_FS_TP = ("rep", "fs_0", "fs_1", "fs_2", "tp")
MESH = pl.DeviceIdType.MESH
BF = jnp.bfloat16
F32 = jnp.float32
RIGHT, LEFT = 0, 1
UP, DN = 0, 1
COPIES = 280
LAG = 30


ORDER = [
    ("init", 0, 0), ("init", 1, 0), ("turn", "x", 1), ("init", 0, 1), ("init", 1, 1), ("near", 0, 1, 0),
    ("turn", "c", 1), ("fwd", 0, 0, 0, 0), ("near", 0, 1, 1), ("near", 0, 0, 0), ("near", 1, 0, 1),
    ("fwd", 0, 0, 0, 1), ("near", 0, 0, 1), ("step2", 0, 1), ("near", 1, 1, 0), ("near", 1, 1, 1),
    ("near", 1, 0, 0), ("pass", "x", 0), ("fwd", 0, 1, 0, 0), ("fwd", 0, 1, 0, 1), ("pass", "x", 1),
    ("step2", 0, 0), ("fwd", 0, 1, 3, 0), ("fwd", 0, 1, 3, 1), ("fwd", 0, 1, 1, 0), ("turn", "x", 3),
    ("fwd", 1, 0, 0, 1), ("fwd", 0, 0, 1, 1), ("turn", "x", 0), ("fwd", 1, 1, 0, 0), ("fwd", 0, 0, 2, 0),
    ("fwd", 0, 1, 1, 1), ("turn", "c", 0), ("fwd", 0, 1, 2, 1), ("fwd", 0, 1, 2, 0), ("fwd", 1, 0, 2, 1),
    ("fwd", 0, 0, 1, 0), ("step2", 1, 1), ("fwd", 1, 1, 2, 1), ("fwd", 1, 1, 0, 1), ("fwd", 1, 1, 1, 0),
    ("fwd", 0, 0, 3, 0), ("fwd", 0, 0, 2, 1), ("fwd", 1, 1, 1, 1), ("fwd", 0, 0, 3, 1), ("turn", "x", 2),
    ("pass", "c", 0), ("step2", 1, 0), ("proj", 0), ("fwd", 1, 0, 0, 0), ("fwd", 1, 0, 2, 0), ("fwd", 1, 0, 1, 1),
    ("fwd", 1, 0, 3, 0), ("pass", "c", 1), ("ma", 1, 1), ("fwd", 1, 1, 3, 0), ("fwd", 1, 1, 3, 1),
    ("fwd", 1, 0, 1, 0), ("fwd", 1, 0, 3, 1), ("proj", 1), ("fwd", 1, 1, 2, 0), ("turn", "c", 2),
    ("turn", "c", 3), ("mult", 1, 0), ("mult", 1, 1), ("far", 1, 1, 1), ("far", 1, 0, 0), ("nl", 1, 0),
    ("far", 1, 1, 0), ("nr", 1, 1), ("far", 1, 0, 1), ("pull", 1), ("pull", 0), ("nr", 1, 0), ("nl", 1, 1),
    ("ip", 0), ("mult", 0, 0), ("rl", 1, 0, 0, 0), ("rl", 1, 1, 1, 1), ("rl", 1, 1, 0, 1), ("rl", 1, 0, 1, 0),
    ("rl", 1, 1, 0, 0), ("far", 0, 0, 0), ("rl", 1, 1, 1, 0), ("far", 0, 0, 1), ("rl", 1, 0, 0, 1),
    ("mult", 0, 1), ("far", 0, 1, 0), ("ip", 1), ("gz",), ("nr", 0, 1), ("nl", 0, 1), ("rl", 1, 0, 1, 1),
    ("ni", 1, 1), ("rl", 0, 0, 0, 0), ("rl", 0, 0, 1, 0), ("far", 0, 1, 1), ("ni", 1, 0), ("nl", 0, 0),
    ("st2", 1, 1), ("nr", 0, 0), ("rl", 0, 0, 1, 1), ("rl", 0, 0, 0, 1), ("st2", 1, 0), ("ni", 0, 1),
    ("rl2", 1, 0, 1), ("rl2", 1, 0, 0), ("rl", 0, 1, 1, 1), ("rl", 0, 1, 0, 0), ("rl2", 1, 1, 1),
    ("rl", 0, 1, 0, 1), ("rl2", 1, 1, 0), ("rl", 0, 1, 1, 0), ("ni", 0, 0), ("st3", 1, 0), ("st2", 0, 0),
    ("st3", 1, 1), ("st2", 0, 1), ("rl2", 0, 0, 0), ("rl2", 0, 0, 1), ("rl2", 0, 1, 1), ("rl2", 0, 1, 0),
    ("st3", 0, 0), ("fin", 1), ("ex",), ("st3", 0, 1), ("ey",), ("fin", 0), ("eu",), ("gin",), ("eup",), ("edn",),
]


def make_kernel(tokens, width, cols, ff, factor):
    lanes = [pl.ds(c * 128, 128) for c in range(cols // 128)]

    def kernel(
        x_ref, up_ref, dn_ref, cot_ref,
        gin_out, gup_out, gdn_out, eup_ref, edn_ref,
        X, C, XT, CT, W, RP, ACT, GP, G,
        s1s, s1r, c1s, c1r, s2s, s2r, c2s, c2r, s3s, s3r, c3s, c3r,
        PART, DR, ZS, ZR, zsc, EX, EY, EU,
        OTH, gin_ref, gup_ref, gdn_ref, ssem, rsem, lsem,
    ):
        r = lax.axis_index("rep")
        j = lax.axis_index("fs_0")
        y = lax.axis_index("fs_1")
        x = lax.axis_index("fs_2")
        t = lax.axis_index("tp")

        def at(pos, d):
            return lax.rem(pos + d, 4)

        def xdev(d):
            return {"fs_2": at(x, d)}

        def ydev(d):
            return {"fs_1": at(y, d)}

        def yzdev(d):
            return {"fs_0": 1 - j, "fs_1": at(y, d)}

        zpeer = {"fs_0": 1 - j}
        rpeer = {"rep": 1 - r}
        rzpeer = {"rep": 1 - r, "fs_0": 1 - j}
        tpeer = {"tp": 1 - t}

        own = pl.ds(pl.multiple_of(j * cols, cols), cols)
        other = pl.ds(pl.multiple_of((1 - j) * cols, cols), cols)
        loads = [
            pltpu.make_async_copy(up_ref.at[:, :, other], OTH.at[UP], lsem.at[0]),
            pltpu.make_async_copy(dn_ref.at[:, :, other], OTH.at[DN], lsem.at[1]),
            pltpu.make_async_copy(up_ref.at[:, :, own], W.at[UP, j, y, x], lsem.at[2]),
            pltpu.make_async_copy(dn_ref.at[:, :, own], W.at[DN, j, y, x], lsem.at[3]),
            pltpu.make_async_copy(x_ref, X.at[0], lsem.at[4]),
            pltpu.make_async_copy(cot_ref, C.at[0], lsem.at[5]),
        ]
        for c in loads:
            c.start()

        barrier = pltpu.get_barrier_semaphore()
        peers = [xdev(1), xdev(2), xdev(3), ydev(1), ydev(2), ydev(3), zpeer, rpeer, rzpeer, tpeer, yzdev(1), yzdev(2), yzdev(3)]
        for dev in peers:
            pl.semaphore_signal(barrier, inc=1, device_id=dev, device_id_type=MESH)
        pl.semaphore_wait(barrier, len(peers))

        copies = {}
        stores = []

        def store(src, dst):
            c = pltpu.make_async_copy(src, dst, lsem.at[6 + len(stores)])
            c.start()
            stores.append(c)

        def send(key, src, dst, dev):
            n = len(copies)
            c = pltpu.make_async_remote_copy(
                src_ref=src, dst_ref=dst, send_sem=ssem.at[n], recv_sem=rsem.at[n],
                device_id=dev, device_id_type=MESH,
            )
            c.start()
            copies[key] = c

        def recv(key):
            copies[key].wait_recv()

        half = tokens // 2

        def blk(ref, w, h, a, b):
            z = j if h == 0 else 1 - j
            return ref.at[w, z, b, a] if h == 0 else ref.at[w, z, a, b]

        def axes(h):
            return (x, y, xdev, ydev) if h == 0 else (y, x, ydev, xdev)

        def init(w, h):
            a, b, adev, bdev = axes(h)
            if h == 1:
                recv(("a2a", w))
            src = dst = blk(W, w, h, a, b)
            send((1, w, h, 0), src, dst, adev(1))
            send((1, w, h, 1), src, dst, adev(3))
            send((2, w, h, 0, 0), src, dst, bdev(1))
            send((2, w, h, 0, 1), src, dst, bdev(3))

        def spread(w, h, s, a2):
            _, b, _, bdev = axes(h)
            ref = blk(W, w, h, a2, b)
            send((2, w, h, s, 0), ref, ref, bdev(1))
            send((2, w, h, s, 1), ref, ref, bdev(3))

        def near(w, h, side):
            a, b, adev, _ = axes(h)
            recv((1, w, h, side))
            place, away = ((at(a, 3), 1), (at(a, 1), 3))[side]
            ref = blk(W, w, h, place, b).at[side]
            send((1, w, h, 2 + side), ref, ref, adev(away))
            spread(w, h, 1 + side, place)

        def step2(w, h):
            a = axes(h)[0]
            recv((1, w, h, 2))
            recv((1, w, h, 3))
            spread(w, h, 3, at(a, 2))

        def fwd(w, h, s, side):
            a, b, _, bdev = axes(h)
            a2 = at(a, (0, 3, 1, 2)[s])
            recv((2, w, h, s, side))
            place, away = ((at(b, 3), 1), (at(b, 1), 3))[side]
            ref = blk(W, w, h, a2, place).at[side]
            send((2, w, h, s, 2 + side), ref, ref, bdev(away))

        whole = set()

        def fin(w):
            if w in whole:
                return
            whole.add(w)
            for h in (0, 1):
                for s in range(4):
                    recv((2, w, h, s, 2))
                    recv((2, w, h, s, 3))

        stock = {"x": (X, XT), "c": (C, CT)}

        def pass_on(name, i):
            recv((name, "z", i))
            rows = pl.ds(i * half, half)
            buf = stock[name][0]
            send((name, "zt", i), buf.at[2, rows], buf.at[3, rows], tpeer)

        def turn(name, slot):
            if slot == 1:
                recv((name, "t"))
            if slot == 3:
                recv((name, "zt", 0))
                recv((name, "zt", 1))
            src, dst = stock[name]
            v = src[slot].T
            dst[:, :, :, :, slot * tokens:(slot + 1) * tokens] = v.reshape(2, 4, 4, width // 32, tokens)

        def weight(w):
            return W[w].reshape(width, cols)

        def both(ref, s1, s2):
            return jnp.concatenate([ref[s1], ref[s2]], axis=0)

        def project(n):
            s1, s2 = 2 * n, 2 * n + 1
            fin(UP)
            pre = jnp.maximum(jnp.dot(both(X, s1, s2), weight(UP), preferred_element_type=F32), 0.0)
            for n, slot in enumerate((s1, s2)):
                v = pre[n * tokens:(n + 1) * tokens]
                RP[slot] = v
                ACT[slot] = (v * v).astype(BF)

        def pull_back(n):
            s1, s2 = 2 * n, 2 * n + 1
            fin(DN)
            back = jnp.dot(both(C, s1, s2), weight(DN), preferred_element_type=F32)
            for n, slot in enumerate((s1, s2)):
                GP[slot] = (2.0 * RP[slot] * back[n * tokens:(n + 1) * tokens]).astype(BF)

        lhs_of = (XT, CT)
        rhs_of = (GP, ACT)

        def gblk(w, h, a, b):
            z = j if h == 0 else 1 - j
            return G.at[w, z, a, b] if h == 0 else G.at[w, z, b, a]

        def raxes(h):
            return (y, x, ydev, xdev) if h == 0 else (x, y, xdev, ydev)

        def product(w, h, lo, n):
            z = j if h == 0 else 1 - j
            left = lhs_of[w][z, :, :, :, lo * tokens:(lo + n) * tokens].reshape(width // 2, n * tokens)
            right = rhs_of[w][lo:lo + n].reshape(n * tokens, cols)
            out = jnp.dot(left, right, preferred_element_type=F32)
            return G.at[w, z], out.reshape(4, 4, width // 32, cols)

        begun = set()

        def multiply_early(w, h):
            ref, out = product(w, h, 0, 2)
            ref[...] = out
            begun.add((w, h))

        def multiply(w, h):
            if (w, h) in begun:
                ref, out = product(w, h, 2, 2)
                ref[...] = ref[...] + out
            else:
                ref, out = product(w, h, 0, 4)
                ref[...] = out

        def encode(srcs, dst, scale, steps=3):
            top = None
            for src in srcs:
                for c in lanes:
                    m = jnp.max(jnp.abs(src[:, c]).reshape(-1, 8, 128), axis=0)
                    top = m if top is None else jnp.maximum(top, m)
            top = jnp.maximum(top, 2e-34)
            scale[...] = top
            inv = 2.0 ** (120 >> steps) / top
            for i, src in enumerate(srcs):
                for c in lanes:
                    v = src[:, c]
                    v3 = v.reshape(-1, 8, 128) * inv
                    for _ in range(steps):
                        v3 = v3 * jnp.abs(v3)
                    dst[i, :, c] = v3.reshape(v.shape).astype(BF)

        def decode(buf, scale, i, c, steps=3):
            v = buf[i, :, c].astype(F32)
            m = jnp.exp2(jnp.log2(jnp.abs(v)) * 0.5 ** steps)
            m = jnp.where(v < 0, -m, m).reshape(-1, 8, 128) * (scale[...] * 0.5 ** (120 >> steps))
            return m.reshape(v.shape)

        class Ring:
            def __init__(self, stage, w, h, pos, dev, parts, bufs, subs):
                self.k = (stage, w, h)
                self.subs = subs
                self.pos, self.dev, self.parts = pos, dev, parts
                self.sb, self.rb, self.sc, self.rc = (b.at[2 * w + h] for b in bufs)

            def post(self, i, srcs, d, lo, n):
                for m in range(lo, lo + n):
                    encode([srcs[m]], self.sb.at[i, pl.ds(m, 1)], self.sc.at[i, m])
                at_ = pl.ds(lo, n)
                send(self.k + (i, lo, "s"), self.sc.at[i, at_], self.rc.at[i, at_], self.dev(d))
                send(self.k + (i, lo, "v"), self.sb.at[i, at_], self.rb.at[i, at_], self.dev(d))

            def take(self, i, refs, lo, n):
                recv(self.k + (i, lo, "s"))
                recv(self.k + (i, lo, "v"))
                for m in range(lo, lo + n):
                    for c in lanes:
                        refs[m][:, c] = refs[m][:, c] + decode(self.rb.at[i], self.rc.at[i, m], m, c)

            def far(self, lo=0, n=1):
                self.post(0, self.parts(at(self.pos, 2), 0), 1, lo, n)
                self.post(1, self.parts(at(self.pos, 2), 1), 3, lo, n)

            def near_right(self):
                self.post(2, self.parts(at(self.pos, 1), 1), 1, 0, self.subs)

            def near_left(self):
                self.post(3, self.parts(at(self.pos, 3), 0), 3, 0, self.subs)

            def relay(self, side, lo=0, n=1):
                p = self.parts(at(self.pos, (1, 3)[side]), side)
                self.take(side, p, lo, n)
                self.post(4 + side, p, (1, 3)[side], lo, n)

            def near_in(self):
                self.take(3, self.parts(self.pos, 0), 0, self.subs)
                self.take(2, self.parts(self.pos, 1), 0, self.subs)

            def last_in(self):
                for lo in range(self.subs):
                    self.take(4, self.parts(self.pos, 0), lo, 1)
                    self.take(5, self.parts(self.pos, 1), lo, 1)

        def ring1(w, h):
            a, b, adev, bdev = raxes(h)
            return Ring(1, w, h, a, adev,
                        lambda place, side: [gblk(w, h, place, 2 * side + i) for i in (0, 1)],
                        (s1s, s1r, c1s, c1r), 2)

        hr = width // 64

        def ring2(w, h):
            a, b, adev, bdev = raxes(h)
            return Ring(2, w, h, b, bdev,
                        lambda place, side: [gblk(w, h, a, place).at[pl.ds(side * hr, hr)]],
                        (s2s, s2r, c2s, c2r), 1)

        first = {(w, h): ring1(w, h) for w in (UP, DN) for h in (0, 1)}
        second = {(w, h): ring2(w, h) for w in (UP, DN) for h in (0, 1)}

        def second_start(w, h):
            first[w, h].last_in()
            second[w, h].far()
            second[w, h].near_right()
            second[w, h].near_left()

        def third_start(w, h):
            second[w, h].near_in()
            second[w, h].last_in()
            a, b, _, _ = raxes(h)
            encode([gblk(w, h, a, b)], s3s.at[w, h], c3s.at[w, h])
            peers_ = [(0, rpeer)] if h == 0 else [(1, zpeer), (2, rzpeer)]
            for i, dev in peers_:
                send((3, w, i, "s"), c3s.at[w, h], c3r.at[w, i], dev)
                send((3, w, i, "v"), s3s.at[w, h], s3r.at[w, i], dev)

        def finish(w):
            out = (gup_ref, gdn_ref)[w]
            for i in range(3):
                recv((3, w, i, "s"))
                recv((3, w, i, "v"))
            for c in range(len(lanes)):
                lane = lanes[c]
                mine = decode(s3s.at[w, 0], c3s.at[w, 0], 0, lane)
                mine = mine + decode(s3r.at[w, 0], c3r.at[w, 0], 0, lane)
                out[:, pl.ds(pl.multiple_of(j * cols + c * 128, 128), 128)] = mine * factor
                theirs = decode(s3r.at[w, 1], c3r.at[w, 1], 0, lane)
                theirs = theirs + decode(s3r.at[w, 2], c3r.at[w, 2], 0, lane)
                out[:, pl.ds(pl.multiple_of((1 - j) * cols + c * 128, 128), 128)] = theirs * factor
            store(out, (gup_out, gdn_out)[w])

        def input_part(n):
            s1, s2 = ((3, 1), (2, 0))[n]
            w = W[UP].reshape(width, cols)
            v = lax.dot_general(both(GP, s1, s2), w, (((1,), (1,)), ((), ())), preferred_element_type=F32)
            PART[s1] = v[:tokens]
            PART[s2] = v[tokens:]
            if n == 0:
                for i, slot in enumerate((3, 1)):
                    send(("g", "t", i), PART.at[slot], DR.at[i], tpeer)

        def input_send():
            recv(("g", "t", 0))
            PART[2] = PART[2] + DR[0]
            encode([PART.at[2]], ZS, zsc.at[0], 4)
            send(("g", "zs"), zsc.at[0], zsc.at[1], zpeer)
            send(("g", "z"), ZS, ZR, zpeer)

        def input_sum():
            recv(("g", "t", 1))
            recv(("g", "zs"))
            recv(("g", "z"))
            for c in lanes:
                far = decode(ZR, zsc.at[1], 0, c, 4)
                gin_ref[:, c] = (PART[0, :, c] + DR[1, :, c] + far).astype(BF)
            store(gin_ref, gin_out)

        def energy_x():
            EX[x] = jnp.sum(gdn_ref[...] * gdn_ref[...], axis=0, keepdims=True)
            for d in (1, 2, 3):
                send(("e", "x", d), EX.at[x], EX.at[x], xdev(d))

        def energy_y():
            for d in (1, 2, 3):
                recv(("e", "x", d))
            EY[j, y] = EX[0] + EX[1] + EX[2] + EX[3]
            send(("e", "y", 4), EY.at[j, y], EY.at[j, y], zpeer)
            for d in (1, 2, 3):
                send(("e", "y", d), EY.at[j, y], EY.at[j, y], ydev(d))
                send(("e", "y", 4 + d), EY.at[j, y], EY.at[j, y], yzdev(d))

        def energy_down():
            for d in range(1, 8):
                recv(("e", "y", d))
            total = EY[0, 0]
            for n in range(1, 8):
                total = total + EY[n // 4, n % 4]
            edn_ref[...] = total * (1.0 / width)

        def energy_pair():
            total = None
            for c in range(2 * len(lanes)):
                v = gup_ref[:, c * 128:(c + 1) * 128]
                total = v * v if total is None else total + v * v
            EU[0] = total
            send(("e", "t"), EU.at[0], EU.at[1], tpeer)

        def energy_up():
            recv(("e", "t"))
            eup_ref[...] = jnp.sum((EU[0] + EU[1]).T, axis=0, keepdims=True) * (1.0 / ff)

        loads[0].wait()
        send(("a2a", UP), OTH.at[UP], W.at[UP, j, y, x], rzpeer)
        loads[1].wait()
        send(("a2a", DN), OTH.at[DN], W.at[DN, j, y, x], rzpeer)
        for c in loads[2:]:
            c.wait()
        for name in ("x", "c"):
            buf = stock[name][0]
            for i in (0, 1):
                rows = pl.ds(i * half, half)
                send((name, "z", i), buf.at[0, rows], buf.at[2, rows], zpeer)
            send((name, "t"), buf.at[0], buf.at[1], tpeer)
        todo = {
            "init": init, "near": near, "step2": step2, "fwd": fwd, "pass": pass_on, "turn": turn,
            "proj": project, "pull": pull_back, "mult": multiply, "ma": multiply_early,
            "far": lambda w, h, lo: first[w, h].far(lo),
            "nr": lambda w, h: first[w, h].near_right(),
            "nl": lambda w, h: first[w, h].near_left(),
            "rl": lambda w, h, side, lo: first[w, h].relay(side, lo),
            "ni": lambda w, h: first[w, h].near_in(),
            "st2": second_start,
            "rl2": lambda w, h, side: second[w, h].relay(side),
            "st3": third_start, "fin": finish, "ip": input_part, "gz": input_send, "gin": input_sum,
            "ex": energy_x, "ey": energy_y, "edn": energy_down,
            "eu": energy_pair, "eup": energy_up,
        }
        drained, marks = 0, [0] * LAG
        for name, *where in ORDER:
            todo[name](*where)
            marks.append(len(copies))
            for key in list(copies)[drained:marks[-LAG]]:
                copies[key].wait_send()
            drained = max(drained, marks[-LAG])
        for key in list(copies)[drained:]:
            copies[key].wait_send()
        for c in stores:
            c.wait()

    return kernel


def hand_over(results):
    vm = pl.BlockSpec(memory_space=pltpu.VMEM)
    shapes = [jax.ShapeDtypeStruct(v.shape, v.dtype) for v in results]
    shapes[4] = jax.ShapeDtypeStruct(results[4].shape[1:], F32)

    def kernel(*refs):
        for src, dst in zip(refs[:4], refs[5:9]):
            dst[...] = src[...]
        refs[9][...] = refs[4][0]

    return pl.pallas_call(kernel, out_shape=tuple(shapes), in_specs=[vm] * 5, out_specs=(vm,) * 5)(*results)


def per_device(inputs, up_proj, down_proj, out_cotangent):
    tokens, width = inputs.shape
    rows, hidden = up_proj.shape
    cols = hidden // 2
    ff = hidden * lax.axis_size("tp")
    all_tokens = tokens * lax.axis_size("rep") * lax.axis_size(FS) * lax.axis_size("tp")
    factor = float(all_tokens) ** (-0.5)
    up3 = up_proj.reshape(2, rows // 2, hidden)
    dn3 = down_proj.T.reshape(2, rows // 2, hidden)
    vm = pl.BlockSpec(memory_space=pltpu.VMEM)
    full = (2, 4, 4, rows)
    results = pl.pallas_call(
        make_kernel(tokens, width, cols, ff, factor),
        out_shape=(
            jax.ShapeDtypeStruct((tokens, width), BF),
            jax.ShapeDtypeStruct((rows, hidden), F32),
            jax.ShapeDtypeStruct((rows, hidden), F32),
            jax.ShapeDtypeStruct((1, rows), F32),
            jax.ShapeDtypeStruct((1, hidden), F32),
        ),
        in_specs=[pl.BlockSpec(memory_space=pl.ANY)] * 4,
        out_specs=(pl.BlockSpec(memory_space=pl.ANY),) * 3 + (vm, vm),
        scratch_shapes=[
            pltpu.VMEM((4, tokens, width), BF),
            pltpu.VMEM((4, tokens, width), BF),
            pltpu.VMEM(full + (4 * tokens,), BF),
            pltpu.VMEM(full + (4 * tokens,), BF),
            pltpu.VMEM((2, 2, 4, 4, 2, rows // 2, cols), BF),
            pltpu.VMEM((4, tokens, cols), F32),
            pltpu.VMEM((4, tokens, cols), BF),
            pltpu.VMEM((4, tokens, cols), BF),
            pltpu.VMEM((2,) + full + (cols,), F32),
            pltpu.VMEM((4, 6, 2, rows, cols), BF),
            pltpu.VMEM((4, 6, 2, rows, cols), BF),
            pltpu.VMEM((4, 6, 2, 8, 128), F32),
            pltpu.VMEM((4, 6, 2, 8, 128), F32),
            pltpu.VMEM((4, 6, 1, rows // 2, cols), BF),
            pltpu.VMEM((4, 6, 1, rows // 2, cols), BF),
            pltpu.VMEM((4, 6, 1, 8, 128), F32),
            pltpu.VMEM((4, 6, 1, 8, 128), F32),
            pltpu.VMEM((2, 2, 1, rows, cols), BF),
            pltpu.VMEM((2, 3, 1, rows, cols), BF),
            pltpu.VMEM((2, 2, 8, 128), F32),
            pltpu.VMEM((2, 3, 8, 128), F32),
            pltpu.VMEM((4, tokens, width), F32),
            pltpu.VMEM((2, tokens, width), F32),
            pltpu.VMEM((1, tokens, width), BF),
            pltpu.VMEM((1, tokens, width), BF),
            pltpu.VMEM((2, 8, 128), F32),
            pltpu.VMEM((4, 1, hidden), F32),
            pltpu.VMEM((2, 4, 1, hidden), F32),
            pltpu.VMEM((2, rows, 128), F32),
            pltpu.VMEM((2, 2, rows // 2, cols), BF),
            pltpu.VMEM((tokens, width), BF),
            pltpu.VMEM((rows, hidden), F32),
            pltpu.VMEM((rows, hidden), F32),
            pltpu.SemaphoreType.DMA((COPIES,)),
            pltpu.SemaphoreType.DMA((COPIES,)),
            pltpu.SemaphoreType.DMA((9,)),
        ],
        compiler_params=pltpu.CompilerParams(
            collective_id=0, has_side_effects=True, vmem_limit_bytes=63 * 1024 * 1024
        ),
    )(inputs, up3, dn3, out_cotangent)
    gin, gup, gdn, eup, edn = hand_over(results)
    return gin, gup, gdn.T, eup.reshape(rows), edn


def solution(mesh):
    torus = Mesh(
        mesh.devices.reshape(mesh.shape["rep"], 2, 4, 4, mesh.shape["tp"]),
        ("rep", "fs_0", "fs_1", "fs_2", "tp"),
    )
    placed = (P(REP_FS_TP, None), P(FS, "tp"), P("tp", FS), P(REP_FS_TP, None))
    return jax.shard_map(
        per_device,
        mesh=torus,
        in_specs=placed,
        out_specs=(P(REP_FS_TP, None), P(FS, "tp"), P("tp", FS), P(FS), P("tp")),
        check_vma=False,
    )
```

```python
import jax
import jax.numpy as jnp
from jax import lax
from jax.experimental import pallas as pl
from jax.experimental.pallas import tpu as pltpu
from jax.sharding import Mesh
from jax.sharding import PartitionSpec as P

FS = ("fs_0", "fs_1", "fs_2")
REP_FS_TP = ("rep", "fs_0", "fs_1", "fs_2", "tp")
MESH = pl.DeviceIdType.MESH
BF = jnp.bfloat16
F32 = jnp.float32
RIGHT, LEFT = 0, 1
UP, DN = 0, 1
WAITS, BATCHES = 110, 26


ORDER = [
    ("init", 0, 0), ("init", 1, 0), ("turn", "x", 1), ("init", 0, 1), ("init", 1, 1), ("near", 0, 1, 0),
    ("turn", "c", 1), ("fwd", 0, 0, 0, 0), ("near", 0, 1, 1), ("near", 0, 0, 0), ("near", 1, 0, 1),
    ("fwd", 0, 0, 0, 1), ("near", 0, 0, 1), ("step2", 0, 1), ("near", 1, 1, 0), ("near", 1, 1, 1),
    ("near", 1, 0, 0), ("pass", "x", 0), ("fwd", 0, 1, 0, 0), ("fwd", 0, 1, 0, 1), ("pass", "x", 1),
    ("step2", 0, 0), ("fwd", 0, 1, 3, 0), ("fwd", 0, 1, 3, 1), ("fwd", 0, 1, 1, 0), ("turn", "x", 3),
    ("fwd", 1, 0, 0, 1), ("fwd", 0, 0, 1, 1), ("turn", "x", 0), ("fwd", 1, 1, 0, 0), ("fwd", 0, 0, 2, 0),
    ("fwd", 0, 1, 1, 1), ("turn", "c", 0), ("fwd", 0, 1, 2, 1), ("fwd", 0, 1, 2, 0), ("fwd", 1, 0, 2, 1),
    ("fwd", 0, 0, 1, 0), ("step2", 1, 1), ("fwd", 1, 1, 2, 1), ("fwd", 1, 1, 0, 1), ("fwd", 1, 1, 1, 0),
    ("fwd", 0, 0, 3, 0), ("fwd", 0, 0, 2, 1), ("fwd", 1, 1, 1, 1), ("fwd", 0, 0, 3, 1), ("turn", "x", 2),
    ("pass", "c", 0), ("step2", 1, 0), ("proj", 0), ("fwd", 1, 0, 0, 0), ("fwd", 1, 0, 2, 0), ("fwd", 1, 0, 1, 1),
    ("fwd", 1, 0, 3, 0), ("pass", "c", 1), ("ma", 1, 1), ("fwd", 1, 1, 3, 0), ("fwd", 1, 1, 3, 1),
    ("fwd", 1, 0, 1, 0), ("fwd", 1, 0, 3, 1), ("proj", 1), ("fwd", 1, 1, 2, 0), ("turn", "c", 2),
    ("turn", "c", 3), ("mult", 1, 0), ("mult", 1, 1), ("far", 1, 1, 1), ("far", 1, 0, 0), ("nl", 1, 0),
    ("far", 1, 1, 0), ("nr", 1, 1), ("far", 1, 0, 1), ("pull", 1), ("pull", 0), ("nr", 1, 0), ("nl", 1, 1),
    ("ip", 0), ("mult", 0, 0), ("rl", 1, 0, 0, 0), ("rl", 1, 1, 1, 1), ("rl", 1, 1, 0, 1), ("rl", 1, 0, 1, 0),
    ("rl", 1, 1, 0, 0), ("far", 0, 0, 0), ("rl", 1, 1, 1, 0), ("far", 0, 0, 1), ("rl", 1, 0, 0, 1),
    ("mult", 0, 1), ("far", 0, 1, 0), ("ip", 1), ("gz",), ("nr", 0, 1), ("nl", 0, 1), ("rl", 1, 0, 1, 1),
    ("ni", 1, 1), ("rl", 0, 0, 0, 0), ("rl", 0, 0, 1, 0), ("far", 0, 1, 1), ("ni", 1, 0), ("nl", 0, 0),
    ("st2", 1, 1), ("nr", 0, 0), ("rl", 0, 0, 1, 1), ("rl", 0, 0, 0, 1), ("st2", 1, 0), ("ni", 0, 1),
    ("rl2", 1, 0, 1), ("rl2", 1, 0, 0), ("rl", 0, 1, 1, 1), ("rl", 0, 1, 0, 0), ("rl2", 1, 1, 1),
    ("rl", 0, 1, 0, 1), ("rl2", 1, 1, 0), ("rl", 0, 1, 1, 0), ("ni", 0, 0), ("st3", 1, 0), ("st2", 0, 0),
    ("st3", 1, 1), ("st2", 0, 1), ("rl2", 0, 0, 0), ("rl2", 0, 0, 1), ("rl2", 0, 1, 1), ("rl2", 0, 1, 0),
    ("st3", 0, 0), ("fin", 1), ("ex",), ("st3", 0, 1), ("ey",), ("fin", 0), ("eu",), ("gin",), ("eup",), ("edn",),
]


def make_kernel(tokens, width, cols, ff, factor):
    lanes = [pl.ds(c * 128, 128) for c in range(cols // 128)]

    def kernel(
        x_ref, up_ref, dn_ref, cot_ref,
        gin_out, gup_out, gdn_out, eup_ref, edn_ref,
        X, C, XT, CT, W, RP, ACT, GP, G,
        s1s, s1r, s2s, s2r, s3s, s3r,
        PART, DR, ZS, ZR, EX, EY, EU,
        OTH, gin_ref, gup_ref, gdn_ref, ssem, rsem, lsem,
    ):
        r = lax.axis_index("rep")
        j = lax.axis_index("fs_0")
        y = lax.axis_index("fs_1")
        x = lax.axis_index("fs_2")
        t = lax.axis_index("tp")

        def at(pos, d):
            return lax.rem(pos + d, 4)

        def xdev(d):
            return {"fs_2": at(x, d)}

        def ydev(d):
            return {"fs_1": at(y, d)}

        def yzdev(d):
            return {"fs_0": 1 - j, "fs_1": at(y, d)}

        zpeer = {"fs_0": 1 - j}
        rpeer = {"rep": 1 - r}
        rzpeer = {"rep": 1 - r, "fs_0": 1 - j}
        tpeer = {"tp": 1 - t}

        own = pl.ds(pl.multiple_of(j * cols, cols), cols)
        other = pl.ds(pl.multiple_of((1 - j) * cols, cols), cols)
        loads = [
            pltpu.make_async_copy(up_ref.at[:, :, other], OTH.at[UP], lsem.at[0]),
            pltpu.make_async_copy(dn_ref.at[:, :, other], OTH.at[DN], lsem.at[1]),
            pltpu.make_async_copy(up_ref.at[:, :, own], W.at[UP, j, y, x], lsem.at[2]),
            pltpu.make_async_copy(dn_ref.at[:, :, own], W.at[DN, j, y, x], lsem.at[3]),
            pltpu.make_async_copy(x_ref, X.at[0], lsem.at[4]),
            pltpu.make_async_copy(cot_ref, C.at[0], lsem.at[5]),
        ]
        for c in loads:
            c.start()

        barrier = pltpu.get_barrier_semaphore()
        peers = [xdev(1), xdev(2), xdev(3), ydev(1), ydev(2), ydev(3), zpeer, rpeer, rzpeer, tpeer, yzdev(1), yzdev(2), yzdev(3)]
        for dev in peers:
            pl.semaphore_signal(barrier, inc=1, device_id=dev, device_id_type=MESH)
        pl.semaphore_wait(barrier, len(peers))

        stores = []

        def store(src, dst):
            c = pltpu.make_async_copy(src, dst, lsem.at[6 + len(stores)])
            c.start()
            stores.append(c)

        arrivals, departures = {}, {}

        def slot_of(table, group):
            return table.setdefault(group, len(table))

        def send(group, src, dst, dev, batch):
            pltpu.make_async_remote_copy(
                src_ref=src, dst_ref=dst,
                send_sem=ssem.at[slot_of(departures, batch)], recv_sem=rsem.at[slot_of(arrivals, group)],
                device_id=dev, device_id_type=MESH,
            ).start()

        def recv(group, ref):
            pltpu.make_async_copy(ref, ref, rsem.at[arrivals[group]]).wait()

        def sent(batch, ref):
            pltpu.make_async_copy(ref, ref, ssem.at[departures[batch]]).wait()

        half = tokens // 2

        def blk(ref, w, h, a, b):
            z = j if h == 0 else 1 - j
            return ref.at[w, z, b, a] if h == 0 else ref.at[w, z, a, b]

        def axes(h):
            return (x, y, xdev, ydev) if h == 0 else (y, x, ydev, xdev)

        def init(w, h):
            a, b, adev, bdev = axes(h)
            ref = blk(W, w, h, a, b)
            if h == 1:
                recv(("a2a", w), ref)
            send((1, w, h, 0), ref, ref, adev(1), (w, h))
            send((1, w, h, 1), ref, ref, adev(3), (w, h))
            spread(w, h, 0, a)

        def spread(w, h, s, a2):
            _, b, _, bdev = axes(h)
            ref = blk(W, w, h, a2, b)
            send((2, w, h, s, 0), ref, ref, bdev(1), (w, h))
            send((2, w, h, s, 1), ref, ref, bdev(3), (w, h))

        def near(w, h, side):
            a, b, adev, _ = axes(h)
            place, away = ((at(a, 3), 1), (at(a, 1), 3))[side]
            ref = blk(W, w, h, place, b)
            recv((1, w, h, side), ref)
            send((1, w, h, 2), ref.at[side], ref.at[side], adev(away), (w, h))
            spread(w, h, 1 + side, place)

        def step2(w, h):
            a, b, _, _ = axes(h)
            recv((1, w, h, 2), blk(W, w, h, at(a, 2), b))
            spread(w, h, 3, at(a, 2))

        def fwd(w, h, s, side):
            a, b, _, bdev = axes(h)
            a2 = at(a, (0, 3, 1, 2)[s])
            place, away = ((at(b, 3), 1), (at(b, 1), 3))[side]
            ref = blk(W, w, h, a2, place)
            recv((2, w, h, s, side), ref)
            send((3, w), ref.at[side], ref.at[side], bdev(away), (w, h))

        whole = set()

        def fin(w):
            if w not in whole:
                whole.add(w)
                recv((3, w), W.at[w, 0, pl.ds(0, 2)])

        stock = {"x": (X, XT), "c": (C, CT)}

        def pass_on(name, i):
            rows = pl.ds(i * half, half)
            buf = stock[name][0]
            recv((name, "z", i), buf.at[2, rows])
            send((name, "zt"), buf.at[2, rows], buf.at[3, rows], tpeer, (name, "zt"))

        def turn(name, slot):
            src, dst = stock[name]
            if slot == 1:
                recv((name, "t"), src.at[1])
            if slot == 3:
                recv((name, "zt"), src.at[3])
            v = src[slot].T
            dst[:, :, :, :, slot * tokens:(slot + 1) * tokens] = v.reshape(2, 4, 4, width // 32, tokens)

        def weight(w):
            return W[w].reshape(width, cols)

        def both(ref, s1, s2):
            return jnp.concatenate([ref[s1], ref[s2]], axis=0)

        def project(n):
            s1, s2 = 2 * n, 2 * n + 1
            fin(UP)
            pre = jnp.maximum(jnp.dot(both(X, s1, s2), weight(UP), preferred_element_type=F32), 0.0)
            for n, slot in enumerate((s1, s2)):
                v = pre[n * tokens:(n + 1) * tokens]
                RP[slot] = v
                ACT[slot] = (v * v).astype(BF)

        def pull_back(n):
            s1, s2 = 2 * n, 2 * n + 1
            fin(DN)
            back = jnp.dot(both(C, s1, s2), weight(DN), preferred_element_type=F32)
            for n, slot in enumerate((s1, s2)):
                GP[slot] = (2.0 * RP[slot] * back[n * tokens:(n + 1) * tokens]).astype(BF)

        lhs_of = (XT, CT)
        rhs_of = (GP, ACT)

        def gblk(w, h, a, b):
            z = j if h == 0 else 1 - j
            return G.at[w, z, a, b] if h == 0 else G.at[w, z, b, a]

        def raxes(h):
            return (y, x, ydev, xdev) if h == 0 else (x, y, xdev, ydev)

        def product(w, h, lo, n):
            z = j if h == 0 else 1 - j
            left = lhs_of[w][z, :, :, :, lo * tokens:(lo + n) * tokens].reshape(width // 2, n * tokens)
            right = rhs_of[w][lo:lo + n].reshape(n * tokens, cols)
            out = jnp.dot(left, right, preferred_element_type=F32)
            return G.at[w, z], out.reshape(4, 4, width // 32, cols)

        begun = set()

        def multiply_early(w, h):
            ref, out = product(w, h, 0, 2)
            ref[...] = out
            begun.add((w, h))

        def multiply(w, h):
            if (w, h) in begun:
                ref, out = product(w, h, 2, 2)
                ref[...] = ref[...] + out
            else:
                ref, out = product(w, h, 0, 4)
                ref[...] = out

        def tiles(rows):
            return [(n, pl.ds(16 * (n % (rows // 16)), 16), lanes[n // (rows // 16)])
                    for n in range(rows // 16 * len(lanes))]

        def encode(src, dst, steps=3):
            every = tiles(src.shape[0])
            top = None
            for _, q, c in every:
                m = jnp.abs(src[q, c])
                top = m if top is None else jnp.maximum(top, m)
            top = jnp.maximum(top, 2e-34).astype(BF)
            dst[len(every)] = top
            inv = 2.0 ** (120 >> steps) / top.astype(F32)
            for n, q, c in every:
                v = src[q, c] * inv
                for _ in range(steps):
                    v = v * jnp.abs(v)
                dst[n] = v.astype(BF)

        def decoder(buf, rows, steps=3):
            every = tiles(rows)
            unit = buf[len(every)].astype(F32) * 0.5 ** (120 >> steps)

            def tile(n):
                v = buf[n].astype(F32)
                m = jnp.exp2(jnp.log2(jnp.abs(v)) * 0.5 ** steps)
                return jnp.where(v < 0, -m, m) * unit
            return every, tile

        def add(ref, buf):
            every, tile = decoder(buf, ref.shape[0])
            for n, q, c in every:
                ref[q, c] = ref[q, c] + tile(n)

        class Ring:
            def __init__(self, stage, w, h, pos, dev, parts, bufs, subs):
                self.k = (stage, w, h)
                self.subs = subs
                self.pos, self.dev, self.parts = pos, dev, parts
                self.sb, self.rb = (b.at[2 * w + h] for b in bufs)

            def post(self, i, srcs, d, lo, n, group):
                for m in range(lo, lo + n):
                    encode(srcs[m], self.sb.at[i, m])
                some = pl.ds(lo, n)
                send(self.k + group, self.sb.at[i, some], self.rb.at[i, some], self.dev(d), self.k)

            def far(self, lo=0):
                self.post(0, self.parts(at(self.pos, 2), 0), 1, lo, 1, ("far", 0, lo))
                self.post(1, self.parts(at(self.pos, 2), 1), 3, lo, 1, ("far", 1, lo))

            def near_right(self):
                self.post(2, self.parts(at(self.pos, 1), 1), 1, 0, self.subs, ("near",))

            def near_left(self):
                self.post(3, self.parts(at(self.pos, 3), 0), 3, 0, self.subs, ("near",))

            def relay(self, side, lo=0):
                p = self.parts(at(self.pos, (1, 3)[side]), side)
                recv(self.k + ("far", side, lo), self.rb.at[side, pl.ds(lo, 1)])
                add(p[lo], self.rb.at[side, lo])
                self.post(4 + side, p, (1, 3)[side], lo, 1, ("last", lo))

            def near_in(self):
                recv(self.k + ("near",), self.rb.at[pl.ds(2, 2)])
                for m in range(self.subs):
                    add(self.parts(self.pos, 0)[m], self.rb.at[3, m])
                    add(self.parts(self.pos, 1)[m], self.rb.at[2, m])

            def last_in(self):
                for m in range(self.subs):
                    recv(self.k + ("last", m), self.rb.at[pl.ds(4, 2), m])
                    add(self.parts(self.pos, 0)[m], self.rb.at[4, m])
                    add(self.parts(self.pos, 1)[m], self.rb.at[5, m])

        def ring1(w, h):
            a, b, adev, bdev = raxes(h)
            return Ring(1, w, h, a, adev,
                        lambda place, side: [gblk(w, h, place, 2 * side + i) for i in (0, 1)],
                        (s1s, s1r), 2)

        hr = width // 64

        def ring2(w, h):
            a, b, adev, bdev = raxes(h)
            return Ring(2, w, h, b, bdev,
                        lambda place, side: [gblk(w, h, a, place).at[pl.ds(side * hr, hr)]],
                        (s2s, s2r), 1)

        first = {(w, h): ring1(w, h) for w in (UP, DN) for h in (0, 1)}
        second = {(w, h): ring2(w, h) for w in (UP, DN) for h in (0, 1)}

        def second_start(w, h):
            first[w, h].last_in()
            second[w, h].far()
            second[w, h].near_right()
            second[w, h].near_left()

        def third_start(w, h):
            second[w, h].near_in()
            second[w, h].last_in()
            a, b, _, _ = raxes(h)
            encode(gblk(w, h, a, b), s3s.at[w, h])
            peers_ = [(0, rpeer)] if h == 0 else [(1, zpeer), (2, rzpeer)]
            for i, dev in peers_:
                send((5, w), s3s.at[w, h], s3r.at[w, i], dev, (5, w))

        def finish(w):
            out = (gup_ref, gdn_ref)[w]
            recv((5, w), s3r.at[w])
            for side, one, two in ((j, s3s.at[w, 0], s3r.at[w, 0]), (1 - j, s3r.at[w, 1], s3r.at[w, 2])):
                every, tile1 = decoder(one, width // 32)
                _, tile2 = decoder(two, width // 32)
                for n, q, c in every:
                    col = pl.ds(pl.multiple_of(side * cols + n // (width // 512) * 128, 128), 128)
                    out[q, col] = (tile1(n) + tile2(n)) * factor
            store(out, (gup_out, gdn_out)[w])

        def input_part(n):
            s1, s2 = ((3, 1), (2, 0))[n]
            w = W[UP].reshape(width, cols)
            v = lax.dot_general(both(GP, s1, s2), w, (((1,), (1,)), ((), ())), preferred_element_type=F32)
            PART[s1] = v[:tokens]
            PART[s2] = v[tokens:]
            if n == 0:
                for i, slot in enumerate((3, 1)):
                    send(("g", "t", i), PART.at[slot], DR.at[i], tpeer, "gt")

        def input_send():
            recv(("g", "t", 0), DR.at[0])
            PART[2] = PART[2] + DR[0]
            encode(PART.at[2], ZS, 4)
            send("gz", ZS, ZR, zpeer, "gz")

        def input_sum():
            recv(("g", "t", 1), DR.at[1])
            recv("gz", ZR)
            every, tile = decoder(ZR, tokens, 4)
            for n, q, c in every:
                gin_ref[q, c] = (PART[0, q, c] + DR[1, q, c] + tile(n)).astype(BF)
            store(gin_ref, gin_out)

        def energy_x():
            EX[x] = jnp.sum(gdn_ref[...] * gdn_ref[...], axis=0, keepdims=True)
            for d in (1, 2, 3):
                send("ex", EX.at[x], EX.at[x], xdev(d), "ex")

        def energy_y():
            recv("ex", EX.at[pl.ds(0, 3)])
            me = 4 * j + y
            EY[me] = EX[0] + EX[1] + EX[2] + EX[3]
            for dev in [zpeer] + [f(d) for d in (1, 2, 3) for f in (ydev, yzdev)]:
                send("ey", EY.at[me], EY.at[me], dev, "ey")

        def energy_down():
            recv("ey", EY.at[pl.ds(0, 7)])
            total = EY[0]
            for n in range(1, 8):
                total = total + EY[n]
            edn_ref[...] = total * (1.0 / width)

        def energy_pair():
            total = None
            for c in range(2 * len(lanes)):
                v = gup_ref[:, c * 128:(c + 1) * 128]
                total = v * v if total is None else total + v * v
            EU[0] = total
            send("et", EU.at[0], EU.at[1], tpeer, "et")

        def energy_up():
            recv("et", EU.at[1])
            eup_ref[...] = jnp.sum((EU[0] + EU[1]).T, axis=0, keepdims=True) * (1.0 / ff)

        for w in (UP, DN):
            loads[w].wait()
            send(("a2a", w), OTH.at[w], W.at[w, j, y, x], rzpeer, "a2a")
        for c in loads[2:]:
            c.wait()
        for name in ("x", "c"):
            buf = stock[name][0]
            for i in (0, 1):
                rows = pl.ds(i * half, half)
                send((name, "z", i), buf.at[0, rows], buf.at[2, rows], zpeer, name)
            send((name, "t"), buf.at[0], buf.at[1], tpeer, name)
        todo = {
            "init": init, "near": near, "step2": step2, "fwd": fwd, "pass": pass_on, "turn": turn,
            "proj": project, "pull": pull_back, "mult": multiply, "ma": multiply_early,
            "far": lambda w, h, lo: first[w, h].far(lo),
            "nr": lambda w, h: first[w, h].near_right(),
            "nl": lambda w, h: first[w, h].near_left(),
            "rl": lambda w, h, side, lo: first[w, h].relay(side, lo),
            "ni": lambda w, h: first[w, h].near_in(),
            "st2": second_start,
            "rl2": lambda w, h, side: second[w, h].relay(side),
            "st3": third_start, "fin": finish, "ip": input_part, "gz": input_send, "gin": input_sum,
            "ex": energy_x, "ey": energy_y, "edn": energy_down,
            "eu": energy_pair, "eup": energy_up,
        }
        for name, *where in ORDER:
            todo[name](*where)
        sent("a2a", OTH)
        for n, name in enumerate(("x", "c")):
            sent(name, RP.at[0])
            sent((name, "zt"), X.at[0])
            for h in (0, 1):
                sent((n, h), RP.at[0, pl.ds(0, 15 * tokens // 16)])
                sent((1, n, h), s1s.at[0])
                sent((2, n, h), s2s.at[0])
            sent((5, n), s3r.at[0])
        sent("gt", PART.at[pl.ds(0, 2)])
        sent("gz", ZS)
        sent("ex", EX.at[pl.ds(0, 3)])
        sent("ey", EY.at[pl.ds(0, 7)])
        sent("et", EU.at[0])
        for c in stores:
            c.wait()

    return kernel


def hand_over(results):
    vm = pl.BlockSpec(memory_space=pltpu.VMEM)
    shapes = [jax.ShapeDtypeStruct(v.shape, v.dtype) for v in results]
    shapes[4] = jax.ShapeDtypeStruct(results[4].shape[1:], F32)

    def kernel(*refs):
        for src, dst in zip(refs[:4], refs[5:9]):
            dst[...] = src[...]
        refs[9][...] = refs[4][0]

    return pl.pallas_call(kernel, out_shape=tuple(shapes), in_specs=[vm] * 5, out_specs=(vm,) * 5)(*results)


def per_device(inputs, up_proj, down_proj, out_cotangent):
    tokens, width = inputs.shape
    rows, hidden = up_proj.shape
    cols = hidden // 2
    ff = hidden * lax.axis_size("tp")
    all_tokens = tokens * lax.axis_size("rep") * lax.axis_size(FS) * lax.axis_size("tp")
    factor = float(all_tokens) ** (-0.5)
    up3 = up_proj.reshape(2, rows // 2, hidden)
    dn3 = down_proj.T.reshape(2, rows // 2, hidden)
    vm = pl.BlockSpec(memory_space=pltpu.VMEM)
    full = (2, 4, 4, rows)
    lines = rows * cols // 2048
    results = pl.pallas_call(
        make_kernel(tokens, width, cols, ff, factor),
        out_shape=(
            jax.ShapeDtypeStruct((tokens, width), BF),
            jax.ShapeDtypeStruct((rows, hidden), F32),
            jax.ShapeDtypeStruct((rows, hidden), F32),
            jax.ShapeDtypeStruct((1, rows), F32),
            jax.ShapeDtypeStruct((1, hidden), F32),
        ),
        in_specs=[pl.BlockSpec(memory_space=pl.ANY)] * 4,
        out_specs=(pl.BlockSpec(memory_space=pl.ANY),) * 3 + (vm, vm),
        scratch_shapes=[
            pltpu.VMEM((4, tokens, width), BF),
            pltpu.VMEM((4, tokens, width), BF),
            pltpu.VMEM(full + (4 * tokens,), BF),
            pltpu.VMEM(full + (4 * tokens,), BF),
            pltpu.VMEM((2, 2, 4, 4, 2, rows // 2, cols), BF),
            pltpu.VMEM((4, tokens, cols), F32),
            pltpu.VMEM((4, tokens, cols), BF),
            pltpu.VMEM((4, tokens, cols), BF),
            pltpu.VMEM((2,) + full + (cols,), F32),
            pltpu.VMEM((4, 6, 2, lines + 1, 16, 128), BF),
            pltpu.VMEM((4, 6, 2, lines + 1, 16, 128), BF),
            pltpu.VMEM((4, 6, 1, lines // 2 + 1, 16, 128), BF),
            pltpu.VMEM((4, 6, 1, lines // 2 + 1, 16, 128), BF),
            pltpu.VMEM((2, 2, lines + 1, 16, 128), BF),
            pltpu.VMEM((2, 3, lines + 1, 16, 128), BF),
            pltpu.VMEM((4, tokens, width), F32),
            pltpu.VMEM((2, tokens, width), F32),
            pltpu.VMEM((tokens * width // 2048 + 1, 16, 128), BF),
            pltpu.VMEM((tokens * width // 2048 + 1, 16, 128), BF),
            pltpu.VMEM((4, 1, hidden), F32),
            pltpu.VMEM((8, 1, hidden), F32),
            pltpu.VMEM((2, rows, 128), F32),
            pltpu.VMEM((2, 2, rows // 2, cols), BF),
            pltpu.VMEM((tokens, width), BF),
            pltpu.VMEM((rows, hidden), F32),
            pltpu.VMEM((rows, hidden), F32),
            pltpu.SemaphoreType.DMA((BATCHES,)),
            pltpu.SemaphoreType.DMA((WAITS,)),
            pltpu.SemaphoreType.DMA((9,)),
        ],
        compiler_params=pltpu.CompilerParams(
            collective_id=0, has_side_effects=True, vmem_limit_bytes=63 * 1024 * 1024
        ),
    )(inputs, up3, dn3, out_cotangent)
    gin, gup, gdn, eup, edn = hand_over(results)
    return gin, gup, gdn.T, eup.reshape(rows), edn


def solution(mesh):
    torus = Mesh(
        mesh.devices.reshape(mesh.shape["rep"], 2, 4, 4, mesh.shape["tp"]),
        ("rep", "fs_0", "fs_1", "fs_2", "tp"),
    )
    placed = (P(REP_FS_TP, None), P(FS, "tp"), P("tp", FS), P(REP_FS_TP, None))
    return jax.shard_map(
        per_device,
        mesh=torus,
        in_specs=placed,
        out_specs=(P(REP_FS_TP, None), P(FS, "tp"), P("tp", FS), P(FS), P("tp")),
        check_vma=False,
    )
```

```python
import jax
import jax.numpy as jnp
from jax import lax
from jax.experimental import pallas as pl
from jax.experimental.pallas import tpu as pltpu
from jax.sharding import Mesh
from jax.sharding import PartitionSpec as P

FS = ("fs_0", "fs_1", "fs_2")
REP_FS_TP = ("rep", "fs_0", "fs_1", "fs_2", "tp")
MESH = pl.DeviceIdType.MESH
BF = jnp.bfloat16
F32 = jnp.float32
RIGHT, LEFT = 0, 1
UP, DN = 0, 1
WAITS, BATCHES = 110, 26


ORDER = [
    ("init", 1, 0), ("init", 0, 0), ("init", 0, 1), ("init", 1, 1), ("near", 0, 0, 0), ("pass", "x", 0),
    ("near", 0, 0, 1), ("near", 0, 1, 0), ("near", 0, 1, 1), ("fwd", 0, 0, 0, 0), ("turn", "x", 0),
    ("near", 1, 1, 0), ("step2", 0, 0), ("fwd", 0, 1, 1, 0), ("turn", "x", 1), ("fwd", 0, 0, 2, 1),
    ("step2", 0, 1), ("near", 1, 0, 1), ("fwd", 0, 0, 1, 1), ("near", 1, 0, 0), ("turn", "c", 0),
    ("near", 1, 1, 1), ("fwd", 0, 0, 3, 0), ("fwd", 0, 1, 0, 1), ("fwd", 1, 1, 0, 1), ("fwd", 0, 1, 3, 0),
    ("fwd", 0, 1, 3, 1), ("fwd", 0, 0, 3, 1), ("fwd", 0, 0, 0, 1), ("fwd", 1, 0, 0, 1), ("pass", "x", 1),
    ("turn", "c", 1), ("fwd", 0, 1, 1, 1), ("fwd", 0, 1, 2, 0), ("fwd", 1, 0, 2, 1), ("fwd", 0, 1, 2, 1),
    ("fwd", 0, 0, 1, 0), ("turn", "x", 2), ("fwd", 1, 1, 1, 0), ("fwd", 0, 0, 2, 0), ("fwd", 0, 1, 0, 0),
    ("step2", 1, 0), ("step2", 1, 1), ("fwd", 1, 0, 1, 1), ("turn", "x", 3), ("fwd", 1, 1, 0, 0),
    ("fwd", 1, 0, 2, 0), ("fwd", 1, 1, 2, 1), ("proj", 0), ("fwd", 1, 1, 2, 0), ("pass", "c", 0),
    ("fwd", 1, 0, 0, 0), ("ma", 1, 1), ("fwd", 1, 1, 3, 1), ("fwd", 1, 1, 1, 1), ("fwd", 1, 0, 3, 0),
    ("fwd", 1, 1, 3, 0), ("fwd", 1, 0, 1, 0), ("pass", "c", 1), ("turn", "c", 2), ("proj", 1),
    ("fwd", 1, 0, 3, 1), ("ma", 1, 0), ("turn", "c", 3), ("mult", 1, 0), ("far", 1, 0, 0), ("mult", 1, 1),
    ("far", 1, 1, 0), ("far", 1, 0, 1), ("far", 1, 1, 1), ("pull", 0), ("nr", 1, 1), ("nr", 1, 0), ("nl", 1, 1),
    ("nl", 1, 0), ("pull", 1), ("ip", 0), ("rl", 1, 0, 1, 1), ("rl", 1, 0, 0, 0), ("rl", 1, 0, 0, 1),
    ("mult", 0, 1), ("rl", 1, 1, 1, 0), ("far", 0, 1, 1), ("rl", 1, 0, 1, 0), ("mult", 0, 0), ("far", 0, 0, 0),
    ("rl", 1, 1, 0, 0), ("far", 0, 0, 1), ("rl", 1, 1, 1, 1), ("ni", 1, 0), ("ip", 1), ("rl", 1, 1, 0, 1),
    ("gz",), ("far", 0, 1, 0), ("nr", 0, 0), ("nl", 0, 0), ("st2", 1, 0), ("rl", 0, 0, 1, 0), ("nl", 0, 1),
    ("nr", 0, 1), ("rl", 0, 0, 0, 1), ("rl", 0, 0, 1, 1), ("rl", 0, 0, 0, 0), ("ni", 1, 1), ("st2", 1, 1),
    ("rl2", 1, 0, 1), ("ni", 0, 0), ("rl2", 1, 0, 0), ("rl", 0, 1, 0, 0), ("rl", 0, 1, 1, 1), ("rl", 0, 1, 0, 1),
    ("rl", 0, 1, 1, 0), ("st2", 0, 0), ("rl2", 1, 1, 1), ("ni", 0, 1), ("st3", 1, 0), ("rl2", 1, 1, 0),
    ("st2", 0, 1), ("rl2", 0, 0, 1), ("st3", 1, 1), ("rl2", 0, 0, 0), ("rl2", 0, 1, 1), ("rl2", 0, 1, 0),
    ("gin",), ("st3", 0, 0), ("fin", 1), ("ex",), ("st3", 0, 1), ("ey",), ("fin", 0), ("eu",), ("eup",), ("edn",),
]


def make_kernel(tokens, width, cols, ff, factor):
    lanes = [pl.ds(c * 128, 128) for c in range(cols // 128)]

    def kernel(
        x_ref, up_ref, dn_ref, cot_ref,
        gin_ref, gup_ref, gdn_ref, eup_ref, edn_ref,
        X, C, XT, CT, W, RP, ACT, GP, G,
        s1s, s1r, s2s, s2r, s3s, s3r,
        PART, DR, ZS, ZR, EX, EY, EU,
        OTH, ssem, rsem, lsem,
    ):
        r = lax.axis_index("rep")
        j = lax.axis_index("fs_0")
        y = lax.axis_index("fs_1")
        x = lax.axis_index("fs_2")
        t = lax.axis_index("tp")

        def at(pos, d):
            return lax.rem(pos + d, 4)

        def xdev(d):
            return {"fs_2": at(x, d)}

        def ydev(d):
            return {"fs_1": at(y, d)}

        def yzdev(d):
            return {"fs_0": 1 - j, "fs_1": at(y, d)}

        zpeer = {"fs_0": 1 - j}
        rpeer = {"rep": 1 - r}
        rzpeer = {"rep": 1 - r, "fs_0": 1 - j}
        tpeer = {"tp": 1 - t}

        own = pl.ds(pl.multiple_of(j * cols, cols), cols)
        other = pl.ds(pl.multiple_of((1 - j) * cols, cols), cols)
        loads = [
            pltpu.make_async_copy(up_ref.at[:, :, other], OTH.at[UP], lsem.at[0]),
            pltpu.make_async_copy(dn_ref.at[:, :, other], OTH.at[DN], lsem.at[1]),
            pltpu.make_async_copy(up_ref.at[:, :, own], W.at[UP, j, y, x], lsem.at[2]),
            pltpu.make_async_copy(dn_ref.at[:, :, own], W.at[DN, j, y, x], lsem.at[3]),
            pltpu.make_async_copy(x_ref, X.at[0], lsem.at[4]),
            pltpu.make_async_copy(cot_ref, C.at[0], lsem.at[5]),
        ]
        for c in loads:
            c.start()

        barrier = pltpu.get_barrier_semaphore()
        peers = [xdev(1), xdev(2), xdev(3), ydev(1), ydev(2), ydev(3), zpeer, rpeer, rzpeer, tpeer, yzdev(1), yzdev(2), yzdev(3)]
        for dev in peers:
            pl.semaphore_signal(barrier, inc=1, device_id=dev, device_id_type=MESH)
        pl.semaphore_wait(barrier, len(peers))

        arrivals, departures = {}, {}

        def slot_of(table, group):
            return table.setdefault(group, len(table))

        def send(group, src, dst, dev, batch):
            pltpu.make_async_remote_copy(
                src_ref=src, dst_ref=dst,
                send_sem=ssem.at[slot_of(departures, batch)], recv_sem=rsem.at[slot_of(arrivals, group)],
                device_id=dev, device_id_type=MESH,
            ).start()

        def recv(group, ref):
            pltpu.make_async_copy(ref, ref, rsem.at[arrivals[group]]).wait()

        def sent(batch, ref):
            pltpu.make_async_copy(ref, ref, ssem.at[departures[batch]]).wait()

        half = tokens // 2

        def blk(ref, w, h, a, b):
            z = j if h == 0 else 1 - j
            return ref.at[w, z, b, a] if h == 0 else ref.at[w, z, a, b]

        def axes(h):
            return (x, y, xdev, ydev) if h == 0 else (y, x, ydev, xdev)

        def init(w, h):
            a, b, adev, bdev = axes(h)
            ref = blk(W, w, h, a, b)
            if h == 1:
                recv(("a2a", w), ref)
            send((1, w, h, 0), ref, ref, adev(1), (w, h))
            send((1, w, h, 1), ref, ref, adev(3), (w, h))
            spread(w, h, 0, a)

        def spread(w, h, s, a2):
            _, b, _, bdev = axes(h)
            ref = blk(W, w, h, a2, b)
            send((2, w, h, s, 0), ref, ref, bdev(1), (w, h))
            send((2, w, h, s, 1), ref, ref, bdev(3), (w, h))

        def near(w, h, side):
            a, b, adev, _ = axes(h)
            place, away = ((at(a, 3), 1), (at(a, 1), 3))[side]
            ref = blk(W, w, h, place, b)
            recv((1, w, h, side), ref)
            send((1, w, h, 2), ref.at[side], ref.at[side], adev(away), (w, h))
            spread(w, h, 1 + side, place)

        def step2(w, h):
            a, b, _, _ = axes(h)
            recv((1, w, h, 2), blk(W, w, h, at(a, 2), b))
            spread(w, h, 3, at(a, 2))

        def fwd(w, h, s, side):
            a, b, _, bdev = axes(h)
            a2 = at(a, (0, 3, 1, 2)[s])
            place, away = ((at(b, 3), 1), (at(b, 1), 3))[side]
            ref = blk(W, w, h, a2, place)
            recv((2, w, h, s, side), ref)
            send((3, w), ref.at[side], ref.at[side], bdev(away), (w, h))

        whole = set()

        def fin(w):
            if w not in whole:
                whole.add(w)
                recv((3, w), W.at[w, 0, pl.ds(0, 2)])

        stock = {"x": (X, XT), "c": (C, CT)}

        def pass_on(name, i):
            rows = pl.ds(i * half, half)
            buf = stock[name][0]
            recv((name, "z", i), buf.at[2, rows])
            send((name, "zt"), buf.at[2, rows], buf.at[3, rows], tpeer, (name, "zt"))

        def turn(name, slot):
            src, dst = stock[name]
            if slot == 1:
                recv((name, "t"), src.at[1])
            if slot == 3:
                recv((name, "zt"), src.at[3])
            v = src[slot].T
            dst[:, :, :, :, slot * tokens:(slot + 1) * tokens] = v.reshape(2, 4, 4, width // 32, tokens)

        def weight(w):
            return W[w].reshape(width, cols)

        def both(ref, s1, s2):
            return jnp.concatenate([ref[s1], ref[s2]], axis=0)

        def project(n):
            s1, s2 = 2 * n, 2 * n + 1
            fin(UP)
            pre = jnp.maximum(jnp.dot(both(X, s1, s2), weight(UP), preferred_element_type=F32), 0.0)
            for n, slot in enumerate((s1, s2)):
                v = pre[n * tokens:(n + 1) * tokens]
                RP[slot] = v
                ACT[slot] = (v * v).astype(BF)

        def pull_back(n):
            s1, s2 = 2 * n, 2 * n + 1
            fin(DN)
            back = jnp.dot(both(C, s1, s2), weight(DN), preferred_element_type=F32)
            for n, slot in enumerate((s1, s2)):
                GP[slot] = (2.0 * RP[slot] * back[n * tokens:(n + 1) * tokens]).astype(BF)

        lhs_of = (XT, CT)
        rhs_of = (GP, ACT)

        def gblk(w, h, a, b):
            z = j if h == 0 else 1 - j
            return G.at[w, z, a, b] if h == 0 else G.at[w, z, b, a]

        def raxes(h):
            return (y, x, ydev, xdev) if h == 0 else (x, y, xdev, ydev)

        def product(w, h, lo, n):
            z = j if h == 0 else 1 - j
            left = lhs_of[w][z, :, :, :, lo * tokens:(lo + n) * tokens].reshape(width // 2, n * tokens)
            right = rhs_of[w][lo:lo + n].reshape(n * tokens, cols)
            out = jnp.dot(left, right, preferred_element_type=F32)
            return G.at[w, z], out.reshape(4, 4, width // 32, cols)

        begun = set()

        def multiply_early(w, h):
            ref, out = product(w, h, 0, 2)
            ref[...] = out
            begun.add((w, h))

        def multiply(w, h):
            if (w, h) in begun:
                ref, out = product(w, h, 2, 2)
                ref[...] = ref[...] + out
            else:
                ref, out = product(w, h, 0, 4)
                ref[...] = out

        def tiles(rows):
            return [(n, pl.ds(16 * (n % (rows // 16)), 16), lanes[n // (rows // 16)])
                    for n in range(rows // 16 * len(lanes))]

        def encode(src, dst, steps=3):
            every = tiles(src.shape[0])
            top = None
            for _, q, c in every:
                m = jnp.abs(src[q, c])
                top = m if top is None else jnp.maximum(top, m)
            top = jnp.maximum(top, 2e-34).astype(BF)
            dst[len(every)] = top
            inv = 2.0 ** (120 >> steps) / top.astype(F32)
            for n, q, c in every:
                v = src[q, c] * inv
                for _ in range(steps):
                    v = v * jnp.abs(v)
                dst[n] = v.astype(BF)

        def decoder(buf, rows, steps=3):
            every = tiles(rows)
            unit = buf[len(every)].astype(F32) * 0.5 ** (120 >> steps)

            def tile(n):
                v = buf[n].astype(F32)
                m = jnp.exp2(jnp.log2(jnp.abs(v)) * 0.5 ** steps)
                return jnp.where(v < 0, -m, m) * unit
            return every, tile

        def add(ref, buf):
            every, tile = decoder(buf, ref.shape[0])
            for n, q, c in every:
                ref[q, c] = ref[q, c] + tile(n)

        class Ring:
            def __init__(self, stage, w, h, pos, dev, parts, bufs, subs):
                self.k = (stage, w, h)
                self.subs = subs
                self.pos, self.dev, self.parts = pos, dev, parts
                self.sb, self.rb = (b.at[2 * w + h] for b in bufs)

            def post(self, i, srcs, d, lo, n, group):
                for m in range(lo, lo + n):
                    encode(srcs[m], self.sb.at[i, m])
                some = pl.ds(lo, n)
                send(self.k + group, self.sb.at[i, some], self.rb.at[i, some], self.dev(d), self.k)

            def far(self, lo=0):
                self.post(0, self.parts(at(self.pos, 2), 0), 1, lo, 1, ("far", 0, lo))
                self.post(1, self.parts(at(self.pos, 2), 1), 3, lo, 1, ("far", 1, lo))

            def near_right(self):
                self.post(2, self.parts(at(self.pos, 1), 1), 1, 0, self.subs, ("near",))

            def near_left(self):
                self.post(3, self.parts(at(self.pos, 3), 0), 3, 0, self.subs, ("near",))

            def relay(self, side, lo=0):
                p = self.parts(at(self.pos, (1, 3)[side]), side)
                recv(self.k + ("far", side, lo), self.rb.at[side, pl.ds(lo, 1)])
                add(p[lo], self.rb.at[side, lo])
                self.post(4 + side, p, (1, 3)[side], lo, 1, ("last", lo))

            def near_in(self):
                recv(self.k + ("near",), self.rb.at[pl.ds(2, 2)])
                for m in range(self.subs):
                    add(self.parts(self.pos, 0)[m], self.rb.at[3, m])
                    add(self.parts(self.pos, 1)[m], self.rb.at[2, m])

            def last_in(self):
                for m in range(self.subs):
                    recv(self.k + ("last", m), self.rb.at[pl.ds(4, 2), m])
                    add(self.parts(self.pos, 0)[m], self.rb.at[4, m])
                    add(self.parts(self.pos, 1)[m], self.rb.at[5, m])

        def ring1(w, h):
            a, b, adev, bdev = raxes(h)
            return Ring(1, w, h, a, adev,
                        lambda place, side: [gblk(w, h, place, 2 * side + i) for i in (0, 1)],
                        (s1s, s1r), 2)

        hr = width // 64

        def ring2(w, h):
            a, b, adev, bdev = raxes(h)
            return Ring(2, w, h, b, bdev,
                        lambda place, side: [gblk(w, h, a, place).at[pl.ds(side * hr, hr)]],
                        (s2s, s2r), 1)

        first = {(w, h): ring1(w, h) for w in (UP, DN) for h in (0, 1)}
        second = {(w, h): ring2(w, h) for w in (UP, DN) for h in (0, 1)}

        def second_start(w, h):
            first[w, h].last_in()
            second[w, h].far()
            second[w, h].near_right()
            second[w, h].near_left()

        def third_start(w, h):
            second[w, h].near_in()
            second[w, h].last_in()
            a, b, _, _ = raxes(h)
            encode(gblk(w, h, a, b), s3s.at[w, h])
            peers_ = [(0, rpeer)] if h == 0 else [(1, zpeer), (2, rzpeer)]
            for i, dev in peers_:
                send((5, w), s3s.at[w, h], s3r.at[w, i], dev, (5, w))

        def finish(w):
            out = (gup_ref, gdn_ref)[w]
            recv((5, w), s3r.at[w])
            for side, one, two in ((j, s3s.at[w, 0], s3r.at[w, 0]), (1 - j, s3r.at[w, 1], s3r.at[w, 2])):
                every, tile1 = decoder(one, width // 32)
                _, tile2 = decoder(two, width // 32)
                for n, q, c in every:
                    col = pl.ds(pl.multiple_of(side * cols + n // (width // 512) * 128, 128), 128)
                    out[q, col] = (tile1(n) + tile2(n)) * factor

        def input_part(n):
            s1, s2 = ((3, 1), (2, 0))[n]
            w = W[UP].reshape(width, cols)
            v = lax.dot_general(both(GP, s1, s2), w, (((1,), (1,)), ((), ())), preferred_element_type=F32)
            PART[s1] = v[:tokens]
            PART[s2] = v[tokens:]
            if n == 0:
                for i, slot in enumerate((3, 1)):
                    send(("g", "t", i), PART.at[slot], DR.at[i], tpeer, "gt")

        def input_send():
            recv(("g", "t", 0), DR.at[0])
            PART[2] = PART[2] + DR[0]
            encode(PART.at[2], ZS, 4)
            send("gz", ZS, ZR, zpeer, "gz")

        def input_sum():
            recv(("g", "t", 1), DR.at[1])
            recv("gz", ZR)
            every, tile = decoder(ZR, tokens, 4)
            for n, q, c in every:
                gin_ref[q, c] = (PART[0, q, c] + DR[1, q, c] + tile(n)).astype(BF)

        def energy_x():
            EX[x] = jnp.sum(gdn_ref[...] * gdn_ref[...], axis=0, keepdims=True)
            for d in (1, 2, 3):
                send("ex", EX.at[x], EX.at[x], xdev(d), "ex")

        def energy_y():
            recv("ex", EX.at[pl.ds(0, 3)])
            me = 4 * j + y
            EY[me] = EX[0] + EX[1] + EX[2] + EX[3]
            for dev in [zpeer] + [f(d) for d in (1, 2, 3) for f in (ydev, yzdev)]:
                send("ey", EY.at[me], EY.at[me], dev, "ey")

        def energy_down():
            recv("ey", EY.at[pl.ds(0, 7)])
            total = EY[0]
            for n in range(1, 8):
                total = total + EY[n]
            edn_ref[...] = total * (1.0 / width)

        def energy_pair():
            total = None
            for c in range(2 * len(lanes)):
                v = gup_ref[:, c * 128:(c + 1) * 128]
                total = v * v if total is None else total + v * v
            EU[0] = total
            send("et", EU.at[0], EU.at[1], tpeer, "et")

        def energy_up():
            recv("et", EU.at[1])
            eup_ref[...] = jnp.sum((EU[0] + EU[1]).T, axis=0, keepdims=True) * (1.0 / ff)

        for w in (UP, DN):
            loads[w].wait()
            send(("a2a", w), OTH.at[w], W.at[w, j, y, x], rzpeer, "a2a")
        for c in loads[2:]:
            c.wait()
        for name in ("x", "c"):
            buf = stock[name][0]
            for i in (0, 1):
                rows = pl.ds(i * half, half)
                send((name, "z", i), buf.at[0, rows], buf.at[2, rows], zpeer, name)
            send((name, "t"), buf.at[0], buf.at[1], tpeer, name)
        todo = {
            "init": init, "near": near, "step2": step2, "fwd": fwd, "pass": pass_on, "turn": turn,
            "proj": project, "pull": pull_back, "mult": multiply, "ma": multiply_early,
            "far": lambda w, h, lo: first[w, h].far(lo),
            "nr": lambda w, h: first[w, h].near_right(),
            "nl": lambda w, h: first[w, h].near_left(),
            "rl": lambda w, h, side, lo: first[w, h].relay(side, lo),
            "ni": lambda w, h: first[w, h].near_in(),
            "st2": second_start,
            "rl2": lambda w, h, side: second[w, h].relay(side),
            "st3": third_start, "fin": finish, "ip": input_part, "gz": input_send, "gin": input_sum,
            "ex": energy_x, "ey": energy_y, "edn": energy_down,
            "eu": energy_pair, "eup": energy_up,
        }
        for name, *where in ORDER:
            todo[name](*where)
        sent("a2a", OTH)
        for n, name in enumerate(("x", "c")):
            sent(name, RP.at[0])
            sent((name, "zt"), X.at[0])
            for h in (0, 1):
                sent((n, h), RP.at[0, pl.ds(0, 15 * tokens // 16)])
                sent((1, n, h), s1s.at[0])
                sent((2, n, h), s2s.at[0])
            sent((5, n), s3r.at[0])
        sent("gt", PART.at[pl.ds(0, 2)])
        sent("gz", ZS)
        sent("ex", EX.at[pl.ds(0, 3)])
        sent("ey", EY.at[pl.ds(0, 7)])
        sent("et", EU.at[0])

    return kernel


def hand_over(results):
    vm = pl.BlockSpec(memory_space=pltpu.VMEM)
    shapes = [jax.ShapeDtypeStruct(v.shape, v.dtype) for v in results]

    def kernel(*refs):
        sem = refs[10]
        moves = [pltpu.make_async_copy(refs[n], refs[5 + n], sem.at[n]) for n in range(5)]
        for c in moves:
            c.start()
        for c in moves:
            c.wait()

    return pl.pallas_call(kernel, out_shape=tuple(shapes), in_specs=[vm] * 5, out_specs=(pl.BlockSpec(memory_space=pltpu.HBM),) * 5,
        scratch_shapes=[pltpu.SemaphoreType.DMA((5,))],
    )(*[pltpu.with_memory_space_constraint(v, pltpu.VMEM) for v in results])


def per_device(inputs, up_proj, down_proj, out_cotangent):
    tokens, width = inputs.shape
    rows, hidden = up_proj.shape
    cols = hidden // 2
    ff = hidden * lax.axis_size("tp")
    all_tokens = tokens * lax.axis_size("rep") * lax.axis_size(FS) * lax.axis_size("tp")
    factor = float(all_tokens) ** (-0.5)
    up3 = up_proj.reshape(2, rows // 2, hidden)
    dn3 = down_proj.T.reshape(2, rows // 2, hidden)
    vm = pl.BlockSpec(memory_space=pltpu.VMEM)
    full = (2, 4, 4, rows)
    lines = rows * cols // 2048
    results = pl.pallas_call(
        make_kernel(tokens, width, cols, ff, factor),
        out_shape=(
            pltpu.VMEM((tokens, width), BF),
            pltpu.VMEM((rows, hidden), F32),
            pltpu.VMEM((rows, hidden), F32),
            pltpu.VMEM((1, rows), F32),
            pltpu.VMEM((1, hidden), F32),
        ),
        in_specs=[pl.BlockSpec(memory_space=pltpu.HBM)] * 4,
        out_specs=(vm,) * 5,
        scratch_shapes=[
            pltpu.VMEM((4, tokens, width), BF),
            pltpu.VMEM((4, tokens, width), BF),
            pltpu.VMEM(full + (4 * tokens,), BF),
            pltpu.VMEM(full + (4 * tokens,), BF),
            pltpu.VMEM((2, 2, 4, 4, 2, rows // 2, cols), BF),
            pltpu.VMEM((4, tokens, cols), F32),
            pltpu.VMEM((4, tokens, cols), BF),
            pltpu.VMEM((4, tokens, cols), BF),
            pltpu.VMEM((2,) + full + (cols,), F32),
            pltpu.VMEM((4, 6, 2, lines + 1, 16, 128), BF),
            pltpu.VMEM((4, 6, 2, lines + 1, 16, 128), BF),
            pltpu.VMEM((4, 6, 1, lines // 2 + 1, 16, 128), BF),
            pltpu.VMEM((4, 6, 1, lines // 2 + 1, 16, 128), BF),
            pltpu.VMEM((2, 2, lines + 1, 16, 128), BF),
            pltpu.VMEM((2, 3, lines + 1, 16, 128), BF),
            pltpu.VMEM((4, tokens, width), F32),
            pltpu.VMEM((2, tokens, width), F32),
            pltpu.VMEM((tokens * width // 2048 + 1, 16, 128), BF),
            pltpu.VMEM((tokens * width // 2048 + 1, 16, 128), BF),
            pltpu.VMEM((4, 1, hidden), F32),
            pltpu.VMEM((8, 1, hidden), F32),
            pltpu.VMEM((2, rows, 128), F32),
            pltpu.VMEM((2, 2, rows // 2, cols), BF),
            pltpu.SemaphoreType.DMA((BATCHES,)),
            pltpu.SemaphoreType.DMA((WAITS,)),
            pltpu.SemaphoreType.DMA((6,)),
        ],
        compiler_params=pltpu.CompilerParams(
            collective_id=0, has_side_effects=True, vmem_limit_bytes=52 * 1024 * 1024
        ),
    )(*[pltpu.with_memory_space_constraint(v, pltpu.HBM) for v in (inputs, up3, dn3, out_cotangent)])
    gin, gup, gdn, eup, edn = hand_over(results)
    return gin, gup, gdn.T, eup.reshape(rows), edn.reshape(hidden)


def solution(mesh):
    torus = Mesh(
        mesh.devices.reshape(mesh.shape["rep"], 2, 4, 4, mesh.shape["tp"]),
        ("rep", "fs_0", "fs_1", "fs_2", "tp"),
    )
    placed = (P(REP_FS_TP, None), P(FS, "tp"), P("tp", FS), P(REP_FS_TP, None))
    return jax.shard_map(
        per_device,
        mesh=torus,
        in_specs=placed,
        out_specs=(P(REP_FS_TP, None), P(FS, "tp"), P("tp", FS), P(FS), P("tp")),
        check_vma=False,
    )
```

```python
import jax
import jax.numpy as jnp
from jax import lax
from jax.experimental import pallas as pl
from jax.experimental.pallas import tpu as pltpu
from jax.sharding import Mesh
from jax.sharding import PartitionSpec as P

FS = ("fs_0", "fs_1", "fs_2")
REP_FS_TP = ("rep", "fs_0", "fs_1", "fs_2", "tp")
MESH = pl.DeviceIdType.MESH
BF = jnp.bfloat16
F32 = jnp.float32
RIGHT, LEFT = 0, 1
UP, DN = 0, 1
WAITS, BATCHES = 118, 32


ORDER = [
    ("init", 1, 0), ("init", 0, 0), ("init", 0, 1), ("init", 1, 1), ("near", 0, 0, 0), ("near", 0, 0, 1),
    ("near", 0, 1, 0), ("near", 0, 1, 1), ("near", 1, 0, 1), ("near", 1, 0, 0), ("near", 1, 1, 0),
    ("step2", 0, 1), ("fwd", 1, 0, 0, 1), ("step2", 0, 0), ("turn", "c", 0), ("fwd", 0, 0, 0, 1),
    ("near", 1, 1, 1), ("fwd", 0, 1, 1, 1), ("fwd", 0, 1, 1, 0), ("pass", "x", 0), ("fwd", 0, 1, 2, 1),
    ("fwd", 0, 1, 0, 1), ("fwd", 0, 0, 1, 1), ("fwd", 1, 0, 2, 0), ("fwd", 0, 0, 1, 0), ("pass", "x", 1),
    ("turn", "x", 0), ("fwd", 0, 0, 2, 0), ("turn", "x", 1), ("turn", "c", 1), ("fwd", 0, 1, 2, 0),
    ("fwd", 0, 0, 2, 1), ("turn", "x", 3), ("fwd", 0, 1, 0, 0), ("step2", 1, 0), ("fwd", 0, 0, 3, 0),
    ("fwd", 1, 1, 0, 1), ("fwd", 0, 1, 3, 0), ("turn", "x", 2), ("fwd", 0, 1, 3, 1), ("fwd", 1, 1, 2, 0),
    ("fwd", 0, 0, 3, 1), ("pass", "c", 0), ("fwd", 1, 0, 2, 1), ("fwd", 1, 0, 1, 1), ("step2", 1, 1),
    ("fwd", 1, 1, 1, 0), ("fwd", 0, 0, 0, 0), ("proj", 0), ("fwd", 1, 1, 3, 0), ("fwd", 1, 0, 3, 1),
    ("fwd", 1, 1, 0, 0), ("ma", 1, 0), ("fwd", 1, 1, 3, 1), ("fwd", 1, 1, 1, 1), ("fwd", 1, 0, 3, 0),
    ("pass", "c", 1), ("fwd", 1, 0, 1, 0), ("fwd", 1, 0, 0, 0), ("fwd", 1, 1, 2, 1), ("turn", "c", 2),
    ("ma", 1, 1), ("proj", 1), ("turn", "c", 3), ("mult", 1, 1), ("far", 1, 1, 0), ("mult", 1, 0),
    ("far", 1, 0, 0), ("far", 1, 1, 1), ("pull", 1), ("pull", 0), ("nr", 1, 1, 0), ("nr", 1, 0, 1),
    ("nl", 1, 0, 1), ("ip", 0), ("far", 1, 0, 1), ("nl", 1, 1, 1), ("mult", 0, 1), ("nl", 0, 1, 1),
    ("nr", 1, 1, 1), ("rl", 1, 0, 0, 0), ("nl", 1, 0, 0), ("nr", 1, 0, 0), ("far", 0, 1, 0), ("rl", 1, 0, 1, 0),
    ("rl", 1, 1, 0, 0), ("rl", 1, 1, 0, 1), ("mult", 0, 0), ("ip", 1), ("nl", 1, 1, 0), ("rl", 1, 0, 1, 1),
    ("rl", 1, 0, 0, 1), ("rl", 1, 1, 1, 1), ("nr", 0, 1, 1), ("gz",), ("nl", 0, 0, 0), ("far", 0, 0, 1),
    ("nl", 0, 0, 1), ("rl", 1, 1, 1, 0), ("nr", 0, 0, 0), ("ni", 1, 0, 1), ("ni", 1, 0, 0), ("st2", 1, 0),
    ("nr", 0, 0, 1), ("ni", 1, 1, 1), ("far", 0, 1, 1), ("nr", 0, 1, 0), ("rl", 0, 1, 1, 0), ("ni", 1, 1, 0),
    ("far", 0, 0, 0), ("ni", 0, 0, 0), ("st2", 1, 1), ("rl", 0, 0, 1, 1), ("rl", 0, 0, 0, 1), ("rl2", 1, 0, 0),
    ("rl", 0, 1, 0, 0), ("rl2", 1, 0, 1), ("rl", 0, 1, 0, 1), ("rl2", 1, 1, 1), ("nl", 0, 1, 0), ("ni", 0, 0, 1),
    ("rl2", 1, 1, 0), ("ni", 0, 1, 1), ("rl", 0, 0, 1, 0), ("rl", 0, 0, 0, 0), ("st3", 1, 0), ("rl", 0, 1, 1, 1),
    ("st2", 0, 0, 1), ("ni", 0, 1, 0), ("st3", 1, 1), ("st2", 0, 1, 0), ("st2", 0, 1, 1), ("st2", 0, 0, 0),
    ("st3", 0, 0, 1), ("fin", 1), ("ex",), ("gin",), ("st3", 0, 1, 0), ("st3", 0, 0, 0), ("st3", 0, 1, 1),
    ("ey",), ("fin", 0, 0), ("fin", 0, 1), ("eu",), ("eup",), ("edn",),
]


def make_kernel(tokens, width, cols, ff, factor):
    lanes = [pl.ds(c * 128, 128) for c in range(cols // 128)]

    def kernel(
        x_ref, up_ref, dn_ref, cot_ref,
        gin_ref, gup_ref, gdn_ref, eup_ref, edn_ref,
        X, C, XT, CT, W, RP, ACT, GP, G,
        s1s, s1r, s2s, s2r, d2s, d2r, s3s, s3r, u3s, u3r,
        PART, DR, ZS, ZR, EX, EY, EU,
        OTH, ssem, rsem, lsem,
    ):
        r = lax.axis_index("rep")
        j = lax.axis_index("fs_0")
        y = lax.axis_index("fs_1")
        x = lax.axis_index("fs_2")
        t = lax.axis_index("tp")

        def at(pos, d):
            return lax.rem(pos + d, 4)

        def xdev(d):
            return {"fs_2": at(x, d)}

        def ydev(d):
            return {"fs_1": at(y, d)}

        def yzdev(d):
            return {"fs_0": 1 - j, "fs_1": at(y, d)}

        zpeer = {"fs_0": 1 - j}
        rpeer = {"rep": 1 - r}
        rzpeer = {"rep": 1 - r, "fs_0": 1 - j}
        tpeer = {"tp": 1 - t}

        own = pl.ds(pl.multiple_of(j * cols, cols), cols)
        other = pl.ds(pl.multiple_of((1 - j) * cols, cols), cols)
        loads = [
            pltpu.make_async_copy(up_ref.at[:, :, other], OTH.at[UP], lsem.at[0]),
            pltpu.make_async_copy(dn_ref.at[:, :, other], OTH.at[DN], lsem.at[1]),
            pltpu.make_async_copy(up_ref.at[:, :, own], W.at[UP, j, y, x], lsem.at[2]),
            pltpu.make_async_copy(dn_ref.at[:, :, own], W.at[DN, j, y, x], lsem.at[3]),
            pltpu.make_async_copy(x_ref, X.at[0], lsem.at[4]),
            pltpu.make_async_copy(cot_ref, C.at[0], lsem.at[5]),
        ]
        for c in loads:
            c.start()

        barrier = pltpu.get_barrier_semaphore()
        peers = [xdev(1), xdev(2), xdev(3), ydev(1), ydev(2), ydev(3), zpeer, rpeer, rzpeer, tpeer, yzdev(1), yzdev(2), yzdev(3)]
        for dev in peers:
            pl.semaphore_signal(barrier, inc=1, device_id=dev, device_id_type=MESH)
        pl.semaphore_wait(barrier, len(peers))

        arrivals, departures = {}, {}

        def slot_of(table, group):
            return table.setdefault(group, len(table))

        def send(group, src, dst, dev, batch):
            pltpu.make_async_remote_copy(
                src_ref=src, dst_ref=dst,
                send_sem=ssem.at[slot_of(departures, batch)], recv_sem=rsem.at[slot_of(arrivals, group)],
                device_id=dev, device_id_type=MESH,
            ).start()

        def recv(group, ref):
            pltpu.make_async_copy(ref, ref, rsem.at[arrivals[group]]).wait()

        def sent(batch, ref):
            pltpu.make_async_copy(ref, ref, ssem.at[departures[batch]]).wait()

        half = tokens // 2

        def blk(ref, w, h, a, b):
            z = j if h == 0 else 1 - j
            return ref.at[w, z, b, a] if h == 0 else ref.at[w, z, a, b]

        def axes(h):
            return (x, y, xdev, ydev) if h == 0 else (y, x, ydev, xdev)

        def init(w, h):
            a, b, adev, bdev = axes(h)
            ref = blk(W, w, h, a, b)
            if h == 1:
                recv(("a2a", w), ref)
            send((1, w, h, 0), ref, ref, adev(1), (w, h))
            send((1, w, h, 1), ref, ref, adev(3), (w, h))
            spread(w, h, 0, a)

        def spread(w, h, s, a2):
            _, b, _, bdev = axes(h)
            ref = blk(W, w, h, a2, b)
            send((2, w, h, s, 0), ref, ref, bdev(1), (w, h))
            send((2, w, h, s, 1), ref, ref, bdev(3), (w, h))

        def near(w, h, side):
            a, b, adev, _ = axes(h)
            place, away = ((at(a, 3), 1), (at(a, 1), 3))[side]
            ref = blk(W, w, h, place, b)
            recv((1, w, h, side), ref)
            send((1, w, h, 2), ref.at[side], ref.at[side], adev(away), (w, h))
            spread(w, h, 1 + side, place)

        def step2(w, h):
            a, b, _, _ = axes(h)
            recv((1, w, h, 2), blk(W, w, h, at(a, 2), b))
            spread(w, h, 3, at(a, 2))

        def fwd(w, h, s, side):
            a, b, _, bdev = axes(h)
            a2 = at(a, (0, 3, 1, 2)[s])
            place, away = ((at(b, 3), 1), (at(b, 1), 3))[side]
            ref = blk(W, w, h, a2, place)
            recv((2, w, h, s, side), ref)
            send((3, w), ref.at[side], ref.at[side], bdev(away), (w, h))

        whole = set()

        def fin(w):
            if w not in whole:
                whole.add(w)
                recv((3, w), W.at[w, 0, pl.ds(0, 2)])

        stock = {"x": (X, XT), "c": (C, CT)}

        def pass_on(name, i):
            rows = pl.ds(i * half, half)
            buf = stock[name][0]
            recv((name, "z", i), buf.at[2, rows])
            send((name, "zt"), buf.at[2, rows], buf.at[3, rows], tpeer, (name, "zt"))

        def turn(name, slot):
            src, dst = stock[name]
            if slot == 1:
                recv((name, "t"), src.at[1])
            if slot == 3:
                recv((name, "zt"), src.at[3])
            v = src[slot].T
            dst[:, :, :, :, slot * tokens:(slot + 1) * tokens] = v.reshape(2, 4, 4, width // 32, tokens)

        def weight(w):
            return W[w].reshape(width, cols)

        def both(ref, s1, s2):
            return jnp.concatenate([ref[s1], ref[s2]], axis=0)

        def project(n):
            s1, s2 = 2 * n, 2 * n + 1
            fin(UP)
            pre = jnp.maximum(jnp.dot(both(X, s1, s2), weight(UP), preferred_element_type=F32), 0.0)
            for n, slot in enumerate((s1, s2)):
                v = pre[n * tokens:(n + 1) * tokens]
                RP[slot] = v
                ACT[slot] = (v * v).astype(BF)

        def pull_back(n):
            s1, s2 = 2 * n, 2 * n + 1
            fin(DN)
            back = jnp.dot(both(C, s1, s2), weight(DN), preferred_element_type=F32)
            for n, slot in enumerate((s1, s2)):
                GP[slot] = (2.0 * RP[slot] * back[n * tokens:(n + 1) * tokens]).astype(BF)

        lhs_of = (XT, CT)
        rhs_of = (GP, ACT)

        def gblk(w, h, a, b):
            z = j if h == 0 else 1 - j
            return G.at[w, z, a, b] if h == 0 else G.at[w, z, b, a]

        def raxes(h):
            return (y, x, ydev, xdev) if h == 0 else (x, y, xdev, ydev)

        def product(w, h, lo, n):
            z = j if h == 0 else 1 - j
            left = lhs_of[w][z, :, :, :, lo * tokens:(lo + n) * tokens].reshape(width // 2, n * tokens)
            right = rhs_of[w][lo:lo + n].reshape(n * tokens, cols)
            out = jnp.dot(left, right, preferred_element_type=F32)
            return G.at[w, z], out.reshape(4, 4, width // 32, cols)

        begun = set()

        def multiply_early(w, h):
            ref, out = product(w, h, 0, 2)
            ref[...] = out
            begun.add((w, h))

        def multiply(w, h):
            if (w, h) in begun:
                ref, out = product(w, h, 2, 2)
                ref[...] = ref[...] + out
            else:
                ref, out = product(w, h, 0, 4)
                ref[...] = out

        def tiles(refs):
            every = []
            for m, ref in enumerate(refs):
                rows, wide = ref.shape
                for c in range(wide // 128):
                    for q in range(rows // 16):
                        every.append((len(every), m, pl.ds(16 * q, 16), pl.ds(128 * c, 128)))
            return every

        def encode(refs, dst, steps=3):
            every = tiles(refs)
            top = None
            for _, m, q, c in every:
                v = jnp.abs(refs[m][q, c])
                top = v if top is None else jnp.maximum(top, v)
            top = jnp.maximum(top, 2e-34).astype(BF)
            dst[len(every)] = top
            inv = 2.0 ** (120 >> steps) / top.astype(F32)
            for n, m, q, c in every:
                v = refs[m][q, c] * inv
                for _ in range(steps):
                    v = v * jnp.abs(v)
                dst[n] = v.astype(BF)

        def decoder(buf, refs, steps=3):
            every = tiles(refs)
            unit = buf[len(every)].astype(F32) * 0.5 ** (120 >> steps)

            def tile(n):
                v = buf[n].astype(F32)
                m = jnp.exp2(jnp.log2(jnp.abs(v)) * 0.5 ** steps)
                return jnp.where(v < 0, -m, m) * unit
            return every, tile

        def add(refs, buf):
            every, tile = decoder(buf, refs)
            for n, m, q, c in every:
                refs[m][q, c] = refs[m][q, c] + tile(n)

        class Ring:
            def __init__(self, key, pos, dev, parts, sb, rb):
                self.k, self.pos, self.dev, self.parts, self.sb, self.rb = key, pos, dev, parts, sb, rb

            def post(self, i, place, side, d, group):
                encode(self.parts(place, side), self.sb.at[i])
                send(self.k + group, self.sb.at[i], self.rb.at[i], self.dev(d), self.k)

            def far(self):
                self.post(0, at(self.pos, 2), 0, 1, ("far", 0))
                self.post(1, at(self.pos, 2), 1, 3, ("far", 1))

            def near_right(self):
                self.post(2, at(self.pos, 1), 1, 1, ("near",))

            def near_left(self):
                self.post(3, at(self.pos, 3), 0, 3, ("near",))

            def relay(self, side):
                place, d = at(self.pos, (1, 3)[side]), (1, 3)[side]
                recv(self.k + ("far", side), self.rb.at[side])
                add(self.parts(place, side), self.rb.at[side])
                self.post(4 + side, place, side, d, ("last",))

            def near_in(self):
                recv(self.k + ("near",), self.rb.at[pl.ds(2, 2)])
                add(self.parts(self.pos, 0), self.rb.at[3])
                add(self.parts(self.pos, 1), self.rb.at[2])

            def last_in(self):
                recv(self.k + ("last",), self.rb.at[pl.ds(4, 2)])
                add(self.parts(self.pos, 0), self.rb.at[4])
                add(self.parts(self.pos, 1), self.rb.at[5])

        wing = cols // 2
        hr = width // 64

        def ring1(w, h, c):
            a, _, adev, _ = raxes(h)
            return Ring((1, w, h, c), a, adev,
                        lambda place, side: [gblk(w, h, place, 2 * side + i).at[:, pl.ds(c * wing, wing)] for i in (0, 1)],
                        s1s.at[2 * w + h, c], s1r.at[2 * w + h, c])

        def ring2(h):
            a, b, _, bdev = raxes(h)
            return Ring((2, DN, h), b, bdev,
                        lambda place, side: [gblk(DN, h, a, place).at[pl.ds(side * hr, hr)]],
                        s2s.at[h], s2r.at[h])

        first = {(w, h, c): ring1(w, h, c) for w in (UP, DN) for h in (0, 1) for c in (0, 1)}
        second = [ring2(h) for h in (0, 1)]

        def part(h, c, place):
            return gblk(UP, h, raxes(h)[0], place).at[:, pl.ds(c * wing, wing)]

        def second_start(w, h, c=None):
            if w == DN:
                for c in (0, 1):
                    first[w, h, c].last_in()
                second[h].far()
                second[h].near_right()
                second[h].near_left()
                return
            first[w, h, c].last_in()
            _, b, _, bdev = raxes(h)
            for d in (2, 1, 3):
                encode([part(h, c, at(b, d))], d2s.at[h, c, d - 1])
                send(("d2", h, c), d2s.at[h, c, d - 1], d2r.at[h, c, d - 1], bdev(d), ("d2", h, c))

        def third_start(w, h, c=None):
            a, b, _, _ = raxes(h)
            peers_ = [(0, rpeer)] if h == 0 else [(1, zpeer), (2, rzpeer)]
            if w == DN:
                second[h].near_in()
                second[h].last_in()
                encode([gblk(w, h, a, b)], s3s.at[h])
                for i, dev in peers_:
                    send((5, w), s3s.at[h], s3r.at[i], dev, (5, w))
                return
            recv(("d2", h, c), d2r.at[h, c])
            for d in range(3):
                add([part(h, c, b)], d2r.at[h, c, d])
            encode([part(h, c, b)], u3s.at[c, h])
            for i, dev in peers_:
                send((5, w, c), u3s.at[c, h], u3r.at[c, i], dev, (5, w, c))

        def finish(w, c=None):
            if w == DN:
                out, mine, theirs, at_, wide = gdn_ref, s3s, s3r, 0, cols
                recv((5, w), s3r)
            else:
                out, mine, theirs, at_, wide = gup_ref, u3s.at[c], u3r.at[c], c * wing, wing
                recv((5, w, c), u3r.at[c])
            for side, one, two in ((j, mine.at[0], theirs.at[0]), (1 - j, theirs.at[1], theirs.at[2])):
                like = [out.at[:, pl.ds(0, wide)]]
                every, tile1 = decoder(one, like)
                _, tile2 = decoder(two, like)
                for n, _, q, _ in every:
                    col = pl.ds(pl.multiple_of(side * cols + at_ + n // (width // 512) * 128, 128), 128)
                    out[q, col] = (tile1(n) + tile2(n)) * factor

        def input_part(n):
            s1, s2 = ((3, 1), (2, 0))[n]
            w = W[UP].reshape(width, cols)
            v = lax.dot_general(both(GP, s1, s2), w, (((1,), (1,)), ((), ())), preferred_element_type=F32)
            PART[s1] = v[:tokens]
            PART[s2] = v[tokens:]
            if n == 0:
                for i, slot in enumerate((3, 1)):
                    send(("g", "t", i), PART.at[slot], DR.at[i], tpeer, "gt")

        def input_send():
            recv(("g", "t", 0), DR.at[0])
            PART[2] = PART[2] + DR[0]
            encode([PART.at[2]], ZS, 4)
            send("gz", ZS, ZR, zpeer, "gz")

        def input_sum():
            recv(("g", "t", 1), DR.at[1])
            recv("gz", ZR)
            every, tile = decoder(ZR, [PART.at[2]], 4)
            for n, _, q, c in every:
                gin_ref[q, c] = (PART[0, q, c] + DR[1, q, c] + tile(n)).astype(BF)

        def energy_x():
            EX[x] = jnp.sum(gdn_ref[...] * gdn_ref[...], axis=0, keepdims=True)
            for d in (1, 2, 3):
                send("ex", EX.at[x], EX.at[x], xdev(d), "ex")

        def energy_y():
            recv("ex", EX.at[pl.ds(0, 3)])
            me = 4 * j + y
            EY[me] = EX[0] + EX[1] + EX[2] + EX[3]
            for dev in [zpeer] + [f(d) for d in (1, 2, 3) for f in (ydev, yzdev)]:
                send("ey", EY.at[me], EY.at[me], dev, "ey")

        def energy_down():
            recv("ey", EY.at[pl.ds(0, 7)])
            total = EY[0]
            for n in range(1, 8):
                total = total + EY[n]
            edn_ref[...] = total * (1.0 / width)

        def energy_pair():
            total = None
            for c in range(2 * len(lanes)):
                v = gup_ref[:, c * 128:(c + 1) * 128]
                total = v * v if total is None else total + v * v
            EU[0] = total
            send("et", EU.at[0], EU.at[1], tpeer, "et")

        def energy_up():
            recv("et", EU.at[1])
            eup_ref[...] = jnp.sum((EU[0] + EU[1]).T, axis=0, keepdims=True) * (1.0 / ff)

        for w in (UP, DN):
            loads[w].wait()
            send(("a2a", w), OTH.at[w], W.at[w, j, y, x], rzpeer, "a2a")
        for c in loads[2:]:
            c.wait()
        for name in ("x", "c"):
            buf = stock[name][0]
            for i in (0, 1):
                rows = pl.ds(i * half, half)
                send((name, "z", i), buf.at[0, rows], buf.at[2, rows], zpeer, name)
            send((name, "t"), buf.at[0], buf.at[1], tpeer, name)
        todo = {
            "init": init, "near": near, "step2": step2, "fwd": fwd, "pass": pass_on, "turn": turn,
            "proj": project, "pull": pull_back, "mult": multiply, "ma": multiply_early,
            "far": lambda w, h, c: first[w, h, c].far(),
            "nr": lambda w, h, c: first[w, h, c].near_right(),
            "nl": lambda w, h, c: first[w, h, c].near_left(),
            "rl": lambda w, h, side, c: first[w, h, c].relay(side),
            "ni": lambda w, h, c: first[w, h, c].near_in(),
            "st2": second_start,
            "rl2": lambda w, h, side: second[h].relay(side),
            "st3": third_start, "fin": finish, "ip": input_part, "gz": input_send, "gin": input_sum,
            "ex": energy_x, "ey": energy_y, "edn": energy_down,
            "eu": energy_pair, "eup": energy_up,
        }
        for name, *where in ORDER:
            todo[name](*where)
        sent("a2a", OTH)
        for n, name in enumerate(("x", "c")):
            sent(name, RP.at[0])
            sent((name, "zt"), X.at[0])
            for h in (0, 1):
                sent((n, h), RP.at[0, pl.ds(0, 15 * tokens // 16)])
                for c in (0, 1):
                    sent((1, n, h, c), s1s.at[0, 0])
                    if n == UP:
                        sent(("d2", h, c), d2s.at[0, 0])
                if n == DN:
                    sent((2, n, h), s2s.at[0])
        sent((5, DN), s3r)
        for c in (0, 1):
            sent((5, UP, c), u3r.at[0])
        sent("gt", PART.at[pl.ds(0, 2)])
        sent("gz", ZS)
        sent("ex", EX.at[pl.ds(0, 3)])
        sent("ey", EY.at[pl.ds(0, 7)])
        sent("et", EU.at[0])

    return kernel


def hand_over(results):
    vm = pl.BlockSpec(memory_space=pltpu.VMEM)
    shapes = [jax.ShapeDtypeStruct(v.shape, v.dtype) for v in results]

    def kernel(*refs):
        sem = refs[10]
        moves = [pltpu.make_async_copy(refs[n], refs[5 + n], sem.at[n]) for n in range(5)]
        for c in moves:
            c.start()
        for c in moves:
            c.wait()

    return pl.pallas_call(kernel, out_shape=tuple(shapes), in_specs=[vm] * 5, out_specs=(pl.BlockSpec(memory_space=pltpu.HBM),) * 5,
        scratch_shapes=[pltpu.SemaphoreType.DMA((5,))],
    )(*[pltpu.with_memory_space_constraint(v, pltpu.VMEM) for v in results])


def per_device(inputs, up_proj, down_proj, out_cotangent):
    tokens, width = inputs.shape
    rows, hidden = up_proj.shape
    cols = hidden // 2
    ff = hidden * lax.axis_size("tp")
    all_tokens = tokens * lax.axis_size("rep") * lax.axis_size(FS) * lax.axis_size("tp")
    factor = float(all_tokens) ** (-0.5)
    up3 = up_proj.reshape(2, rows // 2, hidden)
    dn3 = down_proj.T.reshape(2, rows // 2, hidden)
    vm = pl.BlockSpec(memory_space=pltpu.VMEM)
    full = (2, 4, 4, rows)
    lines = rows * cols // 2048
    results = pl.pallas_call(
        make_kernel(tokens, width, cols, ff, factor),
        out_shape=(
            pltpu.VMEM((tokens, width), BF),
            pltpu.VMEM((rows, hidden), F32),
            pltpu.VMEM((rows, hidden), F32),
            pltpu.VMEM((1, rows), F32),
            pltpu.VMEM((1, hidden), F32),
        ),
        in_specs=[pl.BlockSpec(memory_space=pltpu.HBM)] * 4,
        out_specs=(vm,) * 5,
        scratch_shapes=[
            pltpu.VMEM((4, tokens, width), BF),
            pltpu.VMEM((4, tokens, width), BF),
            pltpu.VMEM(full + (4 * tokens,), BF),
            pltpu.VMEM(full + (4 * tokens,), BF),
            pltpu.VMEM((2, 2, 4, 4, 2, rows // 2, cols), BF),
            pltpu.VMEM((4, tokens, cols), F32),
            pltpu.VMEM((4, tokens, cols), BF),
            pltpu.VMEM((4, tokens, cols), BF),
            pltpu.VMEM((2,) + full + (cols,), F32),
            pltpu.VMEM((4, 2, 6, lines + 1, 16, 128), BF),
            pltpu.VMEM((4, 2, 6, lines + 1, 16, 128), BF),
            pltpu.VMEM((2, 6, lines // 2 + 1, 16, 128), BF),
            pltpu.VMEM((2, 6, lines // 2 + 1, 16, 128), BF),
            pltpu.VMEM((2, 2, 3, lines // 2 + 1, 16, 128), BF),
            pltpu.VMEM((2, 2, 3, lines // 2 + 1, 16, 128), BF),
            pltpu.VMEM((2, lines + 1, 16, 128), BF),
            pltpu.VMEM((3, lines + 1, 16, 128), BF),
            pltpu.VMEM((2, 2, lines // 2 + 1, 16, 128), BF),
            pltpu.VMEM((2, 3, lines // 2 + 1, 16, 128), BF),
            pltpu.VMEM((4, tokens, width), F32),
            pltpu.VMEM((2, tokens, width), F32),
            pltpu.VMEM((tokens * width // 2048 + 1, 16, 128), BF),
            pltpu.VMEM((tokens * width // 2048 + 1, 16, 128), BF),
            pltpu.VMEM((4, 1, hidden), F32),
            pltpu.VMEM((8, 1, hidden), F32),
            pltpu.VMEM((2, rows, 128), F32),
            pltpu.VMEM((2, 2, rows // 2, cols), BF),
            pltpu.SemaphoreType.DMA((BATCHES,)),
            pltpu.SemaphoreType.DMA((WAITS,)),
            pltpu.SemaphoreType.DMA((6,)),
        ],
        compiler_params=pltpu.CompilerParams(
            collective_id=0, has_side_effects=True, vmem_limit_bytes=52 * 1024 * 1024
        ),
    )(*[pltpu.with_memory_space_constraint(v, pltpu.HBM) for v in (inputs, up3, dn3, out_cotangent)])
    gin, gup, gdn, eup, edn = hand_over(results)
    return gin, gup, gdn.T, eup.reshape(rows), edn.reshape(hidden)


def solution(mesh):
    torus = Mesh(
        mesh.devices.reshape(mesh.shape["rep"], 2, 4, 4, mesh.shape["tp"]),
        ("rep", "fs_0", "fs_1", "fs_2", "tp"),
    )
    placed = (P(REP_FS_TP, None), P(FS, "tp"), P("tp", FS), P(REP_FS_TP, None))
    return jax.shard_map(
        per_device,
        mesh=torus,
        in_specs=placed,
        out_specs=(P(REP_FS_TP, None), P(FS, "tp"), P("tp", FS), P(FS), P("tp")),
        check_vma=False,
    )
```

```python
import jax
import jax.numpy as jnp
from jax import lax
from jax.experimental import pallas as pl
from jax.experimental.pallas import tpu as pltpu
from jax.sharding import Mesh
from jax.sharding import PartitionSpec as P

FS = ("fs_0", "fs_1", "fs_2")
REP_FS_TP = ("rep", "fs_0", "fs_1", "fs_2", "tp")
MESH = pl.DeviceIdType.MESH
BF = jnp.bfloat16
F32 = jnp.float32
RIGHT, LEFT = 0, 1
UP, DN = 0, 1
WAITS, BATCHES = 118, 32


ORDER = [
    ("init", 1, 0), ("init", 0, 0), ("init", 0, 1), ("init", 1, 1), ("turn", "c", 0), ("near", 0, 0, 1),
    ("near", 0, 0, 0), ("near", 0, 1, 1), ("near", 0, 1, 0), ("fwd", 0, 0, 2, 1), ("near", 1, 1, 1),
    ("near", 1, 1, 0), ("step2", 0, 0), ("near", 1, 0, 0), ("step2", 0, 1), ("pass", "x", 0), ("turn", "x", 1),
    ("fwd", 0, 0, 1, 0), ("near", 1, 0, 1), ("fwd", 0, 1, 2, 1), ("pass", "x", 1), ("fwd", 0, 0, 2, 0),
    ("fwd", 0, 0, 1, 1), ("fwd", 1, 1, 2, 0), ("fwd", 0, 1, 0, 1), ("fwd", 0, 1, 0, 0), ("fwd", 0, 1, 2, 0),
    ("fwd", 1, 1, 0, 1), ("fwd", 0, 0, 3, 0), ("fwd", 0, 1, 3, 1), ("turn", "x", 3), ("fwd", 0, 1, 1, 1),
    ("fwd", 0, 1, 3, 0), ("fwd", 0, 0, 0, 1), ("fwd", 1, 1, 2, 1), ("fwd", 0, 0, 0, 0), ("turn", "c", 1),
    ("fwd", 0, 0, 3, 1), ("fwd", 0, 1, 1, 0), ("turn", "x", 0), ("fwd", 1, 1, 1, 0), ("pass", "c", 0),
    ("turn", "x", 2), ("fwd", 1, 0, 2, 0), ("fwd", 1, 0, 0, 1), ("step2", 1, 1), ("step2", 1, 0), ("proj", 0),
    ("ma", 1, 1), ("fwd", 1, 1, 0, 0), ("ma", 1, 0), ("fwd", 1, 0, 1, 1), ("pass", "c", 1), ("fwd", 1, 0, 0, 0),
    ("fwd", 1, 1, 3, 1), ("fwd", 1, 0, 3, 1), ("fwd", 1, 0, 2, 1), ("fwd", 1, 0, 3, 0), ("proj", 1),
    ("fwd", 1, 1, 3, 0), ("fwd", 1, 0, 1, 0), ("fwd", 1, 1, 1, 1), ("turn", "c", 2), ("turn", "c", 3),
    ("mult", 1, 0), ("nr", 1, 0, 0), ("far", 1, 0, 0), ("mult", 1, 1), ("far", 1, 1, 1), ("far", 1, 0, 1),
    ("far", 1, 1, 0), ("nr", 1, 1, 1), ("pull", 1), ("nl", 1, 0, 1), ("pull", 0), ("ip", 0), ("nr", 1, 0, 1),
    ("nl", 1, 0, 0), ("nl", 1, 1, 0), ("rl", 1, 0, 1, 1), ("nl", 1, 1, 1), ("nr", 1, 1, 0), ("rl", 1, 0, 0, 0),
    ("mult", 0, 0), ("rl", 1, 0, 1, 0), ("rl", 1, 1, 0, 1), ("rl", 1, 1, 1, 1), ("rl", 1, 0, 0, 1), ("ip", 1),
    ("gz",), ("rl", 1, 1, 0, 0), ("rl", 1, 1, 1, 0), ("far", 0, 0, 0), ("mult", 0, 1), ("far", 0, 1, 0),
    ("ni", 1, 0, 0), ("far", 0, 0, 1), ("nr", 0, 0, 0), ("ni", 1, 0, 1), ("st2", 1, 0), ("nl", 0, 0, 0),
    ("far", 0, 1, 1), ("ni", 1, 1, 0), ("ni", 1, 1, 1), ("st2", 1, 1), ("rl", 0, 1, 0, 0), ("rl2", 1, 0, 1),
    ("rl2", 1, 0, 0), ("nl", 0, 1, 0), ("rl", 0, 1, 1, 0), ("nr", 0, 1, 0), ("rl", 0, 0, 1, 0), ("nr", 0, 1, 1),
    ("rl", 0, 0, 0, 0), ("rl2", 1, 1, 0), ("rl2", 1, 1, 1), ("rl", 0, 0, 1, 1), ("nl", 0, 1, 1), ("nr", 0, 0, 1),
    ("rl", 0, 0, 0, 1), ("nl", 0, 0, 1), ("ni", 0, 0, 0), ("rl", 0, 1, 1, 1), ("rl", 0, 1, 0, 1), ("st3", 1, 0),
    ("st3", 1, 1), ("st2", 0, 0, 0), ("ni", 0, 1, 0), ("st2", 0, 1, 0), ("ni", 0, 0, 1), ("ni", 0, 1, 1),
    ("st2", 0, 0, 1), ("st2", 0, 1, 1), ("gin",), ("fin", 1), ("ex",), ("st3", 0, 0, 0), ("st3", 0, 1, 0),
    ("st3", 0, 0, 1), ("ey",), ("st3", 0, 1, 1), ("fin", 0, 0), ("fin", 0, 1), ("eu",), ("eup",), ("edn",),
]


def make_kernel(tokens, width, cols, ff, factor):
    lanes = [pl.ds(c * 128, 128) for c in range(cols // 128)]

    def kernel(
        x_ref, up_ref, dn_ref, cot_ref,
        gin_ref, gup_ref, gdn_ref, eup_ref, edn_ref,
        X, C, XT, CT, W, RP, ACT, GP, G,
        s1s, s1r, s2s, s2r, d2s, d2r, s3s, s3r, u3s, u3r,
        PART, DR, ZS, ZR, EX, EY, EU,
        OTH, ssem, rsem, lsem,
    ):
        r = lax.axis_index("rep")
        j = lax.axis_index("fs_0")
        y = lax.axis_index("fs_1")
        x = lax.axis_index("fs_2")
        t = lax.axis_index("tp")

        def at(pos, d):
            return lax.rem(pos + d, 4)

        def xdev(d):
            return {"fs_2": at(x, d)}

        def ydev(d):
            return {"fs_1": at(y, d)}

        def yzdev(d):
            return {"fs_0": 1 - j, "fs_1": at(y, d)}

        zpeer = {"fs_0": 1 - j}
        rpeer = {"rep": 1 - r}
        rzpeer = {"rep": 1 - r, "fs_0": 1 - j}
        tpeer = {"tp": 1 - t}

        own = pl.ds(pl.multiple_of(j * cols, cols), cols)
        other = pl.ds(pl.multiple_of((1 - j) * cols, cols), cols)
        loads = [
            pltpu.make_async_copy(up_ref.at[:, :, other], OTH.at[UP], lsem.at[0]),
            pltpu.make_async_copy(dn_ref.at[:, :, other], OTH.at[DN], lsem.at[1]),
            pltpu.make_async_copy(up_ref.at[:, :, own], W.at[UP, j, y, x], lsem.at[2]),
            pltpu.make_async_copy(dn_ref.at[:, :, own], W.at[DN, j, y, x], lsem.at[3]),
            pltpu.make_async_copy(x_ref, X.at[0], lsem.at[4]),
            pltpu.make_async_copy(cot_ref, C.at[0], lsem.at[5]),
        ]
        for c in loads:
            c.start()

        barrier = pltpu.get_barrier_semaphore()
        peers = [xdev(1), xdev(2), xdev(3), ydev(1), ydev(2), ydev(3), zpeer, rpeer, rzpeer, tpeer, yzdev(1), yzdev(2), yzdev(3)]
        for dev in peers:
            pl.semaphore_signal(barrier, inc=1, device_id=dev, device_id_type=MESH)
        pl.semaphore_wait(barrier, len(peers))

        arrivals, departures = {}, {}

        def slot_of(table, group):
            return table.setdefault(group, len(table))

        def send(group, src, dst, dev, batch):
            pltpu.make_async_remote_copy(
                src_ref=src, dst_ref=dst,
                send_sem=ssem.at[slot_of(departures, batch)], recv_sem=rsem.at[slot_of(arrivals, group)],
                device_id=dev, device_id_type=MESH,
            ).start()

        def recv(group, ref):
            pltpu.make_async_copy(ref, ref, rsem.at[arrivals[group]]).wait()

        def sent(batch, ref):
            pltpu.make_async_copy(ref, ref, ssem.at[departures[batch]]).wait()

        half = tokens // 2

        def blk(ref, w, h, a, b):
            z = j if h == 0 else 1 - j
            return ref.at[w, z, b, a] if h == 0 else ref.at[w, z, a, b]

        def axes(h):
            return (x, y, xdev, ydev) if h == 0 else (y, x, ydev, xdev)

        def init(w, h):
            a, b, adev, bdev = axes(h)
            ref = blk(W, w, h, a, b)
            if h == 1:
                recv(("a2a", w), ref)
            send((1, w, h, 0), ref, ref, adev(1), (w, h))
            send((1, w, h, 1), ref, ref, adev(3), (w, h))
            spread(w, h, 0, a)

        def spread(w, h, s, a2):
            _, b, _, bdev = axes(h)
            ref = blk(W, w, h, a2, b)
            send((2, w, h, s, 0), ref, ref, bdev(1), (w, h))
            send((2, w, h, s, 1), ref, ref, bdev(3), (w, h))

        def near(w, h, side):
            a, b, adev, _ = axes(h)
            place, away = ((at(a, 3), 1), (at(a, 1), 3))[side]
            ref = blk(W, w, h, place, b)
            recv((1, w, h, side), ref)
            send((1, w, h, 2), ref.at[side], ref.at[side], adev(away), (w, h))
            spread(w, h, 1 + side, place)

        def step2(w, h):
            a, b, _, _ = axes(h)
            recv((1, w, h, 2), blk(W, w, h, at(a, 2), b))
            spread(w, h, 3, at(a, 2))

        def fwd(w, h, s, side):
            a, b, _, bdev = axes(h)
            a2 = at(a, (0, 3, 1, 2)[s])
            place, away = ((at(b, 3), 1), (at(b, 1), 3))[side]
            ref = blk(W, w, h, a2, place)
            recv((2, w, h, s, side), ref)
            send((3, w), ref.at[side], ref.at[side], bdev(away), (w, h))

        whole = set()

        def fin(w):
            if w not in whole:
                whole.add(w)
                recv((3, w), W.at[w, 0, pl.ds(0, 2)])

        stock = {"x": (X, XT), "c": (C, CT)}

        def pass_on(name, i):
            rows = pl.ds(i * half, half)
            buf = stock[name][0]
            recv((name, "z", i), buf.at[2, rows])
            send((name, "zt"), buf.at[2, rows], buf.at[3, rows], tpeer, (name, "zt"))

        def turn(name, slot):
            src, dst = stock[name]
            if slot == 1:
                recv((name, "t"), src.at[1])
            if slot == 3:
                recv((name, "zt"), src.at[3])
            v = src[slot].T
            dst[:, :, :, :, slot * tokens:(slot + 1) * tokens] = v.reshape(2, 4, 4, width // 32, tokens)

        def weight(w):
            return W[w].reshape(width, cols)

        def both(ref, s1, s2):
            return jnp.concatenate([ref[s1], ref[s2]], axis=0)

        def project(n):
            s1, s2 = 2 * n, 2 * n + 1
            fin(UP)
            pre = jnp.maximum(jnp.dot(both(X, s1, s2), weight(UP), preferred_element_type=F32), 0.0)
            for n, slot in enumerate((s1, s2)):
                v = pre[n * tokens:(n + 1) * tokens]
                RP[slot] = v
                ACT[slot] = (v * v).astype(BF)

        def pull_back(n):
            s1, s2 = 2 * n, 2 * n + 1
            fin(DN)
            back = jnp.dot(both(C, s1, s2), weight(DN), preferred_element_type=F32)
            for n, slot in enumerate((s1, s2)):
                GP[slot] = (2.0 * RP[slot] * back[n * tokens:(n + 1) * tokens]).astype(BF)

        lhs_of = (XT, CT)
        rhs_of = (GP, ACT)

        def gblk(w, h, a, b):
            z = j if h == 0 else 1 - j
            return G.at[w, z, a, b] if h == 0 else G.at[w, z, b, a]

        def raxes(h):
            return (y, x, ydev, xdev) if h == 0 else (x, y, xdev, ydev)

        def product(w, h, lo, n):
            z = j if h == 0 else 1 - j
            left = lhs_of[w][z, :, :, :, lo * tokens:(lo + n) * tokens].reshape(width // 2, n * tokens)
            right = rhs_of[w][lo:lo + n].reshape(n * tokens, cols)
            out = jnp.dot(left, right, preferred_element_type=F32)
            return G.at[w, z], out.reshape(4, 4, width // 32, cols)

        begun = set()

        def multiply_early(w, h):
            ref, out = product(w, h, 0, 2)
            ref[...] = out
            begun.add((w, h))

        def multiply(w, h):
            if (w, h) in begun:
                ref, out = product(w, h, 2, 2)
                ref[...] = ref[...] + out
            else:
                ref, out = product(w, h, 0, 4)
                ref[...] = out

        def tiles(refs):
            every = []
            for m, ref in enumerate(refs):
                rows, wide = ref.shape
                for c in range(wide // 128):
                    for q in range(rows // 16):
                        every.append((len(every), m, pl.ds(16 * q, 16), pl.ds(128 * c, 128)))
            return every

        def encode(refs, dst, steps=3):
            every = tiles(refs)
            top = None
            for _, m, q, c in every:
                v = jnp.abs(refs[m][q, c])
                top = v if top is None else jnp.maximum(top, v)
            top = jnp.maximum(top, 2e-34).astype(BF)
            dst[len(every)] = top
            inv = 2.0 ** (120 >> steps) / top.astype(F32)
            for n, m, q, c in every:
                v = refs[m][q, c] * inv
                for _ in range(steps):
                    v = v * jnp.abs(v)
                dst[n] = v.astype(BF)

        def decoder(buf, refs, steps=3):
            every = tiles(refs)
            unit = buf[len(every)].astype(F32) * 0.5 ** (120 >> steps)

            def tile(n):
                v = buf[n].astype(F32)
                m = jnp.exp2(jnp.log2(jnp.abs(v)) * 0.5 ** steps)
                return jnp.where(v < 0, -m, m) * unit
            return every, tile

        def add(refs, buf):
            every, tile = decoder(buf, refs)
            for n, m, q, c in every:
                refs[m][q, c] = refs[m][q, c] + tile(n)

        class Ring:
            def __init__(self, key, pos, dev, parts, sb, rb):
                self.k, self.pos, self.dev, self.parts, self.sb, self.rb = key, pos, dev, parts, sb, rb

            def post(self, i, place, side, d, group):
                encode(self.parts(place, side), self.sb.at[i])
                send(self.k + group, self.sb.at[i], self.rb.at[i], self.dev(d), self.k)

            def far(self):
                self.post(0, at(self.pos, 2), 0, 1, ("far", 0))
                self.post(1, at(self.pos, 2), 1, 3, ("far", 1))

            def near_right(self):
                self.post(2, at(self.pos, 1), 1, 1, ("near",))

            def near_left(self):
                self.post(3, at(self.pos, 3), 0, 3, ("near",))

            def relay(self, side):
                place, d = at(self.pos, (1, 3)[side]), (1, 3)[side]
                recv(self.k + ("far", side), self.rb.at[side])
                add(self.parts(place, side), self.rb.at[side])
                self.post(4 + side, place, side, d, ("last",))

            def near_in(self):
                recv(self.k + ("near",), self.rb.at[pl.ds(2, 2)])
                add(self.parts(self.pos, 0), self.rb.at[3])
                add(self.parts(self.pos, 1), self.rb.at[2])

            def last_in(self):
                recv(self.k + ("last",), self.rb.at[pl.ds(4, 2)])
                add(self.parts(self.pos, 0), self.rb.at[4])
                add(self.parts(self.pos, 1), self.rb.at[5])

        wing = cols // 2
        hr = width // 64

        def ring1(w, h, c):
            a, _, adev, _ = raxes(h)
            return Ring((1, w, h, c), a, adev,
                        lambda place, side: [gblk(w, h, place, 2 * side + i).at[:, pl.ds(c * wing, wing)] for i in (0, 1)],
                        s1s.at[2 * w + h, c], s1r.at[2 * w + h, c])

        def ring2(h):
            a, b, _, bdev = raxes(h)
            return Ring((2, DN, h), b, bdev,
                        lambda place, side: [gblk(DN, h, a, place).at[pl.ds(side * hr, hr)]],
                        s2s.at[h], s2r.at[h])

        first = {(w, h, c): ring1(w, h, c) for w in (UP, DN) for h in (0, 1) for c in (0, 1)}
        second = [ring2(h) for h in (0, 1)]

        def part(h, c, place):
            return gblk(UP, h, raxes(h)[0], place).at[:, pl.ds(c * wing, wing)]

        def second_start(w, h, c=None):
            if w == DN:
                for c in (0, 1):
                    first[w, h, c].last_in()
                second[h].far()
                second[h].near_right()
                second[h].near_left()
                return
            first[w, h, c].last_in()
            _, b, _, bdev = raxes(h)
            for d in (2, 1, 3):
                encode([part(h, c, at(b, d))], d2s.at[h, c, d - 1])
                send(("d2", h, c), d2s.at[h, c, d - 1], d2r.at[h, c, d - 1], bdev(d), ("d2", h, c))

        def third_start(w, h, c=None):
            a, b, _, _ = raxes(h)
            peers_ = [(0, rpeer)] if h == 0 else [(1, zpeer), (2, rzpeer)]
            if w == DN:
                second[h].near_in()
                second[h].last_in()
                encode([gblk(w, h, a, b)], s3s.at[h])
                for i, dev in peers_:
                    send((5, w), s3s.at[h], s3r.at[i], dev, (5, w))
                return
            recv(("d2", h, c), d2r.at[h, c])
            for d in range(3):
                add([part(h, c, b)], d2r.at[h, c, d])
            encode([part(h, c, b)], u3s.at[c, h])
            for i, dev in peers_:
                send((5, w, c), u3s.at[c, h], u3r.at[c, i], dev, (5, w, c))

        def finish(w, c=None):
            if w == DN:
                out, mine, theirs, at_, wide = gdn_ref, s3s, s3r, 0, cols
                recv((5, w), s3r)
            else:
                out, mine, theirs, at_, wide = gup_ref, u3s.at[c], u3r.at[c], c * wing, wing
                recv((5, w, c), u3r.at[c])
            for side, one, two in ((j, mine.at[0], theirs.at[0]), (1 - j, theirs.at[1], theirs.at[2])):
                like = [out.at[:, pl.ds(0, wide)]]
                every, tile1 = decoder(one, like)
                _, tile2 = decoder(two, like)
                for n, _, q, _ in every:
                    col = pl.ds(pl.multiple_of(side * cols + at_ + n // (width // 512) * 128, 128), 128)
                    out[q, col] = (tile1(n) + tile2(n)) * factor

        def input_part(n):
            s1, s2 = ((3, 1), (2, 0))[n]
            w = W[UP].reshape(width, cols)
            v = lax.dot_general(both(GP, s1, s2), w, (((1,), (1,)), ((), ())), preferred_element_type=F32)
            PART[s1] = v[:tokens]
            PART[s2] = v[tokens:]
            if n == 0:
                for i, slot in enumerate((3, 1)):
                    send(("g", "t", i), PART.at[slot], DR.at[i], tpeer, "gt")

        def input_send():
            recv(("g", "t", 0), DR.at[0])
            PART[2] = PART[2] + DR[0]
            encode([PART.at[2]], ZS, 4)
            send("gz", ZS, ZR, zpeer, "gz")

        def input_sum():
            recv(("g", "t", 1), DR.at[1])
            recv("gz", ZR)
            every, tile = decoder(ZR, [PART.at[2]], 4)
            for n, _, q, c in every:
                gin_ref[q, c] = (PART[0, q, c] + DR[1, q, c] + tile(n)).astype(BF)

        def energy_x():
            EX[x] = jnp.sum(gdn_ref[...] * gdn_ref[...], axis=0, keepdims=True)
            for d in (1, 2, 3):
                send("ex", EX.at[x], EX.at[x], xdev(d), "ex")

        def energy_y():
            recv("ex", EX.at[pl.ds(0, 3)])
            me = 4 * j + y
            EY[me] = EX[0] + EX[1] + EX[2] + EX[3]
            for dev in [zpeer] + [f(d) for d in (1, 2, 3) for f in (ydev, yzdev)]:
                send("ey", EY.at[me], EY.at[me], dev, "ey")

        def energy_down():
            recv("ey", EY.at[pl.ds(0, 7)])
            total = EY[0]
            for n in range(1, 8):
                total = total + EY[n]
            edn_ref[...] = total * (1.0 / width)

        def energy_pair():
            total = None
            for c in range(2 * len(lanes)):
                v = gup_ref[:, c * 128:(c + 1) * 128]
                total = v * v if total is None else total + v * v
            EU[0] = total
            send("et", EU.at[0], EU.at[1], tpeer, "et")

        def energy_up():
            recv("et", EU.at[1])
            eup_ref[...] = jnp.sum((EU[0] + EU[1]).T, axis=0, keepdims=True) * (1.0 / ff)

        for w in (UP, DN):
            loads[w].wait()
            send(("a2a", w), OTH.at[w], W.at[w, j, y, x], rzpeer, "a2a")
        for c in loads[2:]:
            c.wait()
        for name in ("x", "c"):
            buf = stock[name][0]
            for i in (0, 1):
                rows = pl.ds(i * half, half)
                send((name, "z", i), buf.at[0, rows], buf.at[2, rows], zpeer, name)
            send((name, "t"), buf.at[0], buf.at[1], tpeer, name)
        todo = {
            "init": init, "near": near, "step2": step2, "fwd": fwd, "pass": pass_on, "turn": turn,
            "proj": project, "pull": pull_back, "mult": multiply, "ma": multiply_early,
            "far": lambda w, h, c: first[w, h, c].far(),
            "nr": lambda w, h, c: first[w, h, c].near_right(),
            "nl": lambda w, h, c: first[w, h, c].near_left(),
            "rl": lambda w, h, side, c: first[w, h, c].relay(side),
            "ni": lambda w, h, c: first[w, h, c].near_in(),
            "st2": second_start,
            "rl2": lambda w, h, side: second[h].relay(side),
            "st3": third_start, "fin": finish, "ip": input_part, "gz": input_send, "gin": input_sum,
            "ex": energy_x, "ey": energy_y, "edn": energy_down,
            "eu": energy_pair, "eup": energy_up,
        }
        for name, *where in ORDER:
            todo[name](*where)
        sent("a2a", OTH)
        for n, name in enumerate(("x", "c")):
            sent(name, RP.at[0])
            sent((name, "zt"), X.at[0])
            for h in (0, 1):
                sent((n, h), RP.at[0, pl.ds(0, 15 * tokens // 16)])
                for c in (0, 1):
                    sent((1, n, h, c), s1s.at[0, 0])
                    if n == UP:
                        sent(("d2", h, c), d2s.at[0, 0])
                if n == DN:
                    sent((2, n, h), s2s.at[0])
        sent((5, DN), s3r)
        for c in (0, 1):
            sent((5, UP, c), u3r.at[0])
        sent("gt", PART.at[pl.ds(0, 2)])
        sent("gz", ZS)
        sent("ex", EX.at[pl.ds(0, 3)])
        sent("ey", EY.at[pl.ds(0, 7)])
        sent("et", EU.at[0])

    return kernel


def hand_over(results):
    vm = pl.BlockSpec(memory_space=pltpu.VMEM)
    shapes = [jax.ShapeDtypeStruct(v.shape, v.dtype) for v in results]

    def kernel(*refs):
        sem = refs[10]
        moves = [pltpu.make_async_copy(refs[n], refs[5 + n], sem.at[n]) for n in range(5)]
        for c in moves:
            c.start()
        for c in moves:
            c.wait()

    return pl.pallas_call(kernel, out_shape=tuple(shapes), in_specs=[vm] * 5, out_specs=(pl.BlockSpec(memory_space=pltpu.HBM),) * 5,
        scratch_shapes=[pltpu.SemaphoreType.DMA((5,))],
    )(*[pltpu.with_memory_space_constraint(v, pltpu.VMEM) for v in results])


def per_device(inputs, up_proj, down_proj, out_cotangent):
    tokens, width = inputs.shape
    rows, hidden = up_proj.shape
    cols = hidden // 2
    ff = hidden * lax.axis_size("tp")
    all_tokens = tokens * lax.axis_size("rep") * lax.axis_size(FS) * lax.axis_size("tp")
    factor = float(all_tokens) ** (-0.5)
    up3 = up_proj.reshape(2, rows // 2, hidden)
    dn3 = down_proj.T.reshape(2, rows // 2, hidden)
    vm = pl.BlockSpec(memory_space=pltpu.VMEM)
    full = (2, 4, 4, rows)
    lines = rows * cols // 2048
    results = pl.pallas_call(
        make_kernel(tokens, width, cols, ff, factor),
        out_shape=(
            pltpu.VMEM((tokens, width), BF),
            pltpu.VMEM((rows, hidden), F32),
            pltpu.VMEM((rows, hidden), F32),
            pltpu.VMEM((1, rows), F32),
            pltpu.VMEM((1, hidden), F32),
        ),
        in_specs=[pl.BlockSpec(memory_space=pltpu.HBM)] * 4,
        out_specs=(vm,) * 5,
        scratch_shapes=[
            pltpu.VMEM((4, tokens, width), BF),
            pltpu.VMEM((4, tokens, width), BF),
            pltpu.VMEM(full + (4 * tokens,), BF),
            pltpu.VMEM(full + (4 * tokens,), BF),
            pltpu.VMEM((2, 2, 4, 4, 2, rows // 2, cols), BF),
            pltpu.VMEM((4, tokens, cols), F32),
            pltpu.VMEM((4, tokens, cols), BF),
            pltpu.VMEM((4, tokens, cols), BF),
            pltpu.VMEM((2,) + full + (cols,), F32),
            pltpu.VMEM((4, 2, 6, lines + 1, 16, 128), BF),
            pltpu.VMEM((4, 2, 6, lines + 1, 16, 128), BF),
            pltpu.VMEM((2, 6, lines // 2 + 1, 16, 128), BF),
            pltpu.VMEM((2, 6, lines // 2 + 1, 16, 128), BF),
            pltpu.VMEM((2, 2, 3, lines // 2 + 1, 16, 128), BF),
            pltpu.VMEM((2, 2, 3, lines // 2 + 1, 16, 128), BF),
            pltpu.VMEM((2, lines + 1, 16, 128), BF),
            pltpu.VMEM((3, lines + 1, 16, 128), BF),
            pltpu.VMEM((2, 2, lines // 2 + 1, 16, 128), BF),
            pltpu.VMEM((2, 3, lines // 2 + 1, 16, 128), BF),
            pltpu.VMEM((4, tokens, width), F32),
            pltpu.VMEM((2, tokens, width), F32),
            pltpu.VMEM((tokens * width // 2048 + 1, 16, 128), BF),
            pltpu.VMEM((tokens * width // 2048 + 1, 16, 128), BF),
            pltpu.VMEM((4, 1, hidden), F32),
            pltpu.VMEM((8, 1, hidden), F32),
            pltpu.VMEM((2, rows, 128), F32),
            pltpu.VMEM((2, 2, rows // 2, cols), BF),
            pltpu.SemaphoreType.DMA((BATCHES,)),
            pltpu.SemaphoreType.DMA((WAITS,)),
            pltpu.SemaphoreType.DMA((6,)),
        ],
        compiler_params=pltpu.CompilerParams(
            collective_id=0, has_side_effects=True, vmem_limit_bytes=52 * 1024 * 1024
        ),
    )(*[pltpu.with_memory_space_constraint(v, pltpu.HBM) for v in (inputs, up3, dn3, out_cotangent)])
    gin, gup, gdn, eup, edn = hand_over(results)
    return gin, gup, gdn.T, eup.reshape(rows), edn.reshape(hidden)


def solution(mesh):
    torus = Mesh(
        mesh.devices.reshape(mesh.shape["rep"], 2, 4, 4, mesh.shape["tp"]),
        ("rep", "fs_0", "fs_1", "fs_2", "tp"),
    )
    placed = (P(REP_FS_TP, None), P(FS, "tp"), P("tp", FS), P(REP_FS_TP, None))
    return jax.shard_map(
        per_device,
        mesh=torus,
        in_specs=placed,
        out_specs=(P(REP_FS_TP, None), P(FS, "tp"), P("tp", FS), P(FS), P("tp")),
        check_vma=False,
    )
```

```python
import jax
import jax.numpy as jnp
from jax import lax
from jax.experimental import pallas as pl
from jax.experimental.pallas import tpu as pltpu
from jax.sharding import Mesh
from jax.sharding import PartitionSpec as P

FS = ("fs_0", "fs_1", "fs_2")
REP_FS_TP = ("rep", "fs_0", "fs_1", "fs_2", "tp")
MESH = pl.DeviceIdType.MESH
BF = jnp.bfloat16
F32 = jnp.float32
RIGHT, LEFT = 0, 1
UP, DN = 0, 1
WAITS, BATCHES = 109, 14


ORDER = [
    ("init", 1, 0), ("init", 0, 0), ("init", 0, 1), ("init", 1, 1), ("turn", "c", 0), ("near", 0, 0, 1),
    ("near", 0, 0, 0), ("near", 0, 1, 1), ("near", 0, 1, 0), ("fwd", 0, 0, 2, 1), ("near", 1, 1, 1),
    ("near", 1, 1, 0), ("step2", 0, 0), ("near", 1, 0, 0), ("step2", 0, 1), ("pass", "x", 0), ("turn", "x", 1),
    ("fwd", 0, 0, 1, 0), ("near", 1, 0, 1), ("fwd", 0, 1, 2, 1), ("pass", "x", 1), ("fwd", 0, 0, 2, 0),
    ("fwd", 0, 0, 1, 1), ("fwd", 1, 1, 2, 0), ("fwd", 0, 1, 0, 1), ("fwd", 0, 1, 0, 0), ("fwd", 0, 1, 2, 0),
    ("fwd", 1, 1, 0, 1), ("fwd", 0, 0, 3, 0), ("fwd", 0, 1, 3, 1), ("turn", "x", 3), ("fwd", 0, 1, 1, 1),
    ("fwd", 0, 1, 3, 0), ("fwd", 0, 0, 0, 1), ("fwd", 1, 1, 2, 1), ("fwd", 0, 0, 0, 0), ("turn", "c", 1),
    ("fwd", 0, 0, 3, 1), ("fwd", 0, 1, 1, 0), ("turn", "x", 0), ("fwd", 1, 1, 1, 0), ("pass", "c", 0),
    ("turn", "x", 2), ("fwd", 1, 0, 2, 0), ("fwd", 1, 0, 0, 1), ("step2", 1, 1), ("step2", 1, 0), ("proj", 0),
    ("ma", 1, 1), ("fwd", 1, 1, 0, 0), ("ma", 1, 0), ("fwd", 1, 0, 1, 1), ("pass", "c", 1), ("fwd", 1, 0, 0, 0),
    ("fwd", 1, 1, 3, 1), ("fwd", 1, 0, 3, 1), ("fwd", 1, 0, 2, 1), ("fwd", 1, 0, 3, 0), ("proj", 1),
    ("fwd", 1, 1, 3, 0), ("fwd", 1, 0, 1, 0), ("fwd", 1, 1, 1, 1), ("turn", "c", 2), ("turn", "c", 3),
    ("mult", 1, 0), ("nr", 1, 0, 0), ("far", 1, 0, 0), ("mult", 1, 1), ("far", 1, 1, 1), ("far", 1, 0, 1),
    ("far", 1, 1, 0), ("nr", 1, 1, 1), ("pull", 1), ("nl", 1, 0, 1), ("pull", 0), ("ip", 0), ("nr", 1, 0, 1),
    ("nl", 1, 0, 0), ("nl", 1, 1, 0), ("rl", 1, 0, 1, 1), ("nl", 1, 1, 1), ("nr", 1, 1, 0), ("rl", 1, 0, 0, 0),
    ("mult", 0, 0), ("rl", 1, 0, 1, 0), ("rl", 1, 1, 0, 1), ("rl", 1, 1, 1, 1), ("rl", 1, 0, 0, 1), ("ip", 1),
    ("gz",), ("rl", 1, 1, 0, 0), ("rl", 1, 1, 1, 0), ("far", 0, 0, 0), ("mult", 0, 1), ("far", 0, 1, 0),
    ("ni", 1, 0, 0), ("far", 0, 0, 1), ("nr", 0, 0, 0), ("ni", 1, 0, 1), ("st2", 1, 0), ("nl", 0, 0, 0),
    ("far", 0, 1, 1), ("ni", 1, 1, 0), ("ni", 1, 1, 1), ("st2", 1, 1), ("rl", 0, 1, 0, 0), ("rl2", 1, 0, 1),
    ("rl2", 1, 0, 0), ("nl", 0, 1, 0), ("rl", 0, 1, 1, 0), ("nr", 0, 1, 0), ("rl", 0, 0, 1, 0), ("nr", 0, 1, 1),
    ("rl", 0, 0, 0, 0), ("rl2", 1, 1, 0), ("rl2", 1, 1, 1), ("rl", 0, 0, 1, 1), ("nl", 0, 1, 1), ("nr", 0, 0, 1),
    ("rl", 0, 0, 0, 1), ("nl", 0, 0, 1), ("ni", 0, 0, 0), ("rl", 0, 1, 1, 1), ("rl", 0, 1, 0, 1), ("st3", 1, 0),
    ("st3", 1, 1), ("st2", 0, 0, 0), ("ni", 0, 1, 0), ("st2", 0, 1, 0), ("ni", 0, 0, 1), ("ni", 0, 1, 1),
    ("st2", 0, 0, 1), ("st2", 0, 1, 1), ("gin",), ("fin", 1), ("ex",), ("st3", 0, 0, 0), ("st3", 0, 1, 0),
    ("st3", 0, 0, 1), ("ey",), ("st3", 0, 1, 1), ("fin", 0, 0), ("fin", 0, 1), ("eu",), ("eup",), ("edn",),
]


def make_kernel(tokens, width, cols, ff, factor):
    lanes = [pl.ds(c * 128, 128) for c in range(cols // 128)]

    def kernel(
        x_ref, up_ref, dn_ref, cot_ref,
        gin_ref, gup_ref, gdn_ref, eup_ref, edn_ref,
        X, C, XT, CT, W, RP, ACT, GP, G,
        s1s, s1r, s2s, s2r, d2s, d2r, s3s, s3r, u3s, u3r,
        PART, DR, ZS, ZR, EX, EY, EU,
        OTH, ssem, rsem, lsem,
    ):
        r = lax.axis_index("rep")
        j = lax.axis_index("fs_0")
        y = lax.axis_index("fs_1")
        x = lax.axis_index("fs_2")
        t = lax.axis_index("tp")

        def at(pos, d):
            return lax.rem(pos + d, 4)

        def xdev(d):
            return {"fs_2": at(x, d)}

        def ydev(d):
            return {"fs_1": at(y, d)}

        def yzdev(d):
            return {"fs_0": 1 - j, "fs_1": at(y, d)}

        zpeer = {"fs_0": 1 - j}
        rpeer = {"rep": 1 - r}
        rzpeer = {"rep": 1 - r, "fs_0": 1 - j}
        tpeer = {"tp": 1 - t}

        own = pl.ds(pl.multiple_of(j * cols, cols), cols)
        other = pl.ds(pl.multiple_of((1 - j) * cols, cols), cols)
        loads = [
            pltpu.make_async_copy(up_ref.at[:, :, other], OTH.at[UP], lsem.at[0]),
            pltpu.make_async_copy(dn_ref.at[:, :, other], OTH.at[DN], lsem.at[1]),
            pltpu.make_async_copy(up_ref.at[:, :, own], W.at[UP, j, y, x], lsem.at[2]),
            pltpu.make_async_copy(dn_ref.at[:, :, own], W.at[DN, j, y, x], lsem.at[3]),
            pltpu.make_async_copy(x_ref, X.at[0], lsem.at[4]),
            pltpu.make_async_copy(cot_ref, C.at[0], lsem.at[5]),
        ]
        for c in loads:
            c.start()

        barrier = pltpu.get_barrier_semaphore()
        peers = [xdev(1), xdev(2), xdev(3), ydev(1), ydev(2), ydev(3), zpeer, rpeer, rzpeer, tpeer, yzdev(1), yzdev(2), yzdev(3)]
        for dev in peers:
            pl.semaphore_signal(barrier, inc=1, device_id=dev, device_id_type=MESH)
        pl.semaphore_wait(barrier, len(peers))

        arrivals, departures = {}, {}

        def slot_of(table, group):
            return table.setdefault(group, len(table))

        def send(group, src, dst, dev, batch):
            pltpu.make_async_remote_copy(
                src_ref=src, dst_ref=dst,
                send_sem=ssem.at[slot_of(departures, batch)], recv_sem=rsem.at[slot_of(arrivals, group)],
                device_id=dev, device_id_type=MESH,
            ).start()

        def recv(group, ref):
            pltpu.make_async_copy(ref, ref, rsem.at[arrivals[group]]).wait()

        def sent(batch, ref):
            pltpu.make_async_copy(ref, ref, ssem.at[departures[batch]]).wait()

        half = tokens // 2

        def blk(ref, w, h, a, b):
            z = j if h == 0 else 1 - j
            return ref.at[w, z, b, a] if h == 0 else ref.at[w, z, a, b]

        def axes(h):
            return (x, y, xdev, ydev) if h == 0 else (y, x, ydev, xdev)

        def init(w, h):
            a, b, adev, bdev = axes(h)
            ref = blk(W, w, h, a, b)
            if h == 1:
                recv(("a2a", w), ref)
            send((1, w, h, 0), ref, ref, adev(1), "w")
            send((1, w, h, 1), ref, ref, adev(3), "w")
            spread(w, h, 0, a)

        def spread(w, h, s, a2):
            _, b, _, bdev = axes(h)
            ref = blk(W, w, h, a2, b)
            send((2, w, h, s, 0), ref, ref, bdev(1), "w")
            send((2, w, h, s, 1), ref, ref, bdev(3), "w")

        def near(w, h, side):
            a, b, adev, _ = axes(h)
            place, away = ((at(a, 3), 1), (at(a, 1), 3))[side]
            ref = blk(W, w, h, place, b)
            recv((1, w, h, side), ref)
            send((1, w, h, 2), ref.at[side], ref.at[side], adev(away), "w")
            spread(w, h, 1 + side, place)

        def step2(w, h):
            a, b, _, _ = axes(h)
            recv((1, w, h, 2), blk(W, w, h, at(a, 2), b))
            spread(w, h, 3, at(a, 2))

        def fwd(w, h, s, side):
            a, b, _, bdev = axes(h)
            a2 = at(a, (0, 3, 1, 2)[s])
            place, away = ((at(b, 3), 1), (at(b, 1), 3))[side]
            ref = blk(W, w, h, a2, place)
            recv((2, w, h, s, side), ref)
            send((3, w), ref.at[side], ref.at[side], bdev(away), "w")

        whole = set()

        def fin(w):
            if w not in whole:
                whole.add(w)
                recv((3, w), W.at[w, 0, pl.ds(0, 2)])

        stock = {"x": (X, XT), "c": (C, CT)}

        def pass_on(name, i):
            rows = pl.ds(i * half, half)
            buf = stock[name][0]
            recv((name, "z", i), buf.at[2, rows])
            send((name, "zt"), buf.at[2, rows], buf.at[3, rows], tpeer, "zt")

        def turn(name, slot):
            src, dst = stock[name]
            if slot == 1:
                recv((name, "t"), src.at[1])
            if slot == 3:
                recv((name, "zt"), src.at[3])
            v = src[slot].T
            dst[:, :, :, :, slot * tokens:(slot + 1) * tokens] = v.reshape(2, 4, 4, width // 32, tokens)

        def weight(w):
            return W[w].reshape(width, cols)

        def both(ref, s1, s2):
            return jnp.concatenate([ref[s1], ref[s2]], axis=0)

        def project(n):
            s1, s2 = 2 * n, 2 * n + 1
            fin(UP)
            pre = jnp.maximum(jnp.dot(both(X, s1, s2), weight(UP), preferred_element_type=F32), 0.0)
            for n, slot in enumerate((s1, s2)):
                v = pre[n * tokens:(n + 1) * tokens]
                RP[slot] = v
                ACT[slot] = (v * v).astype(BF)

        def pull_back(n):
            s1, s2 = 2 * n, 2 * n + 1
            fin(DN)
            back = jnp.dot(both(C, s1, s2), weight(DN), preferred_element_type=F32)
            for n, slot in enumerate((s1, s2)):
                GP[slot] = (2.0 * RP[slot] * back[n * tokens:(n + 1) * tokens]).astype(BF)

        lhs_of = (XT, CT)
        rhs_of = (GP, ACT)

        def gblk(w, h, a, b):
            z = j if h == 0 else 1 - j
            return G.at[w, z, a, b] if h == 0 else G.at[w, z, b, a]

        def raxes(h):
            return (y, x, ydev, xdev) if h == 0 else (x, y, xdev, ydev)

        def product(w, h, lo, n):
            z = j if h == 0 else 1 - j
            left = lhs_of[w][z, :, :, :, lo * tokens:(lo + n) * tokens].reshape(width // 2, n * tokens)
            right = rhs_of[w][lo:lo + n].reshape(n * tokens, cols)
            out = jnp.dot(left, right, preferred_element_type=F32)
            return G.at[w, z], out.reshape(4, 4, width // 32, cols)

        begun = set()

        def multiply_early(w, h):
            ref, out = product(w, h, 0, 2)
            ref[...] = out
            begun.add((w, h))

        def multiply(w, h):
            if (w, h) in begun:
                ref, out = product(w, h, 2, 2)
                ref[...] = ref[...] + out
            else:
                ref, out = product(w, h, 0, 4)
                ref[...] = out

        def tiles(refs):
            every = []
            for m, ref in enumerate(refs):
                rows, wide = ref.shape
                for c in range(wide // 128):
                    for q in range(rows // 16):
                        every.append((len(every), m, pl.ds(16 * q, 16), pl.ds(128 * c, 128)))
            return every

        def encode(refs, dst, steps=3):
            every = tiles(refs)
            top = None
            for _, m, q, c in every:
                v = jnp.abs(refs[m][q, c])
                top = v if top is None else jnp.maximum(top, v)
            top = jnp.maximum(top, 2e-34).astype(BF)
            dst[len(every)] = top
            inv = 2.0 ** (120 >> steps) / top.astype(F32)
            for n, m, q, c in every:
                v = refs[m][q, c] * inv
                for _ in range(steps):
                    v = v * jnp.abs(v)
                dst[n] = v.astype(BF)

        def decoder(buf, refs, steps=3):
            every = tiles(refs)
            unit = buf[len(every)].astype(F32) * 0.5 ** (120 >> steps)

            def tile(n):
                v = buf[n].astype(F32)
                m = jnp.exp2(jnp.log2(jnp.abs(v)) * 0.5 ** steps)
                return jnp.where(v < 0, -m, m) * unit
            return every, tile

        def add(refs, buf):
            every, tile = decoder(buf, refs)
            for n, m, q, c in every:
                refs[m][q, c] = refs[m][q, c] + tile(n)

        class Ring:
            def __init__(self, key, pos, dev, parts, sb, rb):
                self.k, self.pos, self.dev, self.parts, self.sb, self.rb = key, pos, dev, parts, sb, rb

            def post(self, i, place, side, d, group):
                encode(self.parts(place, side), self.sb.at[i])
                send(self.k + group, self.sb.at[i], self.rb.at[i], self.dev(d), self.k[0])

            def far(self):
                self.post(0, at(self.pos, 2), 0, 1, ("far", 0))
                self.post(1, at(self.pos, 2), 1, 3, ("far", 1))

            def near_right(self):
                self.post(2, at(self.pos, 1), 1, 1, ("near",))

            def near_left(self):
                self.post(3, at(self.pos, 3), 0, 3, ("near",))

            def relay(self, side):
                place, d = at(self.pos, (1, 3)[side]), (1, 3)[side]
                recv(self.k + ("far", side), self.rb.at[side])
                add(self.parts(place, side), self.rb.at[side])
                self.post(4 + side, place, side, d, ("last",))

            def near_in(self):
                recv(self.k + ("near",), self.rb.at[pl.ds(2, 2)])
                add(self.parts(self.pos, 0), self.rb.at[3])
                add(self.parts(self.pos, 1), self.rb.at[2])

            def last_in(self):
                recv(self.k + ("last",), self.rb.at[pl.ds(4, 2)])
                add(self.parts(self.pos, 0), self.rb.at[4])
                add(self.parts(self.pos, 1), self.rb.at[5])

        wing = cols // 2
        hr = width // 64

        def ring1(w, h, c):
            a, _, adev, _ = raxes(h)
            return Ring((1, w, h, c), a, adev,
                        lambda place, side: [gblk(w, h, place, 2 * side + i).at[:, pl.ds(c * wing, wing)] for i in (0, 1)],
                        s1s.at[2 * w + h, c], s1r.at[2 * w + h, c])

        def ring2(h):
            a, b, _, bdev = raxes(h)
            return Ring((2, DN, h), b, bdev,
                        lambda place, side: [gblk(DN, h, a, place).at[pl.ds(side * hr, hr)]],
                        s2s.at[h], s2r.at[h])

        first = {(w, h, c): ring1(w, h, c) for w in (UP, DN) for h in (0, 1) for c in (0, 1)}
        second = [ring2(h) for h in (0, 1)]

        def part(h, c, place):
            return gblk(UP, h, raxes(h)[0], place).at[:, pl.ds(c * wing, wing)]

        def second_start(w, h, c=None):
            if w == DN:
                for c in (0, 1):
                    first[w, h, c].last_in()
                second[h].far()
                second[h].near_right()
                second[h].near_left()
                return
            first[w, h, c].last_in()
            _, b, _, bdev = raxes(h)
            for d in (2, 1, 3):
                encode([part(h, c, at(b, d))], d2s.at[h, c, d - 1])
                send(("d2", h, c), d2s.at[h, c, d - 1], d2r.at[h, c, d - 1], bdev(d), "d2")

        def third_start(w, h, c=None):
            a, b, _, _ = raxes(h)
            peers_ = [(0, rpeer)] if h == 0 else [(1, zpeer), (2, rzpeer)]
            if w == DN:
                second[h].near_in()
                second[h].last_in()
                encode([gblk(w, h, a, b)], s3s.at[h])
                for i, dev in peers_:
                    send((5, w), s3s.at[h], s3r.at[i], dev, "d3")
                return
            recv(("d2", h, c), d2r.at[h, c])
            for d in range(3):
                add([part(h, c, b)], d2r.at[h, c, d])
            encode([part(h, c, b)], u3s.at[c, h])
            for i, dev in peers_:
                send((5, w, c), u3s.at[c, h], u3r.at[c, i], dev, "u3")

        def finish(w, c=None):
            if w == DN:
                out, mine, theirs, at_, wide = gdn_ref, s3s, s3r, 0, cols
                recv((5, w), s3r)
            else:
                out, mine, theirs, at_, wide = gup_ref, u3s.at[c], u3r.at[c], c * wing, wing
                recv((5, w, c), u3r.at[c])
            for side, one, two in ((j, mine.at[0], theirs.at[0]), (1 - j, theirs.at[1], theirs.at[2])):
                like = [out.at[:, pl.ds(0, wide)]]
                every, tile1 = decoder(one, like)
                _, tile2 = decoder(two, like)
                for n, _, q, _ in every:
                    col = pl.ds(pl.multiple_of(side * cols + at_ + n // (width // 512) * 128, 128), 128)
                    out[q, col] = (tile1(n) + tile2(n)) * factor

        def input_part(n):
            s1, s2 = ((3, 1), (2, 0))[n]
            w = W[UP].reshape(width, cols)
            v = lax.dot_general(both(GP, s1, s2), w, (((1,), (1,)), ((), ())), preferred_element_type=F32)
            PART[s1] = v[:tokens]
            PART[s2] = v[tokens:]
            if n == 0:
                for i, slot in enumerate((3, 1)):
                    send(("g", "t", i), PART.at[slot], DR.at[i], tpeer, "gt")

        def input_send():
            recv(("g", "t", 0), DR.at[0])
            PART[2] = PART[2] + DR[0]
            encode([PART.at[2]], ZS, 4)
            send("gz", ZS, ZR, zpeer, "gz")

        def input_sum():
            recv(("g", "t", 1), DR.at[1])
            recv("gz", ZR)
            every, tile = decoder(ZR, [PART.at[2]], 4)
            for n, _, q, c in every:
                gin_ref[q, c] = (PART[0, q, c] + DR[1, q, c] + tile(n)).astype(BF)

        def energy_x():
            EX[x] = jnp.sum(gdn_ref[...] * gdn_ref[...], axis=0, keepdims=True)
            for d in (1, 2, 3):
                send("ex", EX.at[x], EX.at[x], xdev(d), "ex")

        def energy_y():
            recv("ex", EX.at[pl.ds(0, 3)])
            me = 4 * j + y
            EY[me] = EX[0] + EX[1] + EX[2] + EX[3]
            for dev in [zpeer] + [f(d) for d in (1, 2, 3) for f in (ydev, yzdev)]:
                send("ey", EY.at[me], EY.at[me], dev, "ey")

        def energy_down():
            recv("ey", EY.at[pl.ds(0, 7)])
            total = EY[0]
            for n in range(1, 8):
                total = total + EY[n]
            edn_ref[...] = total * (1.0 / width)

        def energy_pair():
            total = None
            for c in range(2 * len(lanes)):
                v = gup_ref[:, c * 128:(c + 1) * 128]
                total = v * v if total is None else total + v * v
            EU[0] = total
            send("et", EU.at[0], EU.at[1], tpeer, "et")

        def energy_up():
            recv("et", EU.at[1])
            eup_ref[...] = jnp.sum((EU[0] + EU[1]).T, axis=0, keepdims=True) * (1.0 / ff)

        for w in (UP, DN):
            loads[w].wait()
            send(("a2a", w), OTH.at[w], W.at[w, j, y, x], rzpeer, "a2a")
        for c in loads[2:]:
            c.wait()
        for name in ("x", "c"):
            buf = stock[name][0]
            for i in (0, 1):
                rows = pl.ds(i * half, half)
                send((name, "z", i), buf.at[0, rows], buf.at[2, rows], zpeer, "own")
            send((name, "t"), buf.at[0], buf.at[1], tpeer, "own")
        todo = {
            "init": init, "near": near, "step2": step2, "fwd": fwd, "pass": pass_on, "turn": turn,
            "proj": project, "pull": pull_back, "mult": multiply, "ma": multiply_early,
            "far": lambda w, h, c: first[w, h, c].far(),
            "nr": lambda w, h, c: first[w, h, c].near_right(),
            "nl": lambda w, h, c: first[w, h, c].near_left(),
            "rl": lambda w, h, side, c: first[w, h, c].relay(side),
            "ni": lambda w, h, c: first[w, h, c].near_in(),
            "st2": second_start,
            "rl2": lambda w, h, side: second[h].relay(side),
            "st3": third_start, "fin": finish, "ip": input_part, "gz": input_send, "gin": input_sum,
            "ex": energy_x, "ey": energy_y, "edn": energy_down,
            "eu": energy_pair, "eup": energy_up,
        }
        for name, *where in ORDER:
            todo[name](*where)
        for batch, ref in (
            ("a2a", OTH), ("own", RP.at[pl.ds(0, 2)]), ("zt", X.at[pl.ds(0, 2)]),
            ("w", RP.at[:, pl.ds(0, 15 * tokens // 16)]),
            (1, s1s), (2, s2s), ("d2", d2s), ("d3", s3r), ("u3", u3r),
        ):
            sent(batch, ref)
        sent("gt", PART.at[pl.ds(0, 2)])
        sent("gz", ZS)
        sent("ex", EX.at[pl.ds(0, 3)])
        sent("ey", EY.at[pl.ds(0, 7)])
        sent("et", EU.at[0])

    return kernel


def hand_over(results):
    vm = pl.BlockSpec(memory_space=pltpu.VMEM)
    shapes = [jax.ShapeDtypeStruct(v.shape, v.dtype) for v in results]

    def kernel(*refs):
        sem = refs[10]
        moves = [pltpu.make_async_copy(refs[n], refs[5 + n], sem.at[n]) for n in range(5)]
        for c in moves:
            c.start()
        for c in moves:
            c.wait()

    return pl.pallas_call(kernel, out_shape=tuple(shapes), in_specs=[vm] * 5, out_specs=(pl.BlockSpec(memory_space=pltpu.HBM),) * 5,
        scratch_shapes=[pltpu.SemaphoreType.DMA((5,))],
    )(*[pltpu.with_memory_space_constraint(v, pltpu.VMEM) for v in results])


def per_device(inputs, up_proj, down_proj, out_cotangent):
    tokens, width = inputs.shape
    rows, hidden = up_proj.shape
    cols = hidden // 2
    ff = hidden * lax.axis_size("tp")
    all_tokens = tokens * lax.axis_size("rep") * lax.axis_size(FS) * lax.axis_size("tp")
    factor = float(all_tokens) ** (-0.5)
    up3 = up_proj.reshape(2, rows // 2, hidden)
    dn3 = down_proj.T.reshape(2, rows // 2, hidden)
    vm = pl.BlockSpec(memory_space=pltpu.VMEM)
    full = (2, 4, 4, rows)
    lines = rows * cols // 2048
    results = pl.pallas_call(
        make_kernel(tokens, width, cols, ff, factor),
        out_shape=(
            pltpu.VMEM((tokens, width), BF),
            pltpu.VMEM((rows, hidden), F32),
            pltpu.VMEM((rows, hidden), F32),
            pltpu.VMEM((1, rows), F32),
            pltpu.VMEM((1, hidden), F32),
        ),
        in_specs=[pl.BlockSpec(memory_space=pltpu.HBM)] * 4,
        out_specs=(vm,) * 5,
        scratch_shapes=[
            pltpu.VMEM((4, tokens, width), BF),
            pltpu.VMEM((4, tokens, width), BF),
            pltpu.VMEM(full + (4 * tokens,), BF),
            pltpu.VMEM(full + (4 * tokens,), BF),
            pltpu.VMEM((2, 2, 4, 4, 2, rows // 2, cols), BF),
            pltpu.VMEM((4, tokens, cols), F32),
            pltpu.VMEM((4, tokens, cols), BF),
            pltpu.VMEM((4, tokens, cols), BF),
            pltpu.VMEM((2,) + full + (cols,), F32),
            pltpu.VMEM((4, 2, 6, lines + 1, 16, 128), BF),
            pltpu.VMEM((4, 2, 6, lines + 1, 16, 128), BF),
            pltpu.VMEM((2, 6, lines // 2 + 1, 16, 128), BF),
            pltpu.VMEM((2, 6, lines // 2 + 1, 16, 128), BF),
            pltpu.VMEM((2, 2, 3, lines // 2 + 1, 16, 128), BF),
            pltpu.VMEM((2, 2, 3, lines // 2 + 1, 16, 128), BF),
            pltpu.VMEM((2, lines + 1, 16, 128), BF),
            pltpu.VMEM((3, lines + 1, 16, 128), BF),
            pltpu.VMEM((2, 2, lines // 2 + 1, 16, 128), BF),
            pltpu.VMEM((2, 3, lines // 2 + 1, 16, 128), BF),
            pltpu.VMEM((4, tokens, width), F32),
            pltpu.VMEM((2, tokens, width), F32),
            pltpu.VMEM((tokens * width // 2048 + 1, 16, 128), BF),
            pltpu.VMEM((tokens * width // 2048 + 1, 16, 128), BF),
            pltpu.VMEM((4, 1, hidden), F32),
            pltpu.VMEM((8, 1, hidden), F32),
            pltpu.VMEM((2, rows, 128), F32),
            pltpu.VMEM((2, 2, rows // 2, cols), BF),
            pltpu.SemaphoreType.DMA((BATCHES,)),
            pltpu.SemaphoreType.DMA((WAITS,)),
            pltpu.SemaphoreType.DMA((6,)),
        ],
        compiler_params=pltpu.CompilerParams(
            collective_id=0, has_side_effects=True, vmem_limit_bytes=52 * 1024 * 1024
        ),
    )(*[pltpu.with_memory_space_constraint(v, pltpu.HBM) for v in (inputs, up3, dn3, out_cotangent)])
    gin, gup, gdn, eup, edn = hand_over(results)
    return gin, gup, gdn.T, eup.reshape(rows), edn.reshape(hidden)


def solution(mesh):
    torus = Mesh(
        mesh.devices.reshape(mesh.shape["rep"], 2, 4, 4, mesh.shape["tp"]),
        ("rep", "fs_0", "fs_1", "fs_2", "tp"),
    )
    placed = (P(REP_FS_TP, None), P(FS, "tp"), P("tp", FS), P(REP_FS_TP, None))
    return jax.shard_map(
        per_device,
        mesh=torus,
        in_specs=placed,
        out_specs=(P(REP_FS_TP, None), P(FS, "tp"), P("tp", FS), P(FS), P("tp")),
        check_vma=False,
    )
```

```python
import jax
import jax.numpy as jnp
from jax import lax
from jax.experimental import pallas as pl
from jax.experimental.pallas import tpu as pltpu
from jax.sharding import Mesh
from jax.sharding import PartitionSpec as P

FS = ("fs_0", "fs_1", "fs_2")
REP_FS_TP = ("rep", "fs_0", "fs_1", "fs_2", "tp")
MESH = pl.DeviceIdType.MESH
BF = jnp.bfloat16
F32 = jnp.float32
RIGHT, LEFT = 0, 1
UP, DN = 0, 1
WAITS, BATCHES = 109, 14


ORDER = [
    ("init", 0, 0), ("init", 1, 0), ("init", 0, 1), ("init", 1, 1), ("near", 0, 0, 1), ("near", 0, 0, 0),
    ("near", 0, 1, 0), ("near", 0, 1, 1), ("turn", "c", 1), ("step2", 0, 0), ("fwd", 0, 0, 2, 1),
    ("near", 1, 1, 1), ("near", 1, 0, 1), ("near", 1, 1, 0), ("step2", 0, 1), ("fwd", 0, 0, 2, 0),
    ("fwd", 0, 1, 2, 0), ("fwd", 1, 1, 2, 0), ("near", 1, 0, 0), ("pass", "x", 0), ("fwd", 0, 1, 2, 1),
    ("fwd", 0, 0, 0, 1), ("fwd", 0, 1, 0, 1), ("fwd", 1, 0, 0, 0), ("fwd", 1, 1, 0, 0), ("turn", "x", 1),
    ("pass", "x", 1), ("fwd", 1, 1, 1, 1), ("fwd", 0, 1, 0, 0), ("fwd", 0, 0, 1, 0), ("fwd", 0, 1, 3, 0),
    ("fwd", 0, 0, 3, 0), ("fwd", 1, 0, 2, 0), ("turn", "x", 0), ("fwd", 0, 0, 1, 1), ("fwd", 0, 1, 3, 1),
    ("fwd", 0, 0, 3, 1), ("fwd", 0, 1, 1, 1), ("turn", "x", 3), ("turn", "c", 0), ("fwd", 0, 0, 0, 0),
    ("fwd", 1, 0, 2, 1), ("fwd", 0, 1, 1, 0), ("fwd", 1, 1, 1, 0), ("step2", 1, 1), ("fwd", 1, 1, 2, 1),
    ("turn", "x", 2), ("pass", "c", 0), ("step2", 1, 0), ("proj", 0), ("ma", 1, 1), ("fwd", 1, 1, 0, 1),
    ("fwd", 1, 0, 3, 0), ("fwd", 1, 0, 3, 1), ("ma", 1, 0), ("pass", "c", 1), ("fwd", 1, 1, 3, 0),
    ("fwd", 1, 0, 1, 0), ("turn", "c", 2), ("fwd", 1, 1, 3, 1), ("fwd", 1, 0, 1, 1), ("fwd", 1, 0, 0, 1),
    ("proj", 1), ("turn", "c", 3), ("mult", 1, 0), ("far", 1, 0, 0), ("far", 1, 0, 1), ("mult", 1, 1),
    ("nr", 1, 0, 0), ("far", 1, 1, 0), ("pull", 0), ("nr", 1, 1, 0), ("nl", 1, 0, 0), ("pull", 1),
    ("far", 1, 1, 1), ("ip", 0), ("rl", 1, 0, 0, 0), ("nl", 1, 0, 1), ("nl", 1, 1, 0), ("nr", 1, 1, 1),
    ("rl", 1, 1, 1, 0), ("rl", 1, 0, 1, 1), ("nr", 1, 0, 1), ("nl", 1, 1, 1), ("mult", 0, 0), ("rl", 1, 0, 1, 0),
    ("rl", 1, 1, 0, 0), ("rl", 1, 0, 0, 1), ("ip", 1), ("gz",), ("rl", 1, 1, 0, 1), ("far", 0, 0, 1),
    ("rl", 1, 1, 1, 1), ("mult", 0, 1), ("nr", 0, 1, 0), ("ni", 1, 0, 0), ("far", 0, 1, 0), ("ni", 1, 0, 1),
    ("far", 0, 0, 0), ("ni", 1, 1, 0), ("ni", 1, 1, 1), ("nl", 0, 0, 0), ("nr", 0, 0, 0), ("st2", 1, 0),
    ("st2", 1, 1), ("far", 0, 1, 1), ("rl", 0, 0, 1, 0), ("rl", 0, 0, 0, 0), ("rl2", 1, 0, 1), ("nl", 0, 1, 0),
    ("rl", 0, 1, 1, 0), ("rl2", 1, 0, 0), ("rl", 0, 1, 0, 0), ("rl2", 1, 1, 1), ("nl", 0, 1, 1), ("rl2", 1, 1, 0),
    ("nr", 0, 1, 1), ("nr", 0, 0, 1), ("rl", 0, 1, 1, 1), ("ni", 0, 0, 0), ("nl", 0, 0, 1), ("rl", 0, 0, 0, 1),
    ("rl", 0, 1, 0, 1), ("rl", 0, 0, 1, 1), ("st2", 0, 0, 0), ("st3", 1, 0), ("st3", 1, 1), ("ni", 0, 1, 0),
    ("ni", 0, 0, 1), ("st2", 0, 1, 0), ("ni", 0, 1, 1), ("st2", 0, 0, 1), ("st2", 0, 1, 1), ("fin", 1), ("ex",),
    ("st3", 0, 1, 0), ("gin",), ("st3", 0, 0, 0), ("st3", 0, 0, 1), ("ey",), ("st3", 0, 1, 1), ("fin", 0, 0),
    ("fin", 0, 1), ("eu",), ("eup",), ("edn",),
]


def make_kernel(tokens, width, cols, ff, factor):
    lanes = [pl.ds(c * 128, 128) for c in range(cols // 128)]

    def kernel(
        x_ref, up_ref, dn_ref, cot_ref,
        gin_ref, gup_ref, gdn_ref, eup_ref, edn_ref,
        X, C, XT, CT, W, RP, ACT, GP, G,
        s1s, s1r, s2s, s2r, d2s, d2r, s3s, s3r, u3s, u3r,
        PART, DR, ZS, ZR, EX, EY, EU,
        OTH, ssem, rsem, lsem,
    ):
        r = lax.axis_index("rep")
        j = lax.axis_index("fs_0")
        y = lax.axis_index("fs_1")
        x = lax.axis_index("fs_2")
        t = lax.axis_index("tp")

        def at(pos, d):
            return lax.rem(pos + d, 4)

        def xdev(d):
            return {"fs_2": at(x, d)}

        def ydev(d):
            return {"fs_1": at(y, d)}

        def yzdev(d):
            return {"fs_0": 1 - j, "fs_1": at(y, d)}

        zpeer = {"fs_0": 1 - j}
        rpeer = {"rep": 1 - r}
        rzpeer = {"rep": 1 - r, "fs_0": 1 - j}
        tpeer = {"tp": 1 - t}

        own = pl.ds(pl.multiple_of(j * cols, cols), cols)
        other = pl.ds(pl.multiple_of((1 - j) * cols, cols), cols)
        loads = [
            pltpu.make_async_copy(up_ref.at[:, :, other], OTH.at[UP], lsem.at[0]),
            pltpu.make_async_copy(dn_ref.at[:, :, other], OTH.at[DN], lsem.at[1]),
            pltpu.make_async_copy(up_ref.at[:, :, own], W.at[UP, j, y, x], lsem.at[2]),
            pltpu.make_async_copy(dn_ref.at[:, :, own], W.at[DN, j, y, x], lsem.at[3]),
            pltpu.make_async_copy(x_ref, X.at[0], lsem.at[4]),
            pltpu.make_async_copy(cot_ref, C.at[0], lsem.at[5]),
        ]
        for c in loads:
            c.start()

        barrier = pltpu.get_barrier_semaphore()
        peers = [xdev(1), xdev(2), xdev(3), ydev(1), ydev(2), ydev(3), zpeer, rpeer, rzpeer, tpeer, yzdev(1), yzdev(2), yzdev(3)]
        for dev in peers:
            pl.semaphore_signal(barrier, inc=1, device_id=dev, device_id_type=MESH)
        pl.semaphore_wait(barrier, len(peers))

        arrivals, departures = {}, {}

        def slot_of(table, group):
            return table.setdefault(group, len(table))

        def send(group, src, dst, dev, batch):
            pltpu.make_async_remote_copy(
                src_ref=src, dst_ref=dst,
                send_sem=ssem.at[slot_of(departures, batch)], recv_sem=rsem.at[slot_of(arrivals, group)],
                device_id=dev, device_id_type=MESH,
            ).start()

        def recv(group, ref):
            pltpu.make_async_copy(ref, ref, rsem.at[arrivals[group]]).wait()

        def sent(batch, ref):
            pltpu.make_async_copy(ref, ref, ssem.at[departures[batch]]).wait()

        half = tokens // 2

        def blk(ref, w, h, a, b):
            z = j if h == 0 else 1 - j
            return ref.at[w, z, b, a] if h == 0 else ref.at[w, z, a, b]

        def axes(h):
            return (x, y, xdev, ydev) if h == 0 else (y, x, ydev, xdev)

        def init(w, h):
            a, b, adev, bdev = axes(h)
            ref = blk(W, w, h, a, b)
            if h == 1:
                recv(("a2a", w), ref)
            send((1, w, h, 0), ref, ref, adev(1), "w")
            send((1, w, h, 1), ref, ref, adev(3), "w")
            spread(w, h, 0, a)

        def spread(w, h, s, a2):
            _, b, _, bdev = axes(h)
            ref = blk(W, w, h, a2, b)
            send((2, w, h, s, 0), ref, ref, bdev(1), "w")
            send((2, w, h, s, 1), ref, ref, bdev(3), "w")

        def near(w, h, side):
            a, b, adev, _ = axes(h)
            place, away = ((at(a, 3), 1), (at(a, 1), 3))[side]
            ref = blk(W, w, h, place, b)
            recv((1, w, h, side), ref)
            send((1, w, h, 2), ref.at[side], ref.at[side], adev(away), "w")
            spread(w, h, 1 + side, place)

        def step2(w, h):
            a, b, _, _ = axes(h)
            recv((1, w, h, 2), blk(W, w, h, at(a, 2), b))
            spread(w, h, 3, at(a, 2))

        def fwd(w, h, s, side):
            a, b, _, bdev = axes(h)
            a2 = at(a, (0, 3, 1, 2)[s])
            place, away = ((at(b, 3), 1), (at(b, 1), 3))[side]
            ref = blk(W, w, h, a2, place)
            recv((2, w, h, s, side), ref)
            send((3, w), ref.at[side], ref.at[side], bdev(away), "w")

        whole = set()

        def fin(w):
            if w not in whole:
                whole.add(w)
                recv((3, w), W.at[w, 0, pl.ds(0, 2)])

        stock = {"x": (X, XT), "c": (C, CT)}

        def pass_on(name, i):
            rows = pl.ds(i * half, half)
            buf = stock[name][0]
            recv((name, "z", i), buf.at[2, rows])
            send((name, "zt"), buf.at[2, rows], buf.at[3, rows], tpeer, "zt")

        def turn(name, slot):
            src, dst = stock[name]
            if slot == 1:
                recv((name, "t"), src.at[1])
            if slot == 3:
                recv((name, "zt"), src.at[3])
            v = src[slot].T
            dst[:, :, :, :, slot * tokens:(slot + 1) * tokens] = v.reshape(2, 4, 4, width // 32, tokens)

        def weight(w):
            return W[w].reshape(width, cols)

        def both(ref, s1, s2):
            return jnp.concatenate([ref[s1], ref[s2]], axis=0)

        def project(n):
            s1, s2 = 2 * n, 2 * n + 1
            fin(UP)
            pre = jnp.maximum(jnp.dot(both(X, s1, s2), weight(UP), preferred_element_type=F32), 0.0)
            for n, slot in enumerate((s1, s2)):
                v = pre[n * tokens:(n + 1) * tokens]
                RP[slot] = v
                ACT[slot] = (v * v).astype(BF)

        def pull_back(n):
            s1, s2 = 2 * n, 2 * n + 1
            fin(DN)
            back = jnp.dot(both(C, s1, s2), weight(DN), preferred_element_type=F32)
            for n, slot in enumerate((s1, s2)):
                GP[slot] = (2.0 * RP[slot] * back[n * tokens:(n + 1) * tokens]).astype(BF)

        lhs_of = (XT, CT)
        rhs_of = (GP, ACT)

        def gblk(w, h, a, b):
            z = j if h == 0 else 1 - j
            return G.at[w, z, a, b] if h == 0 else G.at[w, z, b, a]

        def raxes(h):
            return (y, x, ydev, xdev) if h == 0 else (x, y, xdev, ydev)

        def product(w, h, lo, n):
            z = j if h == 0 else 1 - j
            left = lhs_of[w][z, :, :, :, lo * tokens:(lo + n) * tokens].reshape(width // 2, n * tokens)
            right = rhs_of[w][lo:lo + n].reshape(n * tokens, cols)
            out = jnp.dot(left, right, preferred_element_type=F32)
            return G.at[w, z], out.reshape(4, 4, width // 32, cols)

        begun = set()

        def multiply_early(w, h):
            ref, out = product(w, h, 0, 2)
            ref[...] = out
            begun.add((w, h))

        def multiply(w, h):
            if (w, h) in begun:
                ref, out = product(w, h, 2, 2)
                ref[...] = ref[...] + out
            else:
                ref, out = product(w, h, 0, 4)
                ref[...] = out

        def tiles(refs):
            every = []
            for m, ref in enumerate(refs):
                rows, wide = ref.shape
                for c in range(wide // 128):
                    for q in range(rows // 16):
                        every.append((len(every), m, pl.ds(16 * q, 16), pl.ds(128 * c, 128)))
            return every

        def encode(refs, dst, steps=3):
            every = tiles(refs)
            top = None
            for _, m, q, c in every:
                v = jnp.abs(refs[m][q, c])
                top = v if top is None else jnp.maximum(top, v)
            top = jnp.maximum(top, 2e-34).astype(BF)
            dst[len(every)] = top
            inv = 2.0 ** (120 >> steps) / top.astype(F32)
            for n, m, q, c in every:
                v = refs[m][q, c] * inv
                for _ in range(steps):
                    v = v * jnp.abs(v)
                dst[n] = v.astype(BF)

        def decoder(buf, refs, steps=3):
            every = tiles(refs)
            unit = buf[len(every)].astype(F32) * 0.5 ** (120 >> steps)

            def tile(n):
                v = buf[n].astype(F32)
                m = jnp.exp2(jnp.log2(jnp.abs(v)) * 0.5 ** steps)
                return jnp.where(v < 0, -m, m) * unit
            return every, tile

        def add(refs, buf):
            every, tile = decoder(buf, refs)
            for n, m, q, c in every:
                refs[m][q, c] = refs[m][q, c] + tile(n)

        class Ring:
            def __init__(self, key, pos, dev, parts, sb, rb):
                self.k, self.pos, self.dev, self.parts, self.sb, self.rb = key, pos, dev, parts, sb, rb

            def post(self, i, place, side, d, group):
                encode(self.parts(place, side), self.sb.at[i])
                send(self.k + group, self.sb.at[i], self.rb.at[i], self.dev(d), self.k[0])

            def far(self):
                self.post(0, at(self.pos, 2), 0, 1, ("far", 0))
                self.post(1, at(self.pos, 2), 1, 3, ("far", 1))

            def near_right(self):
                self.post(2, at(self.pos, 1), 1, 1, ("near",))

            def near_left(self):
                self.post(3, at(self.pos, 3), 0, 3, ("near",))

            def relay(self, side):
                place, d = at(self.pos, (1, 3)[side]), (1, 3)[side]
                recv(self.k + ("far", side), self.rb.at[side])
                add(self.parts(place, side), self.rb.at[side])
                self.post(4 + side, place, side, d, ("last",))

            def near_in(self):
                recv(self.k + ("near",), self.rb.at[pl.ds(2, 2)])
                add(self.parts(self.pos, 0), self.rb.at[3])
                add(self.parts(self.pos, 1), self.rb.at[2])

            def last_in(self):
                recv(self.k + ("last",), self.rb.at[pl.ds(4, 2)])
                add(self.parts(self.pos, 0), self.rb.at[4])
                add(self.parts(self.pos, 1), self.rb.at[5])

        wing = cols // 2
        hr = width // 64

        def ring1(w, h, c):
            a, _, adev, _ = raxes(h)
            return Ring((1, w, h, c), a, adev,
                        lambda place, side: [gblk(w, h, place, 2 * side + i).at[:, pl.ds(c * wing, wing)] for i in (0, 1)],
                        s1s.at[2 * w + h, c], s1r.at[2 * w + h, c])

        def ring2(h):
            a, b, _, bdev = raxes(h)
            return Ring((2, DN, h), b, bdev,
                        lambda place, side: [gblk(DN, h, a, place).at[pl.ds(side * hr, hr)]],
                        s2s.at[h], s2r.at[h])

        first = {(w, h, c): ring1(w, h, c) for w in (UP, DN) for h in (0, 1) for c in (0, 1)}
        second = [ring2(h) for h in (0, 1)]

        def part(h, c, place):
            return gblk(UP, h, raxes(h)[0], place).at[:, pl.ds(c * wing, wing)]

        def second_start(w, h, c=None):
            if w == DN:
                for c in (0, 1):
                    first[w, h, c].last_in()
                second[h].far()
                second[h].near_right()
                second[h].near_left()
                return
            first[w, h, c].last_in()
            _, b, _, bdev = raxes(h)
            for d in (2, 1, 3):
                encode([part(h, c, at(b, d))], d2s.at[h, c, d - 1])
                send(("d2", h, c), d2s.at[h, c, d - 1], d2r.at[h, c, d - 1], bdev(d), "d2")

        def third_start(w, h, c=None):
            a, b, _, _ = raxes(h)
            peers_ = [(0, rpeer)] if h == 0 else [(1, zpeer), (2, rzpeer)]
            if w == DN:
                second[h].near_in()
                second[h].last_in()
                encode([gblk(w, h, a, b)], s3s.at[h])
                for i, dev in peers_:
                    send((5, w), s3s.at[h], s3r.at[i], dev, "d3")
                return
            recv(("d2", h, c), d2r.at[h, c])
            for d in range(3):
                add([part(h, c, b)], d2r.at[h, c, d])
            encode([part(h, c, b)], u3s.at[c, h])
            for i, dev in peers_:
                send((5, w, c), u3s.at[c, h], u3r.at[c, i], dev, "u3")

        def finish(w, c=None):
            if w == DN:
                out, mine, theirs, at_, wide = gdn_ref, s3s, s3r, 0, cols
                recv((5, w), s3r)
            else:
                out, mine, theirs, at_, wide = gup_ref, u3s.at[c], u3r.at[c], c * wing, wing
                recv((5, w, c), u3r.at[c])
            for side, one, two in ((j, mine.at[0], theirs.at[0]), (1 - j, theirs.at[1], theirs.at[2])):
                like = [out.at[:, pl.ds(0, wide)]]
                every, tile1 = decoder(one, like)
                _, tile2 = decoder(two, like)
                for n, _, q, _ in every:
                    col = pl.ds(pl.multiple_of(side * cols + at_ + n // (width // 512) * 128, 128), 128)
                    out[q, col] = (tile1(n) + tile2(n)) * factor

        def input_part(n):
            s1, s2 = ((3, 1), (2, 0))[n]
            w = W[UP].reshape(width, cols)
            v = lax.dot_general(both(GP, s1, s2), w, (((1,), (1,)), ((), ())), preferred_element_type=F32)
            PART[s1] = v[:tokens]
            PART[s2] = v[tokens:]
            if n == 0:
                for i, slot in enumerate((3, 1)):
                    send(("g", "t", i), PART.at[slot], DR.at[i], tpeer, "gt")

        def input_send():
            recv(("g", "t", 0), DR.at[0])
            PART[2] = PART[2] + DR[0]
            encode([PART.at[2]], ZS, 4)
            send("gz", ZS, ZR, zpeer, "gz")

        def input_sum():
            recv(("g", "t", 1), DR.at[1])
            recv("gz", ZR)
            every, tile = decoder(ZR, [PART.at[2]], 4)
            for n, _, q, c in every:
                gin_ref[q, c] = (PART[0, q, c] + DR[1, q, c] + tile(n)).astype(BF)

        def energy_x():
            EX[x] = jnp.sum(gdn_ref[...] * gdn_ref[...], axis=0, keepdims=True)
            for d in (1, 2, 3):
                send("ex", EX.at[x], EX.at[x], xdev(d), "ex")

        def energy_y():
            recv("ex", EX.at[pl.ds(0, 3)])
            me = 4 * j + y
            EY[me] = EX[0] + EX[1] + EX[2] + EX[3]
            for dev in [zpeer] + [f(d) for d in (1, 2, 3) for f in (ydev, yzdev)]:
                send("ey", EY.at[me], EY.at[me], dev, "ey")

        def energy_down():
            recv("ey", EY.at[pl.ds(0, 7)])
            total = EY[0]
            for n in range(1, 8):
                total = total + EY[n]
            edn_ref[...] = total * (1.0 / width)

        def energy_pair():
            total = None
            for c in range(2 * len(lanes)):
                v = gup_ref[:, c * 128:(c + 1) * 128]
                total = v * v if total is None else total + v * v
            EU[0] = total
            send("et", EU.at[0], EU.at[1], tpeer, "et")

        def energy_up():
            recv("et", EU.at[1])
            eup_ref[...] = jnp.sum((EU[0] + EU[1]).T, axis=0, keepdims=True) * (1.0 / ff)

        for w in (UP, DN):
            loads[w].wait()
            send(("a2a", w), OTH.at[w], W.at[w, j, y, x], rzpeer, "a2a")
        for c in loads[2:]:
            c.wait()
        for name in ("x", "c"):
            buf = stock[name][0]
            for i in (0, 1):
                rows = pl.ds(i * half, half)
                send((name, "z", i), buf.at[0, rows], buf.at[2, rows], zpeer, "own")
            send((name, "t"), buf.at[0], buf.at[1], tpeer, "own")
        todo = {
            "init": init, "near": near, "step2": step2, "fwd": fwd, "pass": pass_on, "turn": turn,
            "proj": project, "pull": pull_back, "mult": multiply, "ma": multiply_early,
            "far": lambda w, h, c: first[w, h, c].far(),
            "nr": lambda w, h, c: first[w, h, c].near_right(),
            "nl": lambda w, h, c: first[w, h, c].near_left(),
            "rl": lambda w, h, side, c: first[w, h, c].relay(side),
            "ni": lambda w, h, c: first[w, h, c].near_in(),
            "st2": second_start,
            "rl2": lambda w, h, side: second[h].relay(side),
            "st3": third_start, "fin": finish, "ip": input_part, "gz": input_send, "gin": input_sum,
            "ex": energy_x, "ey": energy_y, "edn": energy_down,
            "eu": energy_pair, "eup": energy_up,
        }
        for name, *where in ORDER:
            todo[name](*where)
        for batch, ref in (
            ("a2a", OTH), ("own", RP.at[pl.ds(0, 2)]), ("zt", X.at[pl.ds(0, 2)]),
            ("w", RP.at[:, pl.ds(0, 15 * tokens // 16)]),
            (1, s1s), (2, s2s), ("d2", d2s), ("d3", s3r), ("u3", u3r),
        ):
            sent(batch, ref)
        sent("gt", PART.at[pl.ds(0, 2)])
        sent("gz", ZS)
        sent("ex", EX.at[pl.ds(0, 3)])
        sent("ey", EY.at[pl.ds(0, 7)])
        sent("et", EU.at[0])

    return kernel


def hand_over(results):
    vm = pl.BlockSpec(memory_space=pltpu.VMEM)
    shapes = [jax.ShapeDtypeStruct(v.shape, v.dtype) for v in results]

    def kernel(*refs):
        sem = refs[10]
        moves = [pltpu.make_async_copy(refs[n], refs[5 + n], sem.at[n]) for n in range(5)]
        for c in moves:
            c.start()
        for c in moves:
            c.wait()

    return pl.pallas_call(kernel, out_shape=tuple(shapes), in_specs=[vm] * 5, out_specs=(pl.BlockSpec(memory_space=pltpu.HBM),) * 5,
        scratch_shapes=[pltpu.SemaphoreType.DMA((5,))],
    )(*[pltpu.with_memory_space_constraint(v, pltpu.VMEM) for v in results])


def per_device(inputs, up_proj, down_proj, out_cotangent):
    tokens, width = inputs.shape
    rows, hidden = up_proj.shape
    cols = hidden // 2
    ff = hidden * lax.axis_size("tp")
    all_tokens = tokens * lax.axis_size("rep") * lax.axis_size(FS) * lax.axis_size("tp")
    factor = float(all_tokens) ** (-0.5)
    up3 = up_proj.reshape(2, rows // 2, hidden)
    dn3 = down_proj.T.reshape(2, rows // 2, hidden)
    vm = pl.BlockSpec(memory_space=pltpu.VMEM)
    full = (2, 4, 4, rows)
    lines = rows * cols // 2048
    results = pl.pallas_call(
        make_kernel(tokens, width, cols, ff, factor),
        out_shape=(
            pltpu.VMEM((tokens, width), BF),
            pltpu.VMEM((rows, hidden), F32),
            pltpu.VMEM((rows, hidden), F32),
            pltpu.VMEM((1, rows), F32),
            pltpu.VMEM((1, hidden), F32),
        ),
        in_specs=[pl.BlockSpec(memory_space=pltpu.HBM)] * 4,
        out_specs=(vm,) * 5,
        scratch_shapes=[
            pltpu.VMEM((4, tokens, width), BF),
            pltpu.VMEM((4, tokens, width), BF),
            pltpu.VMEM(full + (4 * tokens,), BF),
            pltpu.VMEM(full + (4 * tokens,), BF),
            pltpu.VMEM((2, 2, 4, 4, 2, rows // 2, cols), BF),
            pltpu.VMEM((4, tokens, cols), F32),
            pltpu.VMEM((4, tokens, cols), BF),
            pltpu.VMEM((4, tokens, cols), BF),
            pltpu.VMEM((2,) + full + (cols,), F32),
            pltpu.VMEM((4, 2, 6, lines + 1, 16, 128), BF),
            pltpu.VMEM((4, 2, 6, lines + 1, 16, 128), BF),
            pltpu.VMEM((2, 6, lines // 2 + 1, 16, 128), BF),
            pltpu.VMEM((2, 6, lines // 2 + 1, 16, 128), BF),
            pltpu.VMEM((2, 2, 3, lines // 2 + 1, 16, 128), BF),
            pltpu.VMEM((2, 2, 3, lines // 2 + 1, 16, 128), BF),
            pltpu.VMEM((2, lines + 1, 16, 128), BF),
            pltpu.VMEM((3, lines + 1, 16, 128), BF),
            pltpu.VMEM((2, 2, lines // 2 + 1, 16, 128), BF),
            pltpu.VMEM((2, 3, lines // 2 + 1, 16, 128), BF),
            pltpu.VMEM((4, tokens, width), F32),
            pltpu.VMEM((2, tokens, width), F32),
            pltpu.VMEM((tokens * width // 2048 + 1, 16, 128), BF),
            pltpu.VMEM((tokens * width // 2048 + 1, 16, 128), BF),
            pltpu.VMEM((4, 1, hidden), F32),
            pltpu.VMEM((8, 1, hidden), F32),
            pltpu.VMEM((2, rows, 128), F32),
            pltpu.VMEM((2, 2, rows // 2, cols), BF),
            pltpu.SemaphoreType.DMA((BATCHES,)),
            pltpu.SemaphoreType.DMA((WAITS,)),
            pltpu.SemaphoreType.DMA((6,)),
        ],
        compiler_params=pltpu.CompilerParams(
            collective_id=0, has_side_effects=True, vmem_limit_bytes=52 * 1024 * 1024
        ),
    )(*[pltpu.with_memory_space_constraint(v, pltpu.HBM) for v in (inputs, up3, dn3, out_cotangent)])
    gin, gup, gdn, eup, edn = hand_over(results)
    return gin, gup, gdn.T, eup.reshape(rows), edn.reshape(hidden)


def solution(mesh):
    torus = Mesh(
        mesh.devices.reshape(mesh.shape["rep"], 2, 4, 4, mesh.shape["tp"]),
        ("rep", "fs_0", "fs_1", "fs_2", "tp"),
    )
    placed = (P(REP_FS_TP, None), P(FS, "tp"), P("tp", FS), P(REP_FS_TP, None))
    return jax.shard_map(
        per_device,
        mesh=torus,
        in_specs=placed,
        out_specs=(P(REP_FS_TP, None), P(FS, "tp"), P("tp", FS), P(FS), P("tp")),
        check_vma=False,
    )
```
